32 devices in a mesh: dp: 4 (over y, x), kv: 4 (over z), tp: 2 (over core).
Axes of the slice: x: 2, y: 2, z: 4, core: 2. Of those that a mesh axis runs over, the one named last changes fastest.
Arguments:
- tokens: bfloat16 [64, 16, 2048], P('dp'), may hold values from -6 to 6
- norm_gain: float32 [2048], replicated, may hold values from 0.1 to 1.9
- query_weight: bfloat16 [2048, 1024], P(None, 'tp'), may hold values from -0.125 to 0.125
- key_weight: bfloat16 [2048, 256], P(None, 'tp'), may hold values from -0.125 to 0.125
- value_weight: bfloat16 [2048, 256], P(None, 'tp'), may hold values from -0.125 to 0.125
- forget_weight: bfloat16 [2048, 8], replicated, may hold values from -0.125 to 0.125
- forget_bias: float32 [8], replicated, may hold values from 0 to 4
- query_gain: float32 [128], replicated, may hold values from 0.1 to 1.9
- key_gain: float32 [128], replicated, may hold values from 0.1 to 1.9
- output_weight: bfloat16 [1024, 2048], P('tp', 'kv'), may hold values from -0.1875 to 0.1875
- cache_keys: bfloat16 [64, 1024, 2, 128], P('dp', 'kv', 'tp'), may hold values from -512 to 512
- cache_values: bfloat16 [64, 1024, 2, 128], P('dp', 'kv', 'tp'), may hold values from -6 to 6
- cache_logcum: float32 [64, 1024, 8], P('dp', 'kv', 'tp'), may hold values from -205 to 0, as said below
- pending_keys: bfloat16 [64, 4, 2, 128], P('dp', None, 'tp'), may hold values from -6 to 6
- pending_values: bfloat16 [64, 4, 2, 128], P('dp', None, 'tp'), may hold values from -6 to 6
- pending_logcum: float32 [64, 4, 8], P('dp', None, 'tp'), may hold values from -205 to 0, as said below
- lengths: int32 [64], P('dp'), may hold values from 512 to 1020, as said below
- accepted: int32 [64], P('dp'), may hold values from 1 to 4
- parents: int32 [64, 16], P('dp'), may hold values from -1 to 14, as said below
Outputs:
- result: bfloat16 [64, 16, 2048], P('dp', None, ('kv', 'tp'))
The draws below stay inside these ranges and needn't reach their ends.
Inputs may be any that keep to these rules, and one draw needn't show every extreme that they name: Positions below lengths hold a sequence's past; the last step's accepted proposals go to positions lengths to lengths + accepted - 1. `parents`: the parent of proposal i is -1 (the last accepted token) or a proposal before i. `cache_logcum`: non-increasing along positions for every sequence and head. `pending_logcum`: the cumulative log gates at positions lengths to lengths + 3, continuing cache_logcum.
All inputs are finite; a program needn't handle non-finite values.
Results may differ from the reference program's by a relative error of at most 0.014.
Values may be sent and summed in bfloat16 or wider, within the bound.
No kernel may reach another device: no remote copies, remote signals or barrier semaphores. Data moves between devices by JAX's collectives and lax.ppermute only.
A program may use at most 128 MiB of HBM per device.

```python
import math
import jax
import jax.numpy as jnp
from jax import lax

D = 2048
HEADS = 8
KV_HEADS = 2
HEAD_DIM = 128
PROP = 16
ACC_MAX = 4
POS_DEV = 256
SEQUENCE_COUNT = 64
LEN = 1024
BLOCKS = 4
GROUPS = 2
Q_WIDTH = 1024
KV_WIDTH = 256


def gate_tables(key):
    overall_length = LEN + ACC_MAX
    lengths = jax.random.randint(jax.random.fold_in(key, 101), (SEQUENCE_COUNT,), LEN // 2, LEN - ACC_MAX + 1, dtype=jnp.int32)
    head_order = jax.random.permutation(jax.random.fold_in(key, 102), HEADS)
    fast_count = HEADS // 2
    quick_fading_heads = (head_order < fast_count).astype(jnp.float32)
    slow_rate = jnp.exp(jax.random.uniform(jax.random.fold_in(key, 103), (SEQUENCE_COUNT, 1, HEADS), jnp.float32, math.log(0.2), math.log(0.8))) / LEN
    fast_rate = jnp.exp(jax.random.uniform(jax.random.fold_in(key, 104), (SEQUENCE_COUNT, 1, HEADS), jnp.float32, math.log(0.01), math.log(1.0 / 30.0)))
    fading_speed = quick_fading_heads * fast_rate + (1.0 - quick_fading_heads) * slow_rate
    block_count = overall_length // POS_DEV + 1
    block_spread = jnp.exp(jax.random.uniform(jax.random.fold_in(key, 105), (SEQUENCE_COUNT, block_count, HEADS), jnp.float32, math.log(0.4), math.log(2.5)))
    token_place = jnp.arange(overall_length, dtype=jnp.int32)
    block_lookup = block_spread[:, token_place // POS_DEV, :]
    jaggedness = jnp.exp(jax.random.uniform(jax.random.fold_in(key, 106), (SEQUENCE_COUNT, overall_length, HEADS), jnp.float32, math.log(0.5), math.log(2.0)))
    spike_location = jax.random.randint(jax.random.fold_in(key, 107), (SEQUENCE_COUNT, 3), 0, overall_length, dtype=jnp.int32)
    spike_magnitude = jax.random.uniform(jax.random.fold_in(key, 108), (SEQUENCE_COUNT, 3), jnp.float32, 0.22, 0.6)
    spike_penalty = jnp.sum((token_place[None, None, :] == spike_location[:, :, None]).astype(jnp.float32) * spike_magnitude[:, :, None], axis=1)
    length_steps = fading_speed * block_lookup * jaggedness + spike_penalty[:, :, None] * (1.0 - quick_fading_heads)
    return (lengths, -jnp.cumsum(length_steps, axis=1))


def draw_lengths(key, part):
    lengths, cumulative = gate_tables(key)
    return lengths


def draw_cache_logcum(key, part):
    lengths, cumulative = gate_tables(key)
    return cumulative[:, :LEN, :].astype(jnp.float32)


def draw_pending_logcum(key, part):
    lengths, cumulative = gate_tables(key)
    indices = lengths[:, None] + jnp.arange(ACC_MAX, dtype=jnp.int32)[None, :]
    return jnp.take_along_axis(cumulative, indices[:, :, None], axis=1).astype(jnp.float32)


def draw_parents(key, part):
    bounds = jnp.arange(PROP, dtype=jnp.int32)[None, :]
    return jax.random.randint(key, (SEQUENCE_COUNT, PROP), -1, bounds, dtype=jnp.int32)


def draw_cache_keys(key, part):
    shape = (SEQUENCE_COUNT, LEN, KV_HEADS, HEAD_DIM)
    drawn = jnp.clip(jax.random.normal(jax.random.fold_in(key, 201), shape, jnp.float32), -6.0, 6.0)
    return drawn.astype(jnp.bfloat16)


def with_ends(values, stream_key, least, largest):
    index_at = [jax.random.randint(jax.random.fold_in(stream_key, axis), (), 0, length) for axis, length in enumerate(values.shape)]
    main_axis = values.shape.index(max(values.shape))
    next_to = index_at[:main_axis] + [(index_at[main_axis] + 1) % values.shape[main_axis]] + index_at[main_axis + 1:]
    return values.at[tuple(index_at)].set(least).at[tuple(next_to)].set(largest)


def level_of(key, extent, pieces, smallest, largest):
    gain = 1.0
    for dim, shards_of in pieces:
        heights = jax.random.uniform(jax.random.fold_in(jax.random.fold_in(key, 6), dim), (shards_of,), jnp.float32, smallest / len(pieces), largest / len(pieces))
        gain = gain * jnp.repeat(jnp.exp(heights), extent[dim] // shards_of).reshape((-1,) + (1,) * (len(extent) - 1 - dim))
    return gain


def centred(own_key, extent, width, reach, shards=(), kind=jnp.bfloat16):
    array = jax.random.normal(own_key, extent, jnp.float32) * width
    if len(shards) > 0:
        array = level_of(own_key, extent, shards, -0.22, 0.18) * array
    return jnp.clip(array, min=-reach, max=reach).astype(kind)


def setup_inputs(seed: int = 0) -> dict:
    streams_of = jax.random.split(jax.random.key(seed), 20)
    return {
        "tokens": centred(streams_of[0], (SEQUENCE_COUNT, PROP, D), 1.0, 6.0, ((0, 4),)),
        "norm_gain": jnp.clip(1.0 + 0.18 * jax.random.normal(streams_of[1], (D,), jnp.float32), 0.1, 1.9),
        "query_weight": centred(streams_of[2], (D, Q_WIDTH), D ** -0.5, 0.125, ((1, 2),)),
        "key_weight": centred(streams_of[3], (D, KV_WIDTH), D ** -0.5, 0.125, ((1, 2),)),
        "value_weight": centred(streams_of[4], (D, KV_WIDTH), D ** -0.5, 0.125, ((1, 2),)),
        "forget_weight": centred(streams_of[5], (D, HEADS), D ** -0.5, 0.125),
        "forget_bias": jnp.clip(jax.random.uniform(streams_of[6], (HEADS,), jnp.float32, 0.0, 4.0), 0.0, 4.0),
        "query_gain": jnp.clip(1.0 + 0.18 * jax.random.normal(streams_of[7], (HEAD_DIM,), jnp.float32), 0.1, 1.9),
        "key_gain": jnp.clip(1.0 + 0.18 * jax.random.normal(streams_of[8], (HEAD_DIM,), jnp.float32), 0.1, 1.9),
        "output_weight": centred(streams_of[9], (Q_WIDTH, D), Q_WIDTH ** -0.5, 0.1875, ((0, 2), (1, 4))),
        "cache_keys": draw_cache_keys(jax.random.fold_in(streams_of[19], 71), 0),
        "cache_values": centred(streams_of[11], (SEQUENCE_COUNT, LEN, KV_HEADS, HEAD_DIM), 1.0, 6.0, ((0, 4), (1, 4), (2, 2))),
        "cache_logcum": draw_cache_logcum(jax.random.fold_in(streams_of[19], 71), 0),
        "pending_keys": centred(streams_of[13], (SEQUENCE_COUNT, ACC_MAX, KV_HEADS, HEAD_DIM), 1.0, 6.0, ((0, 4), (2, 2))),
        "pending_values": centred(streams_of[14], (SEQUENCE_COUNT, ACC_MAX, KV_HEADS, HEAD_DIM), 1.0, 6.0, ((0, 4), (2, 2))),
        "pending_logcum": draw_pending_logcum(jax.random.fold_in(streams_of[19], 71), 0),
        "lengths": draw_lengths(jax.random.fold_in(streams_of[19], 71), 0),
        "accepted": with_ends(jax.random.randint(streams_of[17], (SEQUENCE_COUNT,), 1, ACC_MAX + 1), jax.random.fold_in(streams_of[17], 1), 1, ACC_MAX).astype(jnp.int32),
        "parents": draw_parents(jax.random.fold_in(streams_of[19], 71), 0),
    }


EPSILON = 1e-06
NEG_LARGE = -1e+30
HIGHEST = lax.Precision.HIGHEST

def head_norm(vectors, gain_vec):
    return vectors * lax.rsqrt(lax.optimization_barrier(jnp.mean(vectors * vectors, axis=-1, keepdims=True)) + EPSILON) * gain_vec

def ancestors(parents):
    node_count = parents.shape[-1]
    indices = jnp.arange(node_count, dtype=jnp.int32)
    reachable = (parents[..., None] == indices).astype(jnp.float32) + jnp.eye(node_count, dtype=jnp.float32)
    for doubling in range((node_count - 1).bit_length()):
        reachable = jnp.minimum(jnp.einsum('sij,sjk->sik', reachable, reachable, precision=HIGHEST), 1.0)
    return reachable

def one_sequence(inputs):
    query_rows, key_rows, value_rows, cumulative, ancestry, cache_k, cache_v, cache_l, pend_k, pend_v, pend_l, length_now, taken_now = inputs
    sharing = HEADS // KV_HEADS
    scaling = HEAD_DIM ** (-0.5)
    token_place = jnp.arange(LEN, dtype=jnp.int32)
    offset = token_place - length_now
    inserted = (offset >= 0) & (offset < taken_now)
    one_hot = ((offset[:, None] == jnp.arange(ACC_MAX, dtype=jnp.int32)[None, :]) & inserted[:, None]).astype(jnp.float32)
    all_keys = jnp.where(inserted[:, None, None], jnp.einsum('la,akd->lkd', one_hot, pend_k.astype(jnp.float32), precision=HIGHEST), cache_k.astype(jnp.float32))
    all_values = jnp.where(inserted[:, None, None], jnp.einsum('la,akd->lkd', one_hot, pend_v.astype(jnp.float32), precision=HIGHEST), cache_v.astype(jnp.float32))
    all_logcum = jnp.where(inserted[:, None], jnp.einsum('la,ah->lh', one_hot, pend_l, precision=HIGHEST), cache_l)
    usable = token_place < length_now + taken_now
    query_group = query_rows.astype(jnp.float32).reshape(PROP, KV_HEADS, sharing, HEAD_DIM)
    scores = jnp.einsum('pkgd,lkd->kgpl', query_group, all_keys, precision=HIGHEST).reshape(HEADS, PROP, LEN)
    scores = scores * scaling + cumulative.T[:, :, None] - all_logcum.T[:, None, :]
    blocked = scores.reshape(HEADS, PROP, BLOCKS, POS_DEV)
    visible = usable.reshape(BLOCKS, POS_DEV)[None, None]
    block_max = lax.optimization_barrier(jnp.max(jnp.where(visible, blocked, NEG_LARGE), axis=-1))
    weights = jnp.where(visible, jnp.exp(blocked - block_max[..., None]), 0.0)
    block_sum = lax.optimization_barrier(jnp.sum(weights, axis=-1))
    rounded = lax.optimization_barrier(weights.astype(jnp.bfloat16)).astype(jnp.float32)
    rounded = rounded.reshape(KV_HEADS, sharing, PROP, BLOCKS, POS_DEV)
    block_values = jnp.einsum('kgpnl,nlkd->kgpnd', rounded, all_values.reshape(BLOCKS, POS_DEV, KV_HEADS, HEAD_DIM), precision=HIGHEST)
    block_values = block_values.reshape(HEADS, PROP, BLOCKS, HEAD_DIM)
    tree_scores = jnp.einsum('pkgd,jkd->kgpj', query_group, key_rows.astype(jnp.float32), precision=HIGHEST).reshape(HEADS, PROP, PROP)
    tree_scores = tree_scores * scaling + cumulative.T[:, :, None] - cumulative.T[:, None, :]
    tree_mask = ancestry[None] > 0.5
    tree_max = lax.optimization_barrier(jnp.max(jnp.where(tree_mask, tree_scores, NEG_LARGE), axis=-1))
    tree_weights = jnp.where(tree_mask, jnp.exp(tree_scores - tree_max[..., None]), 0.0)
    tree_sum = lax.optimization_barrier(jnp.sum(tree_weights, axis=-1))
    tree_rounded = lax.optimization_barrier(tree_weights.astype(jnp.bfloat16)).astype(jnp.float32)
    tree_values = jnp.einsum('kgpj,jkd->kgpd', tree_rounded.reshape(KV_HEADS, sharing, PROP, PROP), value_rows.astype(jnp.float32), precision=HIGHEST).reshape(HEADS, PROP, HEAD_DIM)
    overall = jnp.maximum(lax.optimization_barrier(jnp.max(block_max, axis=-1)), tree_max)
    factor_cache = jnp.exp(block_max - overall[..., None])
    factor_tree = jnp.exp(tree_max - overall)
    denominator = lax.optimization_barrier(jnp.sum(block_sum * factor_cache, axis=-1)) + tree_sum * factor_tree
    numerator = lax.optimization_barrier(jnp.sum(block_values * factor_cache[..., None], axis=2)) + tree_values * factor_tree[..., None]
    return jnp.transpose(numerator / denominator[..., None], (1, 0, 2)).astype(jnp.bfloat16)

def reference(tokens, norm_gain, query_weight, key_weight, value_weight, forget_weight, forget_bias, query_gain, key_gain, output_weight, cache_keys, cache_values, cache_logcum, pending_keys, pending_values, pending_logcum, lengths, accepted, parents):
    seq_count, node_count, model_width = tokens.shape
    widened = tokens.astype(jnp.float32)
    normed = (widened * lax.rsqrt(lax.optimization_barrier(jnp.mean(widened * widened, axis=-1, keepdims=True)) + EPSILON) * norm_gain).astype(jnp.bfloat16)
    token_rows = normed.reshape(seq_count * node_count, model_width)
    query_raw = jnp.dot(token_rows, query_weight, preferred_element_type=jnp.float32)
    key_raw = jnp.dot(token_rows, key_weight, preferred_element_type=jnp.float32)
    value_raw = jnp.dot(token_rows, value_weight, preferred_element_type=jnp.float32)
    queries = head_norm(query_raw.reshape(seq_count, node_count, HEADS, HEAD_DIM), query_gain).astype(jnp.bfloat16)
    keys_new = head_norm(key_raw.reshape(seq_count, node_count, KV_HEADS, HEAD_DIM), key_gain).astype(jnp.bfloat16)
    values_new = value_raw.reshape(seq_count, node_count, KV_HEADS, HEAD_DIM).astype(jnp.bfloat16)
    log_gates = jax.nn.log_sigmoid(jnp.dot(token_rows, forget_weight, preferred_element_type=jnp.float32) + forget_bias).reshape(seq_count, node_count, HEADS)
    ancestry = ancestors(parents)
    choose = (jnp.arange(ACC_MAX, dtype=jnp.int32)[None, :] == (accepted - 1)[:, None]).astype(jnp.float32)
    base_gate = jnp.einsum('sa,sah->sh', choose, pending_logcum, precision=HIGHEST)
    cumulative = base_gate[:, None, :] + jnp.einsum('sij,sjh->sih', ancestry, log_gates, precision=HIGHEST)
    attended = lax.map(one_sequence, (queries, keys_new, values_new, cumulative, ancestry, cache_keys, cache_values, cache_logcum, pending_keys, pending_values, pending_logcum, lengths, accepted))
    grouped = attended.reshape(seq_count, node_count, GROUPS, Q_WIDTH // GROUPS).astype(jnp.float32)
    out_rows = output_weight.reshape(GROUPS, Q_WIDTH // GROUPS, model_width).astype(jnp.float32)
    head_part = jnp.einsum('spgc,gcd->gspd', grouped, out_rows, precision=HIGHEST).astype(jnp.bfloat16)
    return lax.optimization_barrier(jnp.sum(head_part.astype(jnp.float32), axis=0)).astype(jnp.bfloat16)
```

```python
import functools
import math

import jax
import jax.numpy as jnp
from jax import lax
from jax.experimental import pallas as pl
from jax.experimental.pallas import tpu as pltpu
from jax.sharding import PartitionSpec as P

EPSILON = 1e-06
NEG_LARGE = -1e30
HIGHEST = lax.Precision.HIGHEST


def joined(shard, axis, join):
    gathered = jax.tree.map(
        lambda a, kind: lax.all_gather(a.astype(kind), axis),
        shard,
        (jnp.bfloat16, jnp.bfloat16, jnp.bfloat16),
    )

    def take(source):
        return jax.tree.map(
            lambda a, own: lax.dynamic_index_in_dim(a, source, 0, False).astype(own.dtype),
            gathered,
            shard,
        )

    return lax.fori_loop(
        1, lax.axis_size(axis), lambda source, state: join(state, take(source)), take(0)
    )


def head_norm(vectors, gain_vec):
    return (
        vectors
        * lax.rsqrt(jnp.mean(vectors * vectors, axis=-1, keepdims=True) + EPSILON)
        * gain_vec
    )


def ancestors(parents):
    node_count = parents.shape[-1]
    indices = jnp.arange(node_count, dtype=jnp.int32)
    reachable = (parents[..., None] == indices).astype(jnp.float32) + jnp.eye(
        node_count, dtype=jnp.float32
    )
    for doubling in range((node_count - 1).bit_length()):
        reachable = jnp.minimum(
            jnp.einsum("sij,sjk->sik", reachable, reachable, precision=HIGHEST), 1.0
        )
    return reachable


def join_blocks(earlier, later):
    larger = jnp.maximum(earlier[0], later[0])
    left_factor = jnp.exp(earlier[0] - larger)
    right_factor = jnp.exp(later[0] - larger)
    return (
        larger,
        earlier[1] * left_factor + later[1] * right_factor,
        earlier[2] * left_factor[..., None] + later[2] * right_factor[..., None],
    )


def to_rows(values):
    moved = jnp.swapaxes(values, 1, 2)
    return moved.reshape((moved.shape[0] * moved.shape[1],) + moved.shape[2:])


def finish_rows(cache_max, cache_sum, cache_acc, tree_max, tree_sum, tree_acc):
    overall = jnp.maximum(cache_max, tree_max)
    factor_cache = jnp.exp(cache_max - overall)
    factor_tree = jnp.exp(tree_max - overall)
    denominator = cache_sum * factor_cache + tree_sum * factor_tree
    numerator = cache_acc * factor_cache[..., None] + tree_acc * factor_tree[..., None]
    attended = (numerator / denominator[..., None]).astype(jnp.bfloat16)
    return attended.reshape(attended.shape[0], attended.shape[1] * attended.shape[2])


def shards(
    tokens,
    norm_gain,
    query_weight,
    key_weight,
    value_weight,
    forget_weight,
    forget_bias,
    query_gain,
    key_gain,
    output_weight,
    cache_keys,
    cache_values,
    cache_logcum,
    pending_keys,
    pending_values,
    pending_logcum,
    lengths,
    accepted,
    parents,
):
    seq_count, node_count, model_width = tokens.shape
    token_rows = seq_count * node_count
    head_size = query_gain.shape[0]
    query_cols = query_weight.shape[1]
    key_cols = key_weight.shape[1]
    local_heads = query_cols // head_size
    key_heads = key_cols // head_size
    sharing = local_heads // key_heads
    block_len = cache_keys.shape[1]
    most_taken = pending_keys.shape[1]
    scaling = head_size ** (-0.5)
    widened = tokens.reshape(token_rows, model_width).astype(jnp.float32)
    normed = (
        widened
        * lax.rsqrt(jnp.mean(widened * widened, axis=-1, keepdims=True) + EPSILON)
        * norm_gain
    ).astype(jnp.bfloat16)
    joined_weight = jnp.concatenate([query_weight, key_weight, value_weight], axis=1)
    summed = jnp.dot(normed, joined_weight, preferred_element_type=jnp.float32)
    query_part = head_norm(
        summed[:, :query_cols].reshape(token_rows, local_heads, head_size), query_gain
    )
    key_part = head_norm(
        summed[:, query_cols : query_cols + key_cols].reshape(token_rows, key_heads, head_size),
        key_gain,
    )
    queries = query_part.astype(jnp.bfloat16).reshape(
        seq_count, node_count, key_heads, sharing, head_size
    )
    keys_new = key_part.astype(jnp.bfloat16).reshape(seq_count, node_count, key_heads, head_size)
    values_new = (
        summed[:, query_cols + key_cols :]
        .astype(jnp.bfloat16)
        .reshape(seq_count, node_count, key_heads, head_size)
    )
    head_start = lax.axis_index("tp") * local_heads
    forget_cols = lax.dynamic_slice_in_dim(forget_weight, head_start, local_heads, 1)
    gate_bias = lax.dynamic_slice_in_dim(forget_bias, head_start, local_heads, 0)
    log_gates = jax.nn.log_sigmoid(
        jnp.dot(normed, forget_cols, preferred_element_type=jnp.float32) + gate_bias
    ).reshape(seq_count, node_count, local_heads)
    ancestry = ancestors(parents)
    choose = (jnp.arange(most_taken, dtype=jnp.int32)[None, :] == (accepted - 1)[:, None]).astype(
        jnp.float32
    )
    base_gate = jnp.einsum("sa,sah->sh", choose, pending_logcum, precision=HIGHEST)
    cumulative = base_gate[:, None, :] + jnp.einsum(
        "sij,sjh->sih", ancestry, log_gates, precision=HIGHEST
    )
    gate_rows = jnp.swapaxes(cumulative, 1, 2)
    token_place = lax.axis_index("kv") * block_len + jnp.arange(block_len, dtype=jnp.int32)
    offset = token_place[None, :] - lengths[:, None]
    inserted = (offset >= 0) & (offset < accepted[:, None])
    one_hot = (offset[..., None] == jnp.arange(most_taken, dtype=jnp.int32)) & inserted[..., None]
    hot_low = one_hot.astype(jnp.bfloat16)
    merged_keys = jnp.where(
        inserted[..., None, None],
        jnp.einsum(
            "sla,sakd->slkd", hot_low, pending_keys, preferred_element_type=jnp.float32
        ).astype(jnp.bfloat16),
        cache_keys,
    )
    merged_values = jnp.where(
        inserted[..., None, None],
        jnp.einsum(
            "sla,sakd->slkd", hot_low, pending_values, preferred_element_type=jnp.float32
        ).astype(jnp.bfloat16),
        cache_values,
    )
    log_cache = jnp.where(
        inserted[..., None],
        jnp.einsum("sla,sah->slh", one_hot.astype(jnp.float32), pending_logcum, precision=HIGHEST),
        cache_logcum,
    )
    usable = token_place[None, :] < (lengths + accepted)[:, None]
    raw_scores = jnp.einsum(
        "spkgd,slkd->skgpl", queries, merged_keys, preferred_element_type=jnp.float32
    )
    scores = (
        raw_scores.reshape(seq_count, local_heads, node_count, block_len) * scaling
        + gate_rows[..., None]
        - jnp.swapaxes(log_cache, 1, 2)[:, :, None, :]
    )
    visible = usable[:, None, None, :]
    block_max = jnp.max(jnp.where(visible, scores, NEG_LARGE), axis=-1)
    weights = jnp.where(visible, jnp.exp(scores - block_max[..., None]), 0.0)
    block_sum = jnp.sum(weights, axis=-1)
    block_acc = jnp.einsum(
        "skgpl,slkd->skgpd",
        weights.astype(jnp.bfloat16).reshape(seq_count, key_heads, sharing, node_count, block_len),
        merged_values,
        preferred_element_type=jnp.float32,
    )
    block_acc = block_acc.reshape(seq_count, local_heads, node_count, head_size)
    tree_raw = jnp.einsum(
        "spkgd,sjkd->skgpj", queries, keys_new, preferred_element_type=jnp.float32
    )
    tree_scores = (
        tree_raw.reshape(seq_count, local_heads, node_count, node_count) * scaling
        + gate_rows[..., :, None]
        - gate_rows[..., None, :]
    )
    tree_mask = ancestry[:, None] > 0.5
    tree_max = jnp.max(jnp.where(tree_mask, tree_scores, NEG_LARGE), axis=-1)
    tree_weights = jnp.where(tree_mask, jnp.exp(tree_scores - tree_max[..., None]), 0.0)
    tree_sum = jnp.sum(tree_weights, axis=-1)
    tree_acc = jnp.einsum(
        "skgpj,sjkd->skgpd",
        tree_weights.astype(jnp.bfloat16).reshape(
            seq_count, key_heads, sharing, node_count, node_count
        ),
        values_new,
        preferred_element_type=jnp.float32,
    )
    tree_acc = tree_acc.reshape(seq_count, local_heads, node_count, head_size)
    tree_max_rows = to_rows(tree_max)
    tree_sum_rows = to_rows(tree_sum)
    tree_acc_rows = to_rows(tree_acc)
    cache_max, cache_sum, cache_acc = joined((block_max, block_sum, block_acc), "kv", join_blocks)
    attended = finish_rows(
        to_rows(cache_max),
        to_rows(cache_sum),
        to_rows(cache_acc),
        tree_max_rows,
        tree_sum_rows,
        tree_acc_rows,
    )
    head_part = jnp.dot(attended, output_weight, preferred_element_type=jnp.float32)
    head_part = head_part.reshape(seq_count, node_count, output_weight.shape[1])
    return lax.psum_scatter(head_part.astype(jnp.bfloat16), "tp", scatter_dimension=2, tiled=True)


LOG2E = math.log2(math.e)
MASKED = 2.0**100
NT = (((1,), (1,)), ((), ()))


def in_vmem(shape, dtype):
    return pltpu.VMEM(shape, dtype)


def held(array):
    return pltpu.with_memory_space_constraint(array, pltpu.VMEM)


def partner_of(place, step):
    return jnp.bitwise_xor(place, step)


def attend_kernel(
    kv_size,
    lengths,
    tokens,
    norm_gain,
    query_weight,
    key_weight,
    value_weight,
    forget_rows,
    query_gain,
    key_gain,
    cache_keys,
    cache_values,
    cache_logcum,
    *refs,
):
    packed = refs[:kv_size]
    own_queries, own_keys, own_values, own_gates = refs[kv_size : kv_size + 4]
    (
        token_buf,
        weight_buf,
        key_buf,
        value_buf,
        normed_buf,
        summed_buf,
        query_buf,
        new_key_buf,
        new_value_buf,
        token_sem,
        weight_sem,
        cache_sem,
    ) = refs[kv_size + 4 :]
    place = lax.axis_index("kv")
    rows, width = tokens.shape
    query_cols = query_weight.shape[1]
    head_size = key_weight.shape[1]
    heads = query_cols // head_size
    seq_count, block_len = cache_keys.shape[0], cache_keys.shape[1]
    nodes = rows // seq_count
    group = seq_count // kv_size
    row_parts = token_sem.shape[0]
    row_part = rows // row_parts
    depth_parts = weight_sem.shape[0]
    depth = width // depth_parts

    def token_copy(part):
        span = pl.ds(part * row_part, row_part)
        return pltpu.make_async_copy(tokens.at[span], token_buf.at[span], token_sem.at[part])

    def weight_copies(part):
        span = pl.ds(part * depth, depth)
        return [
            pltpu.make_async_copy(
                query_weight.at[span],
                weight_buf.at[span, pl.ds(0, query_cols)],
                weight_sem.at[part, 0],
            ),
            pltpu.make_async_copy(
                key_weight.at[span],
                weight_buf.at[span, pl.ds(query_cols, head_size)],
                weight_sem.at[part, 1],
            ),
            pltpu.make_async_copy(
                value_weight.at[span],
                weight_buf.at[span, pl.ds(query_cols + head_size, head_size)],
                weight_sem.at[part, 2],
            ),
        ]

    def cache_copies(step):
        span = pl.ds(partner_of(place, step) * group, group)
        return [
            pltpu.make_async_copy(cache_keys.at[span], key_buf.at[step], cache_sem.at[step, 0]),
            pltpu.make_async_copy(cache_values.at[span], value_buf.at[step], cache_sem.at[step, 1]),
        ]

    order = list(range(kv_size - 1, -1, -1))
    for part in range(row_parts):
        token_copy(part).start()
    for part in range(depth_parts):
        for copy in weight_copies(part):
            copy.start()
    for step in order:
        for copy in cache_copies(step):
            copy.start()

    gain = norm_gain[...]
    for part in range(row_parts):
        token_copy(part).wait()
        for first in range(part * row_part, (part + 1) * row_part, nodes):
            widened = token_buf[pl.ds(first, nodes), :].astype(jnp.float32)
            mean = jnp.mean(widened * widened, axis=1, keepdims=True)
            normed_buf[pl.ds(first, nodes), :] = (
                widened * lax.rsqrt(mean + EPSILON) * gain
            ).astype(jnp.bfloat16)

    for part in range(depth_parts):
        for copy in weight_copies(part):
            copy.wait()
        span = pl.ds(part * depth, depth)
        product = jnp.dot(
            normed_buf[:, span], weight_buf[span, :], preferred_element_type=jnp.float32
        )
        if part == 0:
            summed_buf[...] = product
        else:
            summed_buf[...] += product

    own_rows = pl.ds(pl.multiple_of(place * (group * nodes), group * nodes), group * nodes)
    own_gates[...] = lax.dot_general(
        forget_rows[...], normed_buf[own_rows, :], NT, preferred_element_type=jnp.float32
    )

    def head_norm(vectors, gain_vec):
        mean = jnp.mean(vectors * vectors, axis=1, keepdims=True)
        return (vectors * lax.rsqrt(mean + EPSILON) * gain_vec).astype(jnp.bfloat16)

    for head in range(heads):
        normal = head_norm(
            summed_buf[:, head * head_size : (head + 1) * head_size], query_gain[...]
        )
        query_buf[:, head * nodes : (head + 1) * nodes, :] = normal.reshape(
            seq_count, nodes, head_size
        )
    new_key_buf[...] = head_norm(
        summed_buf[:, query_cols : query_cols + head_size], key_gain[...]
    )
    new_value_buf[...] = summed_buf[:, query_cols + head_size :].astype(jnp.bfloat16)
    own_queries[...] = query_buf[pl.ds(place * group, group)]
    own_keys[...] = new_key_buf[own_rows, :]
    own_values[...] = new_value_buf[own_rows, :]

    scale = head_size ** (-0.5) * LOG2E
    column = lax.broadcasted_iota(jnp.int32, (heads, block_len), 1)
    lane = lax.broadcasted_iota(jnp.int32, (heads * nodes, head_size), 1)
    for step in order:
        for copy in cache_copies(step):
            copy.wait()
        stats = jnp.zeros((heads * nodes, head_size), jnp.float32)
        for item in range(group):
            seq = partner_of(place, step) * group + item
            raw = lax.dot_general(
                query_buf[seq], key_buf[step, item], NT, preferred_element_type=jnp.float32
            )
            valid = lengths[seq] - place * block_len
            decay = jnp.where(column < valid, cache_logcum[seq] * LOG2E, MASKED)
            decay = jnp.concatenate(
                [
                    jnp.broadcast_to(decay[head : head + 1, :], (nodes, block_len))
                    for head in range(heads)
                ],
                axis=0,
            )
            scores = raw * scale - decay
            top = jnp.max(scores, axis=1, keepdims=True).astype(jnp.bfloat16).astype(jnp.float32)
            weights = jnp.exp2(scores - top)
            total = jnp.sum(weights, axis=1, keepdims=True)
            values = jnp.dot(
                weights.astype(jnp.bfloat16),
                value_buf[step, item],
                preferred_element_type=jnp.float32,
            )
            first = item * heads * nodes
            packed[step][first : first + heads * nodes, :] = values.astype(jnp.bfloat16)
            stats = jnp.where(lane == 2 * item, top, stats)
            stats = jnp.where(lane == 2 * item + 1, total, stats)
        packed[step][group * heads * nodes :, :] = stats.astype(jnp.bfloat16)


def tree_kernel(
    kv_size,
    tp_size,
    accepted,
    forget_bias,
    parents,
    queries,
    keys_new,
    values_new,
    gates,
    pending_keys,
    pending_values,
    pending_logcum,
    tree_acc,
    tree_stats,
    key_buf,
    value_buf,
):
    place = lax.axis_index("kv")
    side = lax.axis_index("tp")
    group, head_rows, head_size = queries.shape
    most_taken, heads, seq_count = pending_logcum.shape
    nodes = head_rows // heads
    tree_rows = group * nodes
    size = 2 * tree_rows
    exact = dict(preferred_element_type=jnp.float32, precision=HIGHEST)

    key_buf[...] = jnp.zeros_like(key_buf)
    value_buf[...] = jnp.zeros_like(value_buf)
    key_buf[:tree_rows, :] = keys_new[...].astype(jnp.float32)
    value_buf[:tree_rows, :] = values_new[...].astype(jnp.float32)
    for item in range(group):
        rows = slice(tree_rows + item * most_taken, tree_rows + (item + 1) * most_taken)
        key_buf[rows, :] = pending_keys[place * group + item].astype(jnp.float32)
        value_buf[rows, :] = pending_values[place * group + item].astype(jnp.float32)

    lane = lax.broadcasted_iota(jnp.int32, (1, size), 1)
    in_tree = jnp.where(lane < tree_rows, 1, 0)
    tree_item, tree_node = lane // nodes, lane % nodes
    late = lane - tree_rows
    late_item, late_node = late // most_taken, late % most_taken
    in_late = jnp.where((late >= 0) & (late_item < group), 1, 0)
    item_of = jnp.where(late < 0, tree_item, late_item)
    taken = jnp.zeros((1, size), jnp.int32)
    for item in range(group):
        taken = jnp.where(item_of == item, accepted[place * group + item], taken)

    node_row = lax.broadcasted_iota(jnp.int32, (parents.shape[1], size), 0)
    spread = jnp.dot(
        parents[...].astype(jnp.float32),
        (node_row == tree_node).astype(jnp.float32),
        preferred_element_type=jnp.float32,
    )
    seq_row = lax.broadcasted_iota(jnp.int32, (seq_count, size), 0)
    own_seq = (seq_row == place * group + jnp.where(in_tree + in_late > 0, item_of, -seq_count)).astype(
        jnp.float32
    )
    parent = jnp.sum(own_seq * spread, axis=0, keepdims=True).astype(jnp.int32)
    square_row = lax.broadcasted_iota(jnp.int32, (size, size), 0)
    square_lane = lax.broadcasted_iota(jnp.int32, (size, size), 1)
    identity = (square_row == square_lane).astype(jnp.float32)
    linked = square_row == jnp.where((late < 0) & (parent >= 0), tree_item * nodes + parent, -1)
    reach = linked.astype(jnp.float32) + identity
    for doubling in range((nodes - 1).bit_length()):
        low = reach.astype(jnp.bfloat16)
        reach = jnp.minimum(jnp.dot(low, low, preferred_element_type=jnp.float32), 1.0)
    low = reach.astype(jnp.bfloat16)
    ancestry = lax.dot_general(
        identity.astype(jnp.bfloat16), low, NT, preferred_element_type=jnp.float32
    )

    raw_gates = gates[:heads, :]
    for other in range(1, tp_size):
        raw_gates = jnp.where(side == other, gates[other * heads : (other + 1) * heads, :], raw_gates)
    bias = jnp.concatenate(
        [jnp.full((1, tree_rows), forget_bias[side * heads + head]) for head in range(heads)], axis=0
    )
    logits = raw_gates + bias
    log_gates = jnp.minimum(logits, 0.0) - jnp.log1p(jnp.exp(-jnp.abs(logits)))
    decay = jnp.dot(log_gates, reach[:tree_rows, :], **exact)
    decay = decay * in_tree.astype(jnp.float32)
    picked = jnp.where(late < 0, taken - 1, late_node)
    for node in range(most_taken):
        chosen = own_seq * (picked == node).astype(jnp.float32)
        decay = decay + jnp.dot(pending_logcum[node], chosen, **exact)
    decay = decay * LOG2E

    head_decay = jnp.concatenate(
        [jnp.broadcast_to(decay[head : head + 1, :], (nodes, size)) for head in range(heads)], axis=0
    )
    row = lax.broadcasted_iota(jnp.int32, (head_rows, size), 0)
    keys = key_buf[...].astype(jnp.bfloat16)
    values = value_buf[...].astype(jnp.bfloat16)
    scale = head_size ** (-0.5) * LOG2E
    for item in range(group):
        raw = lax.dot_general(queries[item], keys, NT, preferred_element_type=jnp.float32)
        own_decay = jnp.sum(
            jnp.where(lane == item * nodes + row % nodes, head_decay, 0.0), axis=1, keepdims=True
        )
        scores = raw * scale + own_decay - head_decay
        reached = jnp.concatenate([ancestry[item * nodes : (item + 1) * nodes, :]] * heads, axis=0)
        offered = jnp.where(late_item == item, jnp.where(late_node < taken, in_late, 0), 0)
        seen = reached * in_tree.astype(jnp.float32) + offered.astype(jnp.float32) > 0.5
        top = jnp.max(jnp.where(seen, scores, NEG_LARGE), axis=1, keepdims=True)
        weights = jnp.where(seen, jnp.exp2(scores - top), 0.0)
        total = jnp.sum(weights, axis=1, keepdims=True)
        rows = slice(item * head_rows, (item + 1) * head_rows)
        tree_acc[rows, :] = jnp.dot(
            weights.astype(jnp.bfloat16), values, preferred_element_type=jnp.float32
        )
        stat_lane = lax.broadcasted_iota(jnp.int32, (head_rows, head_size), 1)
        tree_stats[rows, :] = jnp.where(
            stat_lane == 0, top, jnp.where(stat_lane == 1, total, own_decay)
        )


def merge_kernel(kv_size, tree_acc, tree_stats, *refs):
    packed, chunk = refs[:kv_size], refs[kv_size]
    head_size = tree_acc.shape[1]
    heads = chunk.shape[1] // head_size
    nodes_all = chunk.shape[0]
    group = (packed[0].shape[0] * heads) // (nodes_all * heads) - 1
    group = tree_acc.shape[0] // (packed[0].shape[0] - tree_acc.shape[0])
    head_rows = tree_acc.shape[0] // group
    nodes = head_rows // heads
    stats = [p[group * head_rows :, :].astype(jnp.float32) for p in packed]
    for item in range(group):
        rows = slice(item * head_rows, (item + 1) * head_rows)
        own_decay = tree_stats[rows, 2:3]
        tree_top = tree_stats[rows, 0:1]
        tops = [s[:, 2 * item : 2 * item + 1] + own_decay for s in stats]
        top = functools.reduce(jnp.maximum, tops, tree_top)
        factor = jnp.exp2(tree_top - top)
        bottom = tree_stats[rows, 1:2] * factor
        upper = tree_acc[rows, :] * factor
        for source in range(kv_size):
            factor = jnp.exp2(tops[source] - top)
            bottom = bottom + stats[source][:, 2 * item + 1 : 2 * item + 2] * factor
            upper = upper + packed[source][rows, :].astype(jnp.float32) * factor
        attended = (upper / bottom).astype(jnp.bfloat16)
        for head in range(heads):
            chunk[item * nodes : (item + 1) * nodes, head * head_size : (head + 1) * head_size] = (
                attended[head * nodes : (head + 1) * nodes, :]
            )


def project_kernel(kv_size, weight, *refs):
    chunks, (kept, sent) = refs[:kv_size], refs[kv_size:]
    place = lax.axis_index("kv")
    side = lax.axis_index("tp")
    rows = chunks[0].shape[0]
    cols = kept.shape[1]
    for out, half in ((sent, 1 - side), (kept, side)):
        part = weight[:, pl.ds(pl.multiple_of(half * cols, cols), cols)]
        for step in range(kv_size):
            first = pl.multiple_of(partner_of(place, step) * rows, rows)
            out[pl.ds(first, rows), :] = jnp.dot(
                chunks[step][...], part, preferred_element_type=jnp.float32
            ).astype(jnp.bfloat16)


def exchange(array, axis, size, step):
    return lax.ppermute(array, axis, [(i, i ^ step) for i in range(size)])


def fast_shards(
    tokens,
    norm_gain,
    query_weight,
    key_weight,
    value_weight,
    forget_weight,
    forget_bias,
    query_gain,
    key_gain,
    output_weight,
    cache_keys,
    cache_values,
    cache_logcum,
    pending_keys,
    pending_values,
    pending_logcum,
    lengths,
    accepted,
    parents,
):
    kv_size, tp_size = lax.axis_size("kv"), lax.axis_size("tp")
    seq_count, nodes, width = tokens.shape
    query_cols = query_weight.shape[1]
    head_size = query_gain.shape[0]
    heads = query_cols // head_size
    block_len = cache_keys.shape[1]
    most_taken = pending_keys.shape[1]
    rows = seq_count * nodes
    group = seq_count // kv_size
    head_rows = heads * nodes
    bf16, f32 = jnp.bfloat16, jnp.float32
    hbm = pl.BlockSpec(memory_space=pltpu.HBM)
    vmem = pl.BlockSpec(memory_space=pltpu.VMEM)
    smem = pl.BlockSpec(memory_space=pltpu.SMEM)
    row_parts, depth_parts = 4, 4

    results = pl.pallas_call(
        functools.partial(attend_kernel, kv_size),
        name="attend",
        out_shape=[in_vmem(((group + 1) * head_rows, head_size), bf16) for _ in range(kv_size)]
        + [
            in_vmem((group, head_rows, head_size), bf16),
            in_vmem((group * nodes, head_size), bf16),
            in_vmem((group * nodes, head_size), bf16),
            in_vmem((forget_weight.shape[1], group * nodes), f32),
        ],
        in_specs=[smem, hbm, vmem, hbm, hbm, hbm, vmem, vmem, vmem, hbm, hbm, vmem],
        out_specs=[vmem] * (kv_size + 4),
        scratch_shapes=[
            pltpu.VMEM((rows, width), bf16),
            pltpu.VMEM((width, query_cols + 2 * head_size), bf16),
            pltpu.VMEM((kv_size, group, block_len, head_size), bf16),
            pltpu.VMEM((kv_size, group, block_len, head_size), bf16),
            pltpu.VMEM((rows, width), bf16),
            pltpu.VMEM((rows, query_cols + 2 * head_size), f32),
            pltpu.VMEM((seq_count, head_rows, head_size), bf16),
            pltpu.VMEM((rows, head_size), bf16),
            pltpu.VMEM((rows, head_size), bf16),
            pltpu.SemaphoreType.DMA((row_parts,)),
            pltpu.SemaphoreType.DMA((depth_parts, 3)),
            pltpu.SemaphoreType.DMA((kv_size, 2)),
        ],
    )(
        lengths,
        tokens.reshape(rows, width),
        norm_gain.reshape(1, width),
        query_weight,
        key_weight,
        value_weight,
        forget_weight.T,
        query_gain.reshape(1, head_size),
        key_gain.reshape(1, head_size),
        cache_keys.reshape(seq_count, block_len, head_size),
        cache_values.reshape(seq_count, block_len, head_size),
        jnp.swapaxes(cache_logcum, 1, 2),
    )
    packed, (own_queries, own_keys, own_values, own_gates) = results[:kv_size], results[kv_size:]
    moved = {s: exchange(packed[s], "kv", kv_size, s) for s in range(kv_size - 1, 0, -1)}
    tree_acc, tree_stats = pl.pallas_call(
        functools.partial(tree_kernel, kv_size, tp_size),
        name="tree",
        out_shape=[
            in_vmem((group * head_rows, head_size), f32),
            in_vmem((group * head_rows, head_size), f32),
        ],
        in_specs=[smem, smem] + [vmem] * 8,
        out_specs=[vmem, vmem],
        scratch_shapes=[pltpu.VMEM((2 * group * nodes, head_size), f32)] * 2,
        cost_estimate=pl.CostEstimate(flops=4_000_000_000, bytes_accessed=1_000_000, transcendentals=0),
    )(
        accepted,
        forget_bias,
        parents,
        held(own_queries),
        held(own_keys),
        held(own_values),
        held(own_gates),
        pending_keys.reshape(seq_count, most_taken, head_size),
        pending_values.reshape(seq_count, most_taken, head_size),
        jnp.transpose(pending_logcum, (1, 2, 0)),
    )
    chunk = pl.pallas_call(
        functools.partial(merge_kernel, kv_size),
        name="merge",
        out_shape=in_vmem((group * nodes, query_cols), bf16),
        in_specs=[vmem] * (kv_size + 2),
        out_specs=vmem,
    )(
        held(tree_acc),
        held(tree_stats),
        held(packed[0]),
        *[held(moved[s]) for s in range(1, kv_size)],
    )
    chunks = [chunk] + [exchange(chunk, "kv", kv_size, s) for s in range(1, kv_size)]
    cols = output_weight.shape[1] // tp_size
    kept, sent = pl.pallas_call(
        functools.partial(project_kernel, kv_size),
        name="project",
        out_shape=[in_vmem((rows, cols), bf16), in_vmem((rows, cols), bf16)],
        in_specs=[vmem] * (kv_size + 1),
        out_specs=[vmem, vmem],
    )(held(output_weight), *[held(c) for c in chunks])
    received = exchange(sent, "tp", tp_size, 1)
    summed = (kept.astype(f32) + received.astype(f32)).astype(bf16)
    return summed.reshape(seq_count, nodes, cols)


def fits_fast(mesh, shapes):
    kv_size = mesh.shape["kv"]
    seq_count = shapes["tokens"][0] // mesh.shape["dp"]
    one_key_head = shapes["cache_keys"][2] == mesh.shape["tp"]
    small = kv_size <= 4 and kv_size & (kv_size - 1) == 0
    return small and one_key_head and mesh.shape["tp"] == 2 and seq_count % kv_size == 0


def chosen_shards(mesh):
    def run(*args):
        shapes = {"tokens": args[0].shape, "cache_keys": args[10].shape}
        shapes["tokens"] = (shapes["tokens"][0] * mesh.shape["dp"],)
        shapes["cache_keys"] = (0, 0, shapes["cache_keys"][2] * mesh.shape["tp"])
        return (fast_shards if fits_fast(mesh, shapes) else shards)(*args)

    return run


def solution(mesh):
    placed = (
        P("dp", None, None),
        P(),
        P(None, "tp"),
        P(None, "tp"),
        P(None, "tp"),
        P(),
        P(),
        P(),
        P(),
        P("tp", "kv"),
        P("dp", "kv", "tp", None),
        P("dp", "kv", "tp", None),
        P("dp", "kv", "tp"),
        P("dp", None, "tp", None),
        P("dp", None, "tp", None),
        P("dp", None, "tp"),
        P("dp"),
        P("dp"),
        P("dp", None),
    )
    return jax.shard_map(
        chosen_shards(mesh), mesh=mesh, in_specs=placed, out_specs=P("dp", None, ("kv", "tp")), check_vma=False
    )
```

```python
import functools
import math

import jax
import jax.numpy as jnp
from jax import lax
from jax.experimental import pallas as pl
from jax.experimental.pallas import tpu as pltpu
from jax.sharding import PartitionSpec as P

EPSILON = 1e-06
NEG_LARGE = -1e30
HIGHEST = lax.Precision.HIGHEST


def joined(shard, axis, join):
    gathered = jax.tree.map(
        lambda a, kind: lax.all_gather(a.astype(kind), axis),
        shard,
        (jnp.bfloat16, jnp.bfloat16, jnp.bfloat16),
    )

    def take(source):
        return jax.tree.map(
            lambda a, own: lax.dynamic_index_in_dim(a, source, 0, False).astype(own.dtype),
            gathered,
            shard,
        )

    return lax.fori_loop(
        1, lax.axis_size(axis), lambda source, state: join(state, take(source)), take(0)
    )


def head_norm(vectors, gain_vec):
    return (
        vectors
        * lax.rsqrt(jnp.mean(vectors * vectors, axis=-1, keepdims=True) + EPSILON)
        * gain_vec
    )


def ancestors(parents):
    node_count = parents.shape[-1]
    indices = jnp.arange(node_count, dtype=jnp.int32)
    reachable = (parents[..., None] == indices).astype(jnp.float32) + jnp.eye(
        node_count, dtype=jnp.float32
    )
    for _ in range((node_count - 1).bit_length()):
        reachable = jnp.minimum(
            jnp.einsum("sij,sjk->sik", reachable, reachable, precision=HIGHEST), 1.0
        )
    return reachable


def join_blocks(earlier, later):
    larger = jnp.maximum(earlier[0], later[0])
    left_factor = jnp.exp(earlier[0] - larger)
    right_factor = jnp.exp(later[0] - larger)
    return (
        larger,
        earlier[1] * left_factor + later[1] * right_factor,
        earlier[2] * left_factor[..., None] + later[2] * right_factor[..., None],
    )


def to_rows(values):
    moved = jnp.swapaxes(values, 1, 2)
    return moved.reshape((moved.shape[0] * moved.shape[1],) + moved.shape[2:])


def finish_rows(cache_max, cache_sum, cache_acc, tree_max, tree_sum, tree_acc):
    overall = jnp.maximum(cache_max, tree_max)
    factor_cache = jnp.exp(cache_max - overall)
    factor_tree = jnp.exp(tree_max - overall)
    denominator = cache_sum * factor_cache + tree_sum * factor_tree
    numerator = cache_acc * factor_cache[..., None] + tree_acc * factor_tree[..., None]
    attended = (numerator / denominator[..., None]).astype(jnp.bfloat16)
    return attended.reshape(attended.shape[0], attended.shape[1] * attended.shape[2])


def shards(
    tokens,
    norm_gain,
    query_weight,
    key_weight,
    value_weight,
    forget_weight,
    forget_bias,
    query_gain,
    key_gain,
    output_weight,
    cache_keys,
    cache_values,
    cache_logcum,
    pending_keys,
    pending_values,
    pending_logcum,
    lengths,
    accepted,
    parents,
):
    seq_count, node_count, model_width = tokens.shape
    token_rows = seq_count * node_count
    head_size = query_gain.shape[0]
    query_cols = query_weight.shape[1]
    key_cols = key_weight.shape[1]
    local_heads = query_cols // head_size
    key_heads = key_cols // head_size
    sharing = local_heads // key_heads
    block_len = cache_keys.shape[1]
    most_taken = pending_keys.shape[1]
    scaling = head_size ** (-0.5)
    widened = tokens.reshape(token_rows, model_width).astype(jnp.float32)
    normed = (
        widened
        * lax.rsqrt(jnp.mean(widened * widened, axis=-1, keepdims=True) + EPSILON)
        * norm_gain
    ).astype(jnp.bfloat16)
    joined_weight = jnp.concatenate([query_weight, key_weight, value_weight], axis=1)
    summed = jnp.dot(normed, joined_weight, preferred_element_type=jnp.float32)
    query_part = head_norm(
        summed[:, :query_cols].reshape(token_rows, local_heads, head_size), query_gain
    )
    key_part = head_norm(
        summed[:, query_cols : query_cols + key_cols].reshape(token_rows, key_heads, head_size),
        key_gain,
    )
    queries = query_part.astype(jnp.bfloat16).reshape(
        seq_count, node_count, key_heads, sharing, head_size
    )
    keys_new = key_part.astype(jnp.bfloat16).reshape(seq_count, node_count, key_heads, head_size)
    values_new = (
        summed[:, query_cols + key_cols :]
        .astype(jnp.bfloat16)
        .reshape(seq_count, node_count, key_heads, head_size)
    )
    head_start = lax.axis_index("tp") * local_heads
    forget_cols = lax.dynamic_slice_in_dim(forget_weight, head_start, local_heads, 1)
    gate_bias = lax.dynamic_slice_in_dim(forget_bias, head_start, local_heads, 0)
    log_gates = jax.nn.log_sigmoid(
        jnp.dot(normed, forget_cols, preferred_element_type=jnp.float32) + gate_bias
    ).reshape(seq_count, node_count, local_heads)
    ancestry = ancestors(parents)
    choose = (jnp.arange(most_taken, dtype=jnp.int32)[None, :] == (accepted - 1)[:, None]).astype(
        jnp.float32
    )
    base_gate = jnp.einsum("sa,sah->sh", choose, pending_logcum, precision=HIGHEST)
    cumulative = base_gate[:, None, :] + jnp.einsum(
        "sij,sjh->sih", ancestry, log_gates, precision=HIGHEST
    )
    gate_rows = jnp.swapaxes(cumulative, 1, 2)
    token_place = lax.axis_index("kv") * block_len + jnp.arange(block_len, dtype=jnp.int32)
    offset = token_place[None, :] - lengths[:, None]
    inserted = (offset >= 0) & (offset < accepted[:, None])
    one_hot = (offset[..., None] == jnp.arange(most_taken, dtype=jnp.int32)) & inserted[..., None]
    hot_low = one_hot.astype(jnp.bfloat16)
    merged_keys = jnp.where(
        inserted[..., None, None],
        jnp.einsum(
            "sla,sakd->slkd", hot_low, pending_keys, preferred_element_type=jnp.float32
        ).astype(jnp.bfloat16),
        cache_keys,
    )
    merged_values = jnp.where(
        inserted[..., None, None],
        jnp.einsum(
            "sla,sakd->slkd", hot_low, pending_values, preferred_element_type=jnp.float32
        ).astype(jnp.bfloat16),
        cache_values,
    )
    log_cache = jnp.where(
        inserted[..., None],
        jnp.einsum("sla,sah->slh", one_hot.astype(jnp.float32), pending_logcum, precision=HIGHEST),
        cache_logcum,
    )
    usable = token_place[None, :] < (lengths + accepted)[:, None]
    raw_scores = jnp.einsum(
        "spkgd,slkd->skgpl", queries, merged_keys, preferred_element_type=jnp.float32
    )
    scores = (
        raw_scores.reshape(seq_count, local_heads, node_count, block_len) * scaling
        + gate_rows[..., None]
        - jnp.swapaxes(log_cache, 1, 2)[:, :, None, :]
    )
    visible = usable[:, None, None, :]
    block_max = jnp.max(jnp.where(visible, scores, NEG_LARGE), axis=-1)
    weights = jnp.where(visible, jnp.exp(scores - block_max[..., None]), 0.0)
    block_sum = jnp.sum(weights, axis=-1)
    block_acc = jnp.einsum(
        "skgpl,slkd->skgpd",
        weights.astype(jnp.bfloat16).reshape(seq_count, key_heads, sharing, node_count, block_len),
        merged_values,
        preferred_element_type=jnp.float32,
    )
    block_acc = block_acc.reshape(seq_count, local_heads, node_count, head_size)
    tree_raw = jnp.einsum(
        "spkgd,sjkd->skgpj", queries, keys_new, preferred_element_type=jnp.float32
    )
    tree_scores = (
        tree_raw.reshape(seq_count, local_heads, node_count, node_count) * scaling
        + gate_rows[..., :, None]
        - gate_rows[..., None, :]
    )
    tree_mask = ancestry[:, None] > 0.5
    tree_max = jnp.max(jnp.where(tree_mask, tree_scores, NEG_LARGE), axis=-1)
    tree_weights = jnp.where(tree_mask, jnp.exp(tree_scores - tree_max[..., None]), 0.0)
    tree_sum = jnp.sum(tree_weights, axis=-1)
    tree_acc = jnp.einsum(
        "skgpj,sjkd->skgpd",
        tree_weights.astype(jnp.bfloat16).reshape(
            seq_count, key_heads, sharing, node_count, node_count
        ),
        values_new,
        preferred_element_type=jnp.float32,
    )
    tree_acc = tree_acc.reshape(seq_count, local_heads, node_count, head_size)
    tree_max_rows = to_rows(tree_max)
    tree_sum_rows = to_rows(tree_sum)
    tree_acc_rows = to_rows(tree_acc)
    cache_max, cache_sum, cache_acc = joined((block_max, block_sum, block_acc), "kv", join_blocks)
    attended = finish_rows(
        to_rows(cache_max),
        to_rows(cache_sum),
        to_rows(cache_acc),
        tree_max_rows,
        tree_sum_rows,
        tree_acc_rows,
    )
    head_part = jnp.dot(attended, output_weight, preferred_element_type=jnp.float32)
    head_part = head_part.reshape(seq_count, node_count, output_weight.shape[1])
    return lax.psum_scatter(head_part.astype(jnp.bfloat16), "tp", scatter_dimension=2, tiled=True)


LOG2E = math.log2(math.e)
MASKED = 2.0**100
STAT_ROWS = 16
GRANT = 16 * 2**20
NT = (((1,), (1,)), ((), ()))


def in_vmem(shape, dtype):
    return pltpu.VMEM(shape, dtype)


def held(array):
    return pltpu.with_memory_space_constraint(array, pltpu.VMEM)


def partner_of(place, step):
    return jnp.bitwise_xor(place, step)


def tile_rows(rows, nodes):
    return jnp.concatenate(
        [jnp.broadcast_to(rows[i : i + 1, :], (nodes, rows.shape[1])) for i in range(rows.shape[0])],
        axis=0,
    )


def stacked(columns, head_rows, lanes):
    lane = lax.broadcasted_iota(jnp.int32, (head_rows, lanes), 1)
    stats = jnp.zeros((head_rows, lanes), jnp.float32)
    for place, column in enumerate(columns):
        stats = jnp.where(lane == place, column, stats)
    return stats.T


def partials(queries, keys, values, decays, nodes, packed, extra=None):
    head_rows, head_size = queries[0].shape
    scale = head_size ** (-0.5) * LOG2E
    group = len(queries)
    raw = [
        lax.dot_general(q, k, NT, preferred_element_type=jnp.float32)
        for q, k in zip(queries, keys, strict=True)
    ]
    scores = [r * scale - tile_rows(d, nodes) for r, d in zip(raw, decays, strict=True)]
    tops = [jnp.max(s, axis=1, keepdims=True) for s in scores]
    if extra is not None:
        tree_scores, tree_values = extra
        tops = [
            jnp.maximum(t, jnp.max(s, axis=1, keepdims=True))
            for t, s in zip(tops, tree_scores, strict=True)
        ]
    tops = [t.astype(jnp.bfloat16).astype(jnp.float32) for t in tops]
    weights = [jnp.exp2(s - t) for s, t in zip(scores, tops, strict=True)]
    totals = [jnp.sum(w, axis=1, keepdims=True) for w in weights]
    sums = [
        jnp.dot(w.astype(jnp.bfloat16), v, preferred_element_type=jnp.float32)
        for w, v in zip(weights, values, strict=True)
    ]
    if extra is not None:
        weights = [jnp.exp2(s - t) for s, t in zip(tree_scores, tops, strict=True)]
        totals = [
            t + jnp.sum(w, axis=1, keepdims=True) for t, w in zip(totals, weights, strict=True)
        ]
        sums = [
            s + jnp.dot(w.astype(jnp.bfloat16), tree_values, preferred_element_type=jnp.float32)
            for s, w in zip(sums, weights, strict=True)
        ]
    for item in range(group):
        first = item * head_rows
        packed[first : first + head_rows, :] = sums[item].astype(jnp.bfloat16)
    high = [t.astype(jnp.bfloat16).astype(jnp.float32) for t in totals]
    low = [t - h for t, h in zip(totals, high, strict=True)]
    stats = stacked(tops + high + low, head_rows, head_size)
    packed[group * head_rows :, :head_rows] = stats[:STAT_ROWS, :].astype(jnp.bfloat16)
    packed[group * head_rows :, head_rows:] = jnp.zeros(
        (STAT_ROWS, head_size - head_rows), jnp.bfloat16
    )


def first_kernel(
    kv_size,
    lengths,
    tokens,
    norm_gain,
    query_weight,
    key_weight,
    value_weight,
    query_gain,
    key_gain,
    cache_keys,
    cache_values,
    cache_logcum,
    packed,
    normed,
    queries,
    new_keys,
    new_values,
    key_buf,
    value_buf,
    decay_buf,
    length_buf,
    token_buf,
    gain_buf,
    query_gain_buf,
    key_gain_buf,
    query_weight_buf,
    key_weight_buf,
    value_weight_buf,
    logcum_buf,
    summed_buf,
    small_sem,
    token_sem,
    weight_sem,
    cache_sem,
):
    place = lax.axis_index("kv")
    rows, width = tokens.shape
    query_cols = query_weight.shape[1]
    head_size = key_weight.shape[1]
    heads = query_cols // head_size
    seq_count, block_len = cache_keys.shape[0], cache_keys.shape[1]
    nodes = rows // seq_count
    group = seq_count // kv_size
    row_parts = token_sem.shape[0]
    row_part = rows // row_parts
    depth_parts = weight_sem.shape[0]
    depth = width // depth_parts

    def spans(source, target, sem, count, parts):
        part = count // parts
        return [
            pltpu.make_async_copy(
                source.at[pl.ds(i * part, part)], target.at[pl.ds(i * part, part)], sem(i)
            )
            for i in range(parts)
        ]

    small = [
        pltpu.make_async_copy(source, target, small_sem.at[i])
        for i, (source, target) in enumerate(
            (
                (lengths, length_buf),
                (norm_gain, gain_buf),
                (query_gain, query_gain_buf),
                (key_gain, key_gain_buf),
                (cache_logcum, logcum_buf),
            )
        )
    ]
    token_copies = spans(tokens, token_buf, lambda i: token_sem.at[i], rows, row_parts)
    weight_copies = list(
        zip(
            spans(query_weight, query_weight_buf, lambda i: weight_sem.at[i, 0], width, depth_parts),
            spans(key_weight, key_weight_buf, lambda i: weight_sem.at[i, 1], width, depth_parts),
            spans(value_weight, value_weight_buf, lambda i: weight_sem.at[i, 2], width, depth_parts),
            strict=True,
        )
    )
    cache_copies = []
    for step in range(kv_size):
        span = pl.ds(partner_of(place, step) * group, group)
        cache_copies.append(
            (
                pltpu.make_async_copy(cache_keys.at[span], key_buf.at[step], cache_sem.at[step, 0]),
                pltpu.make_async_copy(cache_values.at[span], value_buf.at[step], cache_sem.at[step, 1]),
            )
        )
    small[1].start()
    for copy in token_copies:
        copy.start()
    for copies in weight_copies:
        for copy in copies:
            copy.start()
    for i in (0, 2, 3, 4):
        small[i].start()
    for step in range(kv_size - 1, -1, -1):
        for copy in cache_copies[step]:
            copy.start()

    small[1].wait()
    gain = gain_buf[...]
    for part in range(row_parts):
        token_copies[part].wait()
        for first in range(part * row_part, (part + 1) * row_part, nodes):
            widened = token_buf[pl.ds(first, nodes), :].astype(jnp.float32)
            mean = jnp.mean(widened * widened, axis=1, keepdims=True)
            normed[pl.ds(first, nodes), :] = (
                widened * lax.rsqrt(mean + EPSILON) * gain
            ).astype(jnp.bfloat16)

    for part in range(depth_parts):
        for copy in weight_copies[part]:
            copy.wait()
        span = pl.ds(part * depth, depth)
        left = normed[:, span]
        both = jnp.concatenate([key_weight_buf[span, :], value_weight_buf[span, :]], axis=1)
        for target, right in (
            (pl.ds(0, query_cols), query_weight_buf[span, :]),
            (pl.ds(query_cols, 2 * head_size), both),
        ):
            product = jnp.dot(left, right, preferred_element_type=jnp.float32)
            if part == 0:
                summed_buf[:, target] = product
            else:
                summed_buf[:, target] += product
    for i in (0, 2, 3, 4):
        small[i].wait()

    column = lax.broadcasted_iota(jnp.int32, (heads, block_len), 1)
    for seq in range(seq_count):
        valid = length_buf[seq] - place * block_len
        decay_buf[seq] = jnp.where(column < valid, logcum_buf[seq] * LOG2E, MASKED)

    def head_norm(vectors, gain_vec):
        mean = jnp.mean(vectors * vectors, axis=1, keepdims=True)
        return (vectors * lax.rsqrt(mean + EPSILON) * gain_vec).astype(jnp.bfloat16)

    for head in range(heads):
        normal = head_norm(
            summed_buf[:, head * head_size : (head + 1) * head_size], query_gain_buf[...]
        )
        queries[:, head * nodes : (head + 1) * nodes, :] = normal.reshape(
            seq_count, nodes, head_size
        )
    new_keys[...] = head_norm(
        summed_buf[:, query_cols : query_cols + head_size], key_gain_buf[...]
    )
    new_values[...] = summed_buf[:, query_cols + head_size :].astype(jnp.bfloat16)
    for step in range(kv_size - 1, -1, -1):
        for copy in cache_copies[step]:
            copy.wait()
    step_partials(kv_size - 1, place, nodes, queries, key_buf, value_buf, decay_buf, packed)


def step_partials(step, place, nodes, queries, keys, values, decays, packed, extra=None):
    group = keys.shape[1]
    seqs = [partner_of(place, step) * group + item for item in range(group)]
    partials(
        [queries[seq] for seq in seqs],
        [keys[step, item] for item in range(group)],
        [values[step, item] for item in range(group)],
        [decays[seq] for seq in seqs],
        nodes,
        packed,
        extra,
    )


def next_kernel(step, queries, keys, values, decays, packed):
    nodes = queries.shape[1] // decays.shape[1]
    step_partials(step, lax.axis_index("kv"), nodes, queries, keys, values, decays, packed)


def own_kernel(
    tp_size,
    accepted,
    forget_bias,
    parents,
    forget_rows,
    pending_keys,
    pending_values,
    pending_logcum,
    normed,
    queries,
    new_keys,
    new_values,
    keys,
    values,
    decays,
    packed,
    terms,
    key_buf,
    value_buf,
):
    place = lax.axis_index("kv")
    side = lax.axis_index("tp")
    group = keys.shape[1]
    head_rows, head_size = queries.shape[1], queries.shape[2]
    most_taken, heads, seq_count = pending_logcum.shape
    nodes = head_rows // heads
    tree_rows = group * nodes
    size = 2 * tree_rows
    exact = dict(preferred_element_type=jnp.float32, precision=HIGHEST)
    own_rows = pl.ds(pl.multiple_of(place * tree_rows, tree_rows), tree_rows)

    key_buf[...] = jnp.zeros_like(key_buf)
    value_buf[...] = jnp.zeros_like(value_buf)
    key_buf[:tree_rows, :] = new_keys[own_rows, :].astype(jnp.float32)
    value_buf[:tree_rows, :] = new_values[own_rows, :].astype(jnp.float32)
    for item in range(group):
        rows = slice(tree_rows + item * most_taken, tree_rows + (item + 1) * most_taken)
        key_buf[rows, :] = pending_keys[place * group + item].astype(jnp.float32)
        value_buf[rows, :] = pending_values[place * group + item].astype(jnp.float32)
    gates = lax.dot_general(
        forget_rows[...], normed[own_rows, :], NT, preferred_element_type=jnp.float32
    )

    lane = lax.broadcasted_iota(jnp.int32, (1, size), 1)
    in_tree = jnp.where(lane < tree_rows, 1, 0)
    tree_item, tree_node = lane // nodes, lane % nodes
    late = lane - tree_rows
    late_item, late_node = late // most_taken, late % most_taken
    in_late = jnp.where((late >= 0) & (late_item < group), 1, 0)
    item_of = jnp.where(late < 0, tree_item, late_item)
    taken = jnp.zeros((1, size), jnp.int32)
    for item in range(group):
        taken = jnp.where(item_of == item, accepted[place * group + item], taken)

    node_row = lax.broadcasted_iota(jnp.int32, (parents.shape[1], size), 0)
    spread = jnp.dot(
        parents[...].astype(jnp.float32),
        (node_row == tree_node).astype(jnp.float32),
        preferred_element_type=jnp.float32,
    )
    seq_row = lax.broadcasted_iota(jnp.int32, (seq_count, size), 0)
    own_seq = (seq_row == place * group + jnp.where(in_tree + in_late > 0, item_of, -seq_count)).astype(
        jnp.float32
    )
    parent = jnp.sum(own_seq * spread, axis=0, keepdims=True).astype(jnp.int32)
    square_row = lax.broadcasted_iota(jnp.int32, (size, size), 0)
    square_lane = lax.broadcasted_iota(jnp.int32, (size, size), 1)
    identity = (square_row == square_lane).astype(jnp.float32)
    linked = square_row == jnp.where((late < 0) & (parent >= 0), tree_item * nodes + parent, -1)
    reach = linked.astype(jnp.float32) + identity
    for _ in range((nodes - 1).bit_length()):
        low = reach.astype(jnp.bfloat16)
        reach = jnp.minimum(jnp.dot(low, low, preferred_element_type=jnp.float32), 1.0)
    low = reach.astype(jnp.bfloat16)
    ancestry = lax.dot_general(
        identity.astype(jnp.bfloat16), low, NT, preferred_element_type=jnp.float32
    )

    raw_gates = gates[:heads, :]
    for other in range(1, tp_size):
        raw_gates = jnp.where(side == other, gates[other * heads : (other + 1) * heads, :], raw_gates)
    bias = jnp.concatenate(
        [jnp.full((1, tree_rows), forget_bias[side * heads + head]) for head in range(heads)], axis=0
    )
    logits = raw_gates + bias
    log_gates = jnp.minimum(logits, 0.0) - jnp.log1p(jnp.exp(-jnp.abs(logits)))
    decay = jnp.dot(log_gates, reach[:tree_rows, :], **exact)
    decay = decay * in_tree.astype(jnp.float32)
    picked = jnp.where(late < 0, taken - 1, late_node)
    for node in range(most_taken):
        chosen = own_seq * (picked == node).astype(jnp.float32)
        decay = decay + jnp.dot(pending_logcum[node], chosen, **exact)
    decay = decay * LOG2E

    head_decay = tile_rows(decay, nodes)
    row = lax.broadcasted_iota(jnp.int32, (head_rows, size), 0)
    tree_keys = key_buf[...].astype(jnp.bfloat16)
    scale = head_size ** (-0.5) * LOG2E
    tree_scores, own_terms = [], []
    for item in range(group):
        raw = lax.dot_general(
            queries[place * group + item], tree_keys, NT, preferred_element_type=jnp.float32
        )
        own_terms.append(
            jnp.sum(
                jnp.where(lane == item * nodes + row % nodes, head_decay, 0.0),
                axis=1,
                keepdims=True,
            )
        )
        reached = jnp.concatenate([ancestry[item * nodes : (item + 1) * nodes, :]] * heads, axis=0)
        offered = jnp.where(late_item == item, jnp.where(late_node < taken, in_late, 0), 0)
        seen = reached * in_tree.astype(jnp.float32) + offered.astype(jnp.float32) > 0.5
        tree_scores.append(jnp.where(seen, raw * scale - head_decay, -MASKED))
    terms[...] = stacked(own_terms, head_rows, head_size)[: terms.shape[0], :]
    extra = (tree_scores, value_buf[...].astype(jnp.bfloat16))
    step_partials(0, place, nodes, queries, keys, values, decays, packed, extra)


def merge_kernel(kv_size, terms, *refs):
    packed, chunk = refs[:kv_size], refs[kv_size]
    head_size = packed[0].shape[1]
    heads = chunk.shape[1] // head_size
    head_rows = terms.shape[1]
    nodes = head_rows // heads
    group = chunk.shape[0] // nodes
    base = group * head_rows
    term = terms[:group, :]
    stats = [p[base:, :head_rows].astype(jnp.float32) for p in packed]
    tops = [s[:group] + term for s in stats]
    top = functools.reduce(jnp.maximum, tops)
    factors = [jnp.exp2(t - top) for t in tops]
    bottom = sum(
        (s[group : 2 * group] + s[2 * group : 3 * group]) * f
        for s, f in zip(stats, factors, strict=True)
    )
    factors = [f / bottom for f in factors]
    row = lax.broadcasted_iota(jnp.int32, (head_rows, head_rows), 0)
    lane = lax.broadcasted_iota(jnp.int32, (head_rows, head_rows), 1)
    for item in range(group):
        rows = slice(item * head_rows, (item + 1) * head_rows)
        attended = jnp.zeros((head_rows, head_size), jnp.float32)
        for source in range(kv_size):
            spread = jnp.where(row == lane, factors[source][item : item + 1, :], 0.0)
            high = spread.astype(jnp.bfloat16)
            low = (spread - high.astype(jnp.float32)).astype(jnp.bfloat16)
            held_rows = packed[source][rows, :]
            attended += jnp.dot(high, held_rows, preferred_element_type=jnp.float32)
            attended += jnp.dot(low, held_rows, preferred_element_type=jnp.float32)
        attended = attended.astype(jnp.bfloat16)
        for head in range(heads):
            chunk[item * nodes : (item + 1) * nodes, head * head_size : (head + 1) * head_size] = (
                attended[head * nodes : (head + 1) * nodes, :]
            )


def project_kernel(kv_size, weight, *refs):
    chunks, (kept, sent) = refs[:kv_size], refs[kv_size:]
    place = lax.axis_index("kv")
    side = lax.axis_index("tp")
    rows = chunks[0].shape[0]
    cols = kept.shape[1]
    for out, half in ((sent, 1 - side), (kept, side)):
        part = weight[:, pl.ds(pl.multiple_of(half * cols, cols), cols)]
        for step in range(kv_size):
            first = pl.multiple_of(partner_of(place, step) * rows, rows)
            out[pl.ds(first, rows), :] = jnp.dot(
                chunks[step][...], part, preferred_element_type=jnp.float32
            ).astype(jnp.bfloat16)


def exchange(array, axis, size, step):
    return lax.ppermute(array, axis, [(i, i ^ step) for i in range(size)])


def fast_shards(
    tokens,
    norm_gain,
    query_weight,
    key_weight,
    value_weight,
    forget_weight,
    forget_bias,
    query_gain,
    key_gain,
    output_weight,
    cache_keys,
    cache_values,
    cache_logcum,
    pending_keys,
    pending_values,
    pending_logcum,
    lengths,
    accepted,
    parents,
):
    kv_size, tp_size = lax.axis_size("kv"), lax.axis_size("tp")
    seq_count, nodes, width = tokens.shape
    query_cols = query_weight.shape[1]
    head_size = query_gain.shape[0]
    heads = query_cols // head_size
    block_len = cache_keys.shape[1]
    most_taken = pending_keys.shape[1]
    rows = seq_count * nodes
    group = seq_count // kv_size
    head_rows = heads * nodes
    bf16, f32 = jnp.bfloat16, jnp.float32
    hbm = pl.BlockSpec(memory_space=pltpu.HBM)
    vmem = pl.BlockSpec(memory_space=pltpu.VMEM)
    smem = pl.BlockSpec(memory_space=pltpu.SMEM)
    row_parts, depth_parts = 4, 4
    packed_shape = in_vmem((group * head_rows + STAT_ROWS, head_size), bf16)

    farthest, normed, queries, new_keys, new_values, keys, values, decays = pl.pallas_call(
        functools.partial(first_kernel, kv_size),
        compiler_params=pltpu.CompilerParams(vmem_limit_bytes=GRANT),
        name="first",
        out_shape=[
            packed_shape,
            in_vmem((rows, width), bf16),
            in_vmem((seq_count, head_rows, head_size), bf16),
            in_vmem((rows, head_size), bf16),
            in_vmem((rows, head_size), bf16),
            in_vmem((kv_size, group, block_len, head_size), bf16),
            in_vmem((kv_size, group, block_len, head_size), bf16),
            in_vmem((seq_count, heads, block_len), f32),
        ],
        in_specs=[hbm] * 11,
        out_specs=[vmem] * 8,
        scratch_shapes=[
            pltpu.SMEM((seq_count,), jnp.int32),
            pltpu.VMEM((rows, width), bf16),
            pltpu.VMEM((1, width), f32),
            pltpu.VMEM((1, head_size), f32),
            pltpu.VMEM((1, head_size), f32),
            pltpu.VMEM((width, query_cols), bf16),
            pltpu.VMEM((width, head_size), bf16),
            pltpu.VMEM((width, head_size), bf16),
            pltpu.VMEM((seq_count, heads, block_len), f32),
            pltpu.VMEM((rows, query_cols + 2 * head_size), f32),
            pltpu.SemaphoreType.DMA((5,)),
            pltpu.SemaphoreType.DMA((row_parts,)),
            pltpu.SemaphoreType.DMA((depth_parts, 3)),
            pltpu.SemaphoreType.DMA((kv_size, 2)),
        ],
    )(
        *[
            pltpu.with_memory_space_constraint(a, pltpu.HBM)
            for a in (
                lengths,
                tokens.reshape(rows, width),
                norm_gain.reshape(1, width),
                query_weight,
                key_weight,
                value_weight,
                query_gain.reshape(1, head_size),
                key_gain.reshape(1, head_size),
                cache_keys.reshape(seq_count, block_len, head_size),
                cache_values.reshape(seq_count, block_len, head_size),
                jnp.swapaxes(cache_logcum, 1, 2),
            )
        ]
    )
    shared = [held(a) for a in (queries, keys, values, decays)]
    packed = {kv_size - 1: farthest}
    for step in range(kv_size - 2, 0, -1):
        packed[step] = pl.pallas_call(
            functools.partial(next_kernel, step),
            compiler_params=pltpu.CompilerParams(vmem_limit_bytes=GRANT),
        out_shape=packed_shape,
            in_specs=[vmem] * 4,
            out_specs=vmem,
        )(*shared)
    moved = {}
    for step in range(kv_size - 1, 0, -1):
        moved[step] = exchange(packed[step], "kv", kv_size, step)
    own, terms = pl.pallas_call(
        functools.partial(own_kernel, tp_size),
        compiler_params=pltpu.CompilerParams(vmem_limit_bytes=GRANT),
        name="own",
        out_shape=[packed_shape, in_vmem((8, head_rows), f32)],
        in_specs=[smem, smem] + [vmem] * 12,
        out_specs=[vmem, vmem],
        scratch_shapes=[pltpu.VMEM((2 * group * nodes, head_size), f32)] * 2,
        cost_estimate=pl.CostEstimate(flops=4_000_000_000, bytes_accessed=1_000_000, transcendentals=0),
    )(
        accepted,
        forget_bias,
        parents,
        forget_weight.T,
        pending_keys.reshape(seq_count, most_taken, head_size),
        pending_values.reshape(seq_count, most_taken, head_size),
        jnp.transpose(pending_logcum, (1, 2, 0)),
        held(normed),
        shared[0],
        held(new_keys),
        held(new_values),
        *shared[1:],
    )
    chunk = pl.pallas_call(
        functools.partial(merge_kernel, kv_size),
        compiler_params=pltpu.CompilerParams(vmem_limit_bytes=GRANT),
        name="merge",
        out_shape=in_vmem((group * nodes, query_cols), bf16),
        in_specs=[vmem] * (kv_size + 1),
        out_specs=vmem,
    )(held(terms), held(own), *[held(moved[s]) for s in range(1, kv_size)])
    chunks = {0: chunk}
    for step in range(kv_size - 1, 0, -1):
        chunks[step] = exchange(chunk, "kv", kv_size, step)
    cols = output_weight.shape[1] // tp_size
    kept, sent = pl.pallas_call(
        functools.partial(project_kernel, kv_size),
        compiler_params=pltpu.CompilerParams(vmem_limit_bytes=GRANT),
        name="project",
        out_shape=[in_vmem((rows, cols), bf16), in_vmem((rows, cols), bf16)],
        in_specs=[vmem] * (kv_size + 1),
        out_specs=[vmem, vmem],
    )(held(output_weight), *[held(chunks[c]) for c in range(kv_size)])
    received = exchange(sent, "tp", tp_size, 1)
    summed = (kept.astype(f32) + received.astype(f32)).astype(bf16)
    return summed.reshape(seq_count, nodes, cols)


def fits_fast(mesh, shapes):
    kv_size = mesh.shape["kv"]
    seq_count = shapes["tokens"][0] // mesh.shape["dp"]
    one_key_head = shapes["cache_keys"][2] == mesh.shape["tp"]
    small = kv_size <= 4 and kv_size & (kv_size - 1) == 0
    return small and one_key_head and mesh.shape["tp"] == 2 and seq_count % kv_size == 0


def chosen_shards(mesh):
    def run(*args):
        shapes = {"tokens": args[0].shape, "cache_keys": args[10].shape}
        shapes["tokens"] = (shapes["tokens"][0] * mesh.shape["dp"],)
        shapes["cache_keys"] = (0, 0, shapes["cache_keys"][2] * mesh.shape["tp"])
        if not fits_fast(mesh, shapes):
            return shards(*args)
        return fast_shards(*args)

    return run


def solution(mesh):
    placed = (
        P("dp", None, None),
        P(),
        P(None, "tp"),
        P(None, "tp"),
        P(None, "tp"),
        P(),
        P(),
        P(),
        P(),
        P("tp", "kv"),
        P("dp", "kv", "tp", None),
        P("dp", "kv", "tp", None),
        P("dp", "kv", "tp"),
        P("dp", None, "tp", None),
        P("dp", None, "tp", None),
        P("dp", None, "tp"),
        P("dp"),
        P("dp"),
        P("dp", None),
    )
    return jax.shard_map(
        chosen_shards(mesh), mesh=mesh, in_specs=placed, out_specs=P("dp", None, ("kv", "tp")), check_vma=False
    )
```

```python
import functools
import math

import jax
import jax.numpy as jnp
from jax import lax
from jax.experimental import pallas as pl
from jax.experimental.pallas import tpu as pltpu
from jax.sharding import PartitionSpec as P

EPSILON = 1e-06
NEG_LARGE = -1e30
HIGHEST = lax.Precision.HIGHEST


def joined(shard, axis, join):
    gathered = jax.tree.map(
        lambda a, kind: lax.all_gather(a.astype(kind), axis),
        shard,
        (jnp.bfloat16, jnp.bfloat16, jnp.bfloat16),
    )

    def take(source):
        return jax.tree.map(
            lambda a, own: lax.dynamic_index_in_dim(a, source, 0, False).astype(own.dtype),
            gathered,
            shard,
        )

    return lax.fori_loop(
        1, lax.axis_size(axis), lambda source, state: join(state, take(source)), take(0)
    )


def head_norm(vectors, gain_vec):
    return (
        vectors
        * lax.rsqrt(jnp.mean(vectors * vectors, axis=-1, keepdims=True) + EPSILON)
        * gain_vec
    )


def ancestors(parents):
    node_count = parents.shape[-1]
    indices = jnp.arange(node_count, dtype=jnp.int32)
    reachable = (parents[..., None] == indices).astype(jnp.float32) + jnp.eye(
        node_count, dtype=jnp.float32
    )
    for _ in range((node_count - 1).bit_length()):
        reachable = jnp.minimum(
            jnp.einsum("sij,sjk->sik", reachable, reachable, precision=HIGHEST), 1.0
        )
    return reachable


def join_blocks(earlier, later):
    larger = jnp.maximum(earlier[0], later[0])
    left_factor = jnp.exp(earlier[0] - larger)
    right_factor = jnp.exp(later[0] - larger)
    return (
        larger,
        earlier[1] * left_factor + later[1] * right_factor,
        earlier[2] * left_factor[..., None] + later[2] * right_factor[..., None],
    )


def to_rows(values):
    moved = jnp.swapaxes(values, 1, 2)
    return moved.reshape((moved.shape[0] * moved.shape[1],) + moved.shape[2:])


def finish_rows(cache_max, cache_sum, cache_acc, tree_max, tree_sum, tree_acc):
    overall = jnp.maximum(cache_max, tree_max)
    factor_cache = jnp.exp(cache_max - overall)
    factor_tree = jnp.exp(tree_max - overall)
    denominator = cache_sum * factor_cache + tree_sum * factor_tree
    numerator = cache_acc * factor_cache[..., None] + tree_acc * factor_tree[..., None]
    attended = (numerator / denominator[..., None]).astype(jnp.bfloat16)
    return attended.reshape(attended.shape[0], attended.shape[1] * attended.shape[2])


def shards(
    tokens,
    norm_gain,
    query_weight,
    key_weight,
    value_weight,
    forget_weight,
    forget_bias,
    query_gain,
    key_gain,
    output_weight,
    cache_keys,
    cache_values,
    cache_logcum,
    pending_keys,
    pending_values,
    pending_logcum,
    lengths,
    accepted,
    parents,
):
    seq_count, node_count, model_width = tokens.shape
    token_rows = seq_count * node_count
    head_size = query_gain.shape[0]
    query_cols = query_weight.shape[1]
    key_cols = key_weight.shape[1]
    local_heads = query_cols // head_size
    key_heads = key_cols // head_size
    sharing = local_heads // key_heads
    block_len = cache_keys.shape[1]
    most_taken = pending_keys.shape[1]
    scaling = head_size ** (-0.5)
    widened = tokens.reshape(token_rows, model_width).astype(jnp.float32)
    normed = (
        widened
        * lax.rsqrt(jnp.mean(widened * widened, axis=-1, keepdims=True) + EPSILON)
        * norm_gain
    ).astype(jnp.bfloat16)
    joined_weight = jnp.concatenate([query_weight, key_weight, value_weight], axis=1)
    summed = jnp.dot(normed, joined_weight, preferred_element_type=jnp.float32)
    query_part = head_norm(
        summed[:, :query_cols].reshape(token_rows, local_heads, head_size), query_gain
    )
    key_part = head_norm(
        summed[:, query_cols : query_cols + key_cols].reshape(token_rows, key_heads, head_size),
        key_gain,
    )
    queries = query_part.astype(jnp.bfloat16).reshape(
        seq_count, node_count, key_heads, sharing, head_size
    )
    keys_new = key_part.astype(jnp.bfloat16).reshape(seq_count, node_count, key_heads, head_size)
    values_new = (
        summed[:, query_cols + key_cols :]
        .astype(jnp.bfloat16)
        .reshape(seq_count, node_count, key_heads, head_size)
    )
    head_start = lax.axis_index("tp") * local_heads
    forget_cols = lax.dynamic_slice_in_dim(forget_weight, head_start, local_heads, 1)
    gate_bias = lax.dynamic_slice_in_dim(forget_bias, head_start, local_heads, 0)
    log_gates = jax.nn.log_sigmoid(
        jnp.dot(normed, forget_cols, preferred_element_type=jnp.float32) + gate_bias
    ).reshape(seq_count, node_count, local_heads)
    ancestry = ancestors(parents)
    choose = (jnp.arange(most_taken, dtype=jnp.int32)[None, :] == (accepted - 1)[:, None]).astype(
        jnp.float32
    )
    base_gate = jnp.einsum("sa,sah->sh", choose, pending_logcum, precision=HIGHEST)
    cumulative = base_gate[:, None, :] + jnp.einsum(
        "sij,sjh->sih", ancestry, log_gates, precision=HIGHEST
    )
    gate_rows = jnp.swapaxes(cumulative, 1, 2)
    token_place = lax.axis_index("kv") * block_len + jnp.arange(block_len, dtype=jnp.int32)
    offset = token_place[None, :] - lengths[:, None]
    inserted = (offset >= 0) & (offset < accepted[:, None])
    one_hot = (offset[..., None] == jnp.arange(most_taken, dtype=jnp.int32)) & inserted[..., None]
    hot_low = one_hot.astype(jnp.bfloat16)
    merged_keys = jnp.where(
        inserted[..., None, None],
        jnp.einsum(
            "sla,sakd->slkd", hot_low, pending_keys, preferred_element_type=jnp.float32
        ).astype(jnp.bfloat16),
        cache_keys,
    )
    merged_values = jnp.where(
        inserted[..., None, None],
        jnp.einsum(
            "sla,sakd->slkd", hot_low, pending_values, preferred_element_type=jnp.float32
        ).astype(jnp.bfloat16),
        cache_values,
    )
    log_cache = jnp.where(
        inserted[..., None],
        jnp.einsum("sla,sah->slh", one_hot.astype(jnp.float32), pending_logcum, precision=HIGHEST),
        cache_logcum,
    )
    usable = token_place[None, :] < (lengths + accepted)[:, None]
    raw_scores = jnp.einsum(
        "spkgd,slkd->skgpl", queries, merged_keys, preferred_element_type=jnp.float32
    )
    scores = (
        raw_scores.reshape(seq_count, local_heads, node_count, block_len) * scaling
        + gate_rows[..., None]
        - jnp.swapaxes(log_cache, 1, 2)[:, :, None, :]
    )
    visible = usable[:, None, None, :]
    block_max = jnp.max(jnp.where(visible, scores, NEG_LARGE), axis=-1)
    weights = jnp.where(visible, jnp.exp(scores - block_max[..., None]), 0.0)
    block_sum = jnp.sum(weights, axis=-1)
    block_acc = jnp.einsum(
        "skgpl,slkd->skgpd",
        weights.astype(jnp.bfloat16).reshape(seq_count, key_heads, sharing, node_count, block_len),
        merged_values,
        preferred_element_type=jnp.float32,
    )
    block_acc = block_acc.reshape(seq_count, local_heads, node_count, head_size)
    tree_raw = jnp.einsum(
        "spkgd,sjkd->skgpj", queries, keys_new, preferred_element_type=jnp.float32
    )
    tree_scores = (
        tree_raw.reshape(seq_count, local_heads, node_count, node_count) * scaling
        + gate_rows[..., :, None]
        - gate_rows[..., None, :]
    )
    tree_mask = ancestry[:, None] > 0.5
    tree_max = jnp.max(jnp.where(tree_mask, tree_scores, NEG_LARGE), axis=-1)
    tree_weights = jnp.where(tree_mask, jnp.exp(tree_scores - tree_max[..., None]), 0.0)
    tree_sum = jnp.sum(tree_weights, axis=-1)
    tree_acc = jnp.einsum(
        "skgpj,sjkd->skgpd",
        tree_weights.astype(jnp.bfloat16).reshape(
            seq_count, key_heads, sharing, node_count, node_count
        ),
        values_new,
        preferred_element_type=jnp.float32,
    )
    tree_acc = tree_acc.reshape(seq_count, local_heads, node_count, head_size)
    tree_max_rows = to_rows(tree_max)
    tree_sum_rows = to_rows(tree_sum)
    tree_acc_rows = to_rows(tree_acc)
    cache_max, cache_sum, cache_acc = joined((block_max, block_sum, block_acc), "kv", join_blocks)
    attended = finish_rows(
        to_rows(cache_max),
        to_rows(cache_sum),
        to_rows(cache_acc),
        tree_max_rows,
        tree_sum_rows,
        tree_acc_rows,
    )
    head_part = jnp.dot(attended, output_weight, preferred_element_type=jnp.float32)
    head_part = head_part.reshape(seq_count, node_count, output_weight.shape[1])
    return lax.psum_scatter(head_part.astype(jnp.bfloat16), "tp", scatter_dimension=2, tiled=True)


LOG2E = math.log2(math.e)
MASKED = 2.0**100
STAT_ROWS = 16
GRANT = 16 * 2**20
NT = (((1,), (1,)), ((), ()))


def in_vmem(shape, dtype):
    return pltpu.VMEM(shape, dtype)


def held(array):
    return pltpu.with_memory_space_constraint(array, pltpu.VMEM)


def partner_of(place, step):
    return jnp.bitwise_xor(place, step)


def tile_rows(rows, nodes):
    return jnp.concatenate(
        [jnp.broadcast_to(rows[i : i + 1, :], (nodes, rows.shape[1])) for i in range(rows.shape[0])],
        axis=0,
    )


def stacked(columns, head_rows, lanes):
    lane = lax.broadcasted_iota(jnp.int32, (head_rows, lanes), 1)
    stats = jnp.zeros((head_rows, lanes), jnp.float32)
    for place, column in enumerate(columns):
        stats = jnp.where(lane == place, column, stats)
    return stats.T


def partials(queries, keys, values, decays, nodes, packed, extra=None):
    head_rows, head_size = queries[0].shape
    scale = head_size ** (-0.5) * LOG2E
    group = len(queries)
    raw = [
        lax.dot_general(q, k, NT, preferred_element_type=jnp.float32)
        for q, k in zip(queries, keys, strict=True)
    ]
    scores = [r * scale - tile_rows(d, nodes) for r, d in zip(raw, decays, strict=True)]
    tops = [jnp.max(s, axis=1, keepdims=True) for s in scores]
    if extra is not None:
        tree_scores, tree_values = extra
        tops = [
            jnp.maximum(t, jnp.max(s, axis=1, keepdims=True))
            for t, s in zip(tops, tree_scores, strict=True)
        ]
    tops = [t.astype(jnp.bfloat16).astype(jnp.float32) for t in tops]
    weights = [jnp.exp2(s - t) for s, t in zip(scores, tops, strict=True)]
    totals = [jnp.sum(w, axis=1, keepdims=True) for w in weights]
    sums = [
        jnp.dot(w.astype(jnp.bfloat16), v, preferred_element_type=jnp.float32)
        for w, v in zip(weights, values, strict=True)
    ]
    if extra is not None:
        weights = [jnp.exp2(s - t) for s, t in zip(tree_scores, tops, strict=True)]
        totals = [
            t + jnp.sum(w, axis=1, keepdims=True) for t, w in zip(totals, weights, strict=True)
        ]
        sums = [
            s + jnp.dot(w.astype(jnp.bfloat16), tree_values, preferred_element_type=jnp.float32)
            for s, w in zip(sums, weights, strict=True)
        ]
    for item in range(group):
        first = item * head_rows
        packed[first : first + head_rows, :] = sums[item].astype(jnp.bfloat16)
    high = [t.astype(jnp.bfloat16).astype(jnp.float32) for t in totals]
    low = [t - h for t, h in zip(totals, high, strict=True)]
    stats = stacked(tops + high + low, head_rows, head_size)
    packed[group * head_rows :, :head_rows] = stats[:STAT_ROWS, :].astype(jnp.bfloat16)
    packed[group * head_rows :, head_rows:] = jnp.zeros(
        (STAT_ROWS, head_size - head_rows), jnp.bfloat16
    )


def unit(vectors, gain_vec):
    mean = jnp.mean(vectors * vectors, axis=1, keepdims=True)
    return (vectors * lax.rsqrt(mean + EPSILON) * gain_vec).astype(jnp.bfloat16)


def first_kernel(
    kv_size,
    lengths,
    tokens,
    norm_gain,
    query_weight,
    query_gain,
    cache_keys,
    cache_values,
    cache_logcum,
    packed,
    normed,
    queries,
    key_buf,
    value_buf,
    decay_buf,
    length_buf,
    token_buf,
    gain_buf,
    query_gain_buf,
    query_weight_buf,
    logcum_buf,
    summed_buf,
    small_sem,
    token_sem,
    weight_sem,
    cache_sem,
):
    place = lax.axis_index("kv")
    rows, width = tokens.shape
    query_cols = query_weight.shape[1]
    head_size = query_gain.shape[1]
    heads = query_cols // head_size
    seq_count, block_len = cache_keys.shape[0], cache_keys.shape[1]
    nodes = rows // seq_count
    group = seq_count // kv_size
    row_parts = token_sem.shape[0]
    row_part = rows // row_parts
    depth_parts = weight_sem.shape[0]
    depth = width // depth_parts

    def spans(source, target, sem, count, parts):
        part = count // parts
        return [
            pltpu.make_async_copy(
                source.at[pl.ds(i * part, part)], target.at[pl.ds(i * part, part)], sem(i)
            )
            for i in range(parts)
        ]

    small = [
        pltpu.make_async_copy(source, target, small_sem.at[i])
        for i, (source, target) in enumerate(
            (
                (lengths, length_buf),
                (norm_gain, gain_buf),
                (query_gain, query_gain_buf),
                (cache_logcum, logcum_buf),
            )
        )
    ]
    token_copies = spans(tokens, token_buf, lambda i: token_sem.at[i], rows, row_parts)
    weight_copies = spans(query_weight, query_weight_buf, lambda i: weight_sem.at[i], width, depth_parts)
    cache_copies = []
    for step in range(kv_size):
        span = pl.ds(partner_of(place, step) * group, group)
        cache_copies.append(
            (
                pltpu.make_async_copy(cache_keys.at[span], key_buf.at[step], cache_sem.at[step, 0]),
                pltpu.make_async_copy(cache_values.at[span], value_buf.at[step], cache_sem.at[step, 1]),
            )
        )
    small[1].start()
    for copy in token_copies:
        copy.start()
    for copy in weight_copies:
        copy.start()
    for i in (0, 2, 3):
        small[i].start()
    for step in range(kv_size - 1, -1, -1):
        for copy in cache_copies[step]:
            copy.start()

    small[1].wait()
    gain = gain_buf[...]
    for part in range(row_parts):
        token_copies[part].wait()
        for first in range(part * row_part, (part + 1) * row_part, nodes):
            widened = token_buf[pl.ds(first, nodes), :].astype(jnp.float32)
            mean = jnp.mean(widened * widened, axis=1, keepdims=True)
            normed[pl.ds(first, nodes), :] = (
                widened * lax.rsqrt(mean + EPSILON) * gain
            ).astype(jnp.bfloat16)

    for part in range(depth_parts):
        weight_copies[part].wait()
        span = pl.ds(part * depth, depth)
        product = jnp.dot(
            normed[:, span], query_weight_buf[span, :], preferred_element_type=jnp.float32
        )
        if part == 0:
            summed_buf[...] = product
        else:
            summed_buf[...] += product
    for i in (0, 2, 3):
        small[i].wait()

    column = lax.broadcasted_iota(jnp.int32, (heads, block_len), 1)
    for seq in range(seq_count):
        valid = length_buf[seq] - place * block_len
        decay_buf[seq] = jnp.where(column < valid, logcum_buf[seq] * LOG2E, MASKED)

    for head in range(heads):
        normal = unit(
            summed_buf[:, head * head_size : (head + 1) * head_size], query_gain_buf[...]
        )
        queries[:, head * nodes : (head + 1) * nodes, :] = normal.reshape(
            seq_count, nodes, head_size
        )
    for step in range(kv_size - 1, -1, -1):
        for copy in cache_copies[step]:
            copy.wait()
    step_partials(kv_size - 1, place, nodes, queries, key_buf, value_buf, decay_buf, packed)


def step_partials(step, place, nodes, queries, keys, values, decays, packed, extra=None):
    group = keys.shape[1]
    seqs = [partner_of(place, step) * group + item for item in range(group)]
    partials(
        [queries[seq] for seq in seqs],
        [keys[step, item] for item in range(group)],
        [values[step, item] for item in range(group)],
        [decays[seq] for seq in seqs],
        nodes,
        packed,
        extra,
    )


def next_kernel(step, queries, keys, values, decays, packed):
    nodes = queries.shape[1] // decays.shape[1]
    step_partials(step, lax.axis_index("kv"), nodes, queries, keys, values, decays, packed)


def own_kernel(
    tp_size,
    accepted,
    forget_bias,
    parents,
    forget_rows,
    pending_keys,
    pending_values,
    pending_logcum,
    key_weight,
    value_weight,
    key_gain,
    normed,
    queries,
    keys,
    values,
    decays,
    packed,
    terms,
    key_buf,
    value_buf,
):
    place = lax.axis_index("kv")
    side = lax.axis_index("tp")
    group = keys.shape[1]
    head_rows, head_size = queries.shape[1], queries.shape[2]
    most_taken, heads, seq_count = pending_logcum.shape
    nodes = head_rows // heads
    tree_rows = group * nodes
    size = 2 * tree_rows
    exact = dict(preferred_element_type=jnp.float32, precision=HIGHEST)
    own_rows = pl.ds(pl.multiple_of(place * tree_rows, tree_rows), tree_rows)

    key_buf[...] = jnp.zeros_like(key_buf)
    value_buf[...] = jnp.zeros_like(value_buf)
    summed = jnp.dot(
        normed[own_rows, :],
        jnp.concatenate([key_weight[...], value_weight[...]], axis=1),
        preferred_element_type=jnp.float32,
    )
    key_buf[:tree_rows, :] = unit(summed[:, :head_size], key_gain[...]).astype(jnp.float32)
    value_buf[:tree_rows, :] = summed[:, head_size:]
    for item in range(group):
        rows = slice(tree_rows + item * most_taken, tree_rows + (item + 1) * most_taken)
        key_buf[rows, :] = pending_keys[place * group + item].astype(jnp.float32)
        value_buf[rows, :] = pending_values[place * group + item].astype(jnp.float32)
    gates = lax.dot_general(
        forget_rows[...], normed[own_rows, :], NT, preferred_element_type=jnp.float32
    )

    lane = lax.broadcasted_iota(jnp.int32, (1, size), 1)
    in_tree = jnp.where(lane < tree_rows, 1, 0)
    tree_item, tree_node = lane // nodes, lane % nodes
    late = lane - tree_rows
    late_item, late_node = late // most_taken, late % most_taken
    in_late = jnp.where((late >= 0) & (late_item < group), 1, 0)
    item_of = jnp.where(late < 0, tree_item, late_item)
    taken = jnp.zeros((1, size), jnp.int32)
    for item in range(group):
        taken = jnp.where(item_of == item, accepted[place * group + item], taken)

    node_row = lax.broadcasted_iota(jnp.int32, (parents.shape[1], size), 0)
    spread = jnp.dot(
        parents[...].astype(jnp.float32),
        (node_row == tree_node).astype(jnp.float32),
        preferred_element_type=jnp.float32,
    )
    seq_row = lax.broadcasted_iota(jnp.int32, (seq_count, size), 0)
    own_seq = (seq_row == place * group + jnp.where(in_tree + in_late > 0, item_of, -seq_count)).astype(
        jnp.float32
    )
    parent = jnp.sum(own_seq * spread, axis=0, keepdims=True).astype(jnp.int32)
    square_row = lax.broadcasted_iota(jnp.int32, (size, size), 0)
    square_lane = lax.broadcasted_iota(jnp.int32, (size, size), 1)
    identity = (square_row == square_lane).astype(jnp.float32)
    linked = square_row == jnp.where((late < 0) & (parent >= 0), tree_item * nodes + parent, -1)
    reach = linked.astype(jnp.float32) + identity
    for _ in range((nodes - 1).bit_length()):
        low = reach.astype(jnp.bfloat16)
        reach = jnp.minimum(jnp.dot(low, low, preferred_element_type=jnp.float32), 1.0)
    low = reach.astype(jnp.bfloat16)
    ancestry = lax.dot_general(
        identity.astype(jnp.bfloat16), low, NT, preferred_element_type=jnp.float32
    )

    raw_gates = gates[:heads, :]
    for other in range(1, tp_size):
        raw_gates = jnp.where(side == other, gates[other * heads : (other + 1) * heads, :], raw_gates)
    bias = jnp.concatenate(
        [jnp.full((1, tree_rows), forget_bias[side * heads + head]) for head in range(heads)], axis=0
    )
    logits = raw_gates + bias
    log_gates = jnp.minimum(logits, 0.0) - jnp.log1p(jnp.exp(-jnp.abs(logits)))
    decay = jnp.dot(log_gates, reach[:tree_rows, :], **exact)
    decay = decay * in_tree.astype(jnp.float32)
    picked = jnp.where(late < 0, taken - 1, late_node)
    for node in range(most_taken):
        chosen = own_seq * (picked == node).astype(jnp.float32)
        decay = decay + jnp.dot(pending_logcum[node], chosen, **exact)
    decay = decay * LOG2E

    head_decay = tile_rows(decay, nodes)
    row = lax.broadcasted_iota(jnp.int32, (head_rows, size), 0)
    tree_keys = key_buf[...].astype(jnp.bfloat16)
    scale = head_size ** (-0.5) * LOG2E
    tree_scores, own_terms = [], []
    for item in range(group):
        raw = lax.dot_general(
            queries[place * group + item], tree_keys, NT, preferred_element_type=jnp.float32
        )
        own_terms.append(
            jnp.sum(
                jnp.where(lane == item * nodes + row % nodes, head_decay, 0.0),
                axis=1,
                keepdims=True,
            )
        )
        reached = jnp.concatenate([ancestry[item * nodes : (item + 1) * nodes, :]] * heads, axis=0)
        offered = jnp.where(late_item == item, jnp.where(late_node < taken, in_late, 0), 0)
        seen = reached * in_tree.astype(jnp.float32) + offered.astype(jnp.float32) > 0.5
        tree_scores.append(jnp.where(seen, raw * scale - head_decay, -MASKED))
    terms[...] = stacked(own_terms, head_rows, head_size)[: terms.shape[0], :]
    extra = (tree_scores, value_buf[...].astype(jnp.bfloat16))
    step_partials(0, place, nodes, queries, keys, values, decays, packed, extra)


def merge_kernel(kv_size, terms, *refs):
    packed, chunk = refs[:kv_size], refs[kv_size]
    head_size = packed[0].shape[1]
    heads = chunk.shape[1] // head_size
    head_rows = terms.shape[1]
    nodes = head_rows // heads
    group = chunk.shape[0] // nodes
    base = group * head_rows
    term = terms[:group, :]
    stats = [p[base:, :head_rows].astype(jnp.float32) for p in packed]
    tops = [s[:group] + term for s in stats]
    top = functools.reduce(jnp.maximum, tops)
    factors = [jnp.exp2(t - top) for t in tops]
    bottom = sum(
        (s[group : 2 * group] + s[2 * group : 3 * group]) * f
        for s, f in zip(stats, factors, strict=True)
    )
    factors = [f / bottom for f in factors]
    row = lax.broadcasted_iota(jnp.int32, (head_rows, head_rows), 0)
    lane = lax.broadcasted_iota(jnp.int32, (head_rows, head_rows), 1)
    for item in range(group):
        rows = slice(item * head_rows, (item + 1) * head_rows)
        attended = jnp.zeros((head_rows, head_size), jnp.float32)
        for source in range(kv_size):
            spread = jnp.where(row == lane, factors[source][item : item + 1, :], 0.0)
            high = spread.astype(jnp.bfloat16)
            low = (spread - high.astype(jnp.float32)).astype(jnp.bfloat16)
            held_rows = packed[source][rows, :]
            attended += jnp.dot(high, held_rows, preferred_element_type=jnp.float32)
            attended += jnp.dot(low, held_rows, preferred_element_type=jnp.float32)
        attended = attended.astype(jnp.bfloat16)
        for head in range(heads):
            chunk[item * nodes : (item + 1) * nodes, head * head_size : (head + 1) * head_size] = (
                attended[head * nodes : (head + 1) * nodes, :]
            )


def project_kernel(kv_size, weight, *refs):
    chunks, (kept, sent) = refs[:kv_size], refs[kv_size:]
    place = lax.axis_index("kv")
    side = lax.axis_index("tp")
    rows = chunks[0].shape[0]
    cols = kept.shape[1]
    for out, half in ((sent, 1 - side), (kept, side)):
        part = weight[:, pl.ds(pl.multiple_of(half * cols, cols), cols)]
        for step in range(kv_size):
            first = pl.multiple_of(partner_of(place, step) * rows, rows)
            out[pl.ds(first, rows), :] = jnp.dot(
                chunks[step][...], part, preferred_element_type=jnp.float32
            ).astype(jnp.bfloat16)


def exchange(array, axis, size, step):
    return lax.ppermute(array, axis, [(i, i ^ step) for i in range(size)])


def fast_shards(
    tokens,
    norm_gain,
    query_weight,
    key_weight,
    value_weight,
    forget_weight,
    forget_bias,
    query_gain,
    key_gain,
    output_weight,
    cache_keys,
    cache_values,
    cache_logcum,
    pending_keys,
    pending_values,
    pending_logcum,
    lengths,
    accepted,
    parents,
):
    kv_size, tp_size = lax.axis_size("kv"), lax.axis_size("tp")
    seq_count, nodes, width = tokens.shape
    query_cols = query_weight.shape[1]
    head_size = query_gain.shape[0]
    heads = query_cols // head_size
    block_len = cache_keys.shape[1]
    most_taken = pending_keys.shape[1]
    rows = seq_count * nodes
    group = seq_count // kv_size
    head_rows = heads * nodes
    bf16, f32 = jnp.bfloat16, jnp.float32
    hbm = pl.BlockSpec(memory_space=pltpu.HBM)
    vmem = pl.BlockSpec(memory_space=pltpu.VMEM)
    smem = pl.BlockSpec(memory_space=pltpu.SMEM)
    row_parts, depth_parts = 4, 4
    packed_shape = in_vmem((group * head_rows + STAT_ROWS, head_size), bf16)

    farthest, normed, queries, keys, values, decays = pl.pallas_call(
        functools.partial(first_kernel, kv_size),
        compiler_params=pltpu.CompilerParams(vmem_limit_bytes=GRANT),
        name="first",
        out_shape=[
            packed_shape,
            in_vmem((rows, width), bf16),
            in_vmem((seq_count, head_rows, head_size), bf16),
            in_vmem((kv_size, group, block_len, head_size), bf16),
            in_vmem((kv_size, group, block_len, head_size), bf16),
            in_vmem((seq_count, heads, block_len), f32),
        ],
        in_specs=[hbm] * 8,
        out_specs=[vmem] * 6,
        scratch_shapes=[
            pltpu.SMEM((seq_count,), jnp.int32),
            pltpu.VMEM((rows, width), bf16),
            pltpu.VMEM((1, width), f32),
            pltpu.VMEM((1, head_size), f32),
            pltpu.VMEM((width, query_cols), bf16),
            pltpu.VMEM((seq_count, heads, block_len), f32),
            pltpu.VMEM((rows, query_cols), f32),
            pltpu.SemaphoreType.DMA((4,)),
            pltpu.SemaphoreType.DMA((row_parts,)),
            pltpu.SemaphoreType.DMA((depth_parts,)),
            pltpu.SemaphoreType.DMA((kv_size, 2)),
        ],
    )(
        *[
            pltpu.with_memory_space_constraint(a, pltpu.HBM)
            for a in (
                lengths,
                tokens.reshape(rows, width),
                norm_gain.reshape(1, width),
                query_weight,
                query_gain.reshape(1, head_size),
                cache_keys.reshape(seq_count, block_len, head_size),
                cache_values.reshape(seq_count, block_len, head_size),
                jnp.swapaxes(cache_logcum, 1, 2),
            )
        ]
    )
    shared = [held(a) for a in (queries, keys, values, decays)]
    packed = {kv_size - 1: farthest}
    for step in range(kv_size - 2, 0, -1):
        packed[step] = pl.pallas_call(
            functools.partial(next_kernel, step),
            compiler_params=pltpu.CompilerParams(vmem_limit_bytes=GRANT),
        out_shape=packed_shape,
            in_specs=[vmem] * 4,
            out_specs=vmem,
        )(*shared)
    moved = {}
    for step in range(kv_size - 1, 0, -1):
        moved[step] = exchange(packed[step], "kv", kv_size, step)
    own, terms = pl.pallas_call(
        functools.partial(own_kernel, tp_size),
        compiler_params=pltpu.CompilerParams(vmem_limit_bytes=GRANT),
        name="own",
        out_shape=[packed_shape, in_vmem((8, head_rows), f32)],
        in_specs=[smem, smem] + [vmem] * 13,
        out_specs=[vmem, vmem],
        scratch_shapes=[pltpu.VMEM((2 * group * nodes, head_size), f32)] * 2,
        cost_estimate=pl.CostEstimate(flops=4_000_000_000, bytes_accessed=1_000_000, transcendentals=0),
    )(
        accepted,
        forget_bias,
        parents,
        forget_weight.T,
        pending_keys.reshape(seq_count, most_taken, head_size),
        pending_values.reshape(seq_count, most_taken, head_size),
        jnp.transpose(pending_logcum, (1, 2, 0)),
        held(key_weight),
        held(value_weight),
        key_gain.reshape(1, head_size),
        held(normed),
        *shared,
    )
    chunk = pl.pallas_call(
        functools.partial(merge_kernel, kv_size),
        compiler_params=pltpu.CompilerParams(vmem_limit_bytes=GRANT),
        name="merge",
        out_shape=in_vmem((group * nodes, query_cols), bf16),
        in_specs=[vmem] * (kv_size + 1),
        out_specs=vmem,
    )(held(terms), held(own), *[held(moved[s]) for s in range(1, kv_size)])
    chunks = {0: chunk}
    for step in range(kv_size - 1, 0, -1):
        chunks[step] = exchange(chunk, "kv", kv_size, step)
    cols = output_weight.shape[1] // tp_size
    kept, sent = pl.pallas_call(
        functools.partial(project_kernel, kv_size),
        compiler_params=pltpu.CompilerParams(vmem_limit_bytes=GRANT),
        name="project",
        out_shape=[in_vmem((rows, cols), bf16), in_vmem((rows, cols), bf16)],
        in_specs=[vmem] * (kv_size + 1),
        out_specs=[vmem, vmem],
    )(held(output_weight), *[held(chunks[c]) for c in range(kv_size)])
    received = exchange(sent, "tp", tp_size, 1)
    summed = (kept.astype(f32) + received.astype(f32)).astype(bf16)
    return summed.reshape(seq_count, nodes, cols)


def fits_fast(mesh, shapes):
    kv_size = mesh.shape["kv"]
    seq_count = shapes["tokens"][0] // mesh.shape["dp"]
    one_key_head = shapes["cache_keys"][2] == mesh.shape["tp"]
    small = kv_size <= 4 and kv_size & (kv_size - 1) == 0
    return small and one_key_head and mesh.shape["tp"] == 2 and seq_count % kv_size == 0


def chosen_shards(mesh):
    def run(*args):
        shapes = {"tokens": args[0].shape, "cache_keys": args[10].shape}
        shapes["tokens"] = (shapes["tokens"][0] * mesh.shape["dp"],)
        shapes["cache_keys"] = (0, 0, shapes["cache_keys"][2] * mesh.shape["tp"])
        if not fits_fast(mesh, shapes):
            return shards(*args)
        return fast_shards(*args)

    return run


def solution(mesh):
    placed = (
        P("dp", None, None),
        P(),
        P(None, "tp"),
        P(None, "tp"),
        P(None, "tp"),
        P(),
        P(),
        P(),
        P(),
        P("tp", "kv"),
        P("dp", "kv", "tp", None),
        P("dp", "kv", "tp", None),
        P("dp", "kv", "tp"),
        P("dp", None, "tp", None),
        P("dp", None, "tp", None),
        P("dp", None, "tp"),
        P("dp"),
        P("dp"),
        P("dp", None),
    )
    return jax.shard_map(
        chosen_shards(mesh), mesh=mesh, in_specs=placed, out_specs=P("dp", None, ("kv", "tp")), check_vma=False
    )
```

```python
import functools
import math

import jax
import jax.numpy as jnp
from jax import lax
from jax.experimental import pallas as pl
from jax.experimental.pallas import tpu as pltpu
from jax.sharding import PartitionSpec as P

EPSILON = 1e-06
NEG_LARGE = -1e30
HIGHEST = lax.Precision.HIGHEST


def joined(shard, axis, join):
    gathered = jax.tree.map(
        lambda a, kind: lax.all_gather(a.astype(kind), axis),
        shard,
        (jnp.bfloat16, jnp.bfloat16, jnp.bfloat16),
    )

    def take(source):
        return jax.tree.map(
            lambda a, own: lax.dynamic_index_in_dim(a, source, 0, False).astype(own.dtype),
            gathered,
            shard,
        )

    return lax.fori_loop(
        1, lax.axis_size(axis), lambda source, state: join(state, take(source)), take(0)
    )


def head_norm(vectors, gain_vec):
    return (
        vectors
        * lax.rsqrt(jnp.mean(vectors * vectors, axis=-1, keepdims=True) + EPSILON)
        * gain_vec
    )


def ancestors(parents):
    node_count = parents.shape[-1]
    indices = jnp.arange(node_count, dtype=jnp.int32)
    reachable = (parents[..., None] == indices).astype(jnp.float32) + jnp.eye(
        node_count, dtype=jnp.float32
    )
    for _ in range((node_count - 1).bit_length()):
        reachable = jnp.minimum(
            jnp.einsum("sij,sjk->sik", reachable, reachable, precision=HIGHEST), 1.0
        )
    return reachable


def join_blocks(earlier, later):
    larger = jnp.maximum(earlier[0], later[0])
    left_factor = jnp.exp(earlier[0] - larger)
    right_factor = jnp.exp(later[0] - larger)
    return (
        larger,
        earlier[1] * left_factor + later[1] * right_factor,
        earlier[2] * left_factor[..., None] + later[2] * right_factor[..., None],
    )


def to_rows(values):
    moved = jnp.swapaxes(values, 1, 2)
    return moved.reshape((moved.shape[0] * moved.shape[1],) + moved.shape[2:])


def finish_rows(cache_max, cache_sum, cache_acc, tree_max, tree_sum, tree_acc):
    overall = jnp.maximum(cache_max, tree_max)
    factor_cache = jnp.exp(cache_max - overall)
    factor_tree = jnp.exp(tree_max - overall)
    denominator = cache_sum * factor_cache + tree_sum * factor_tree
    numerator = cache_acc * factor_cache[..., None] + tree_acc * factor_tree[..., None]
    attended = (numerator / denominator[..., None]).astype(jnp.bfloat16)
    return attended.reshape(attended.shape[0], attended.shape[1] * attended.shape[2])


def shards(
    tokens,
    norm_gain,
    query_weight,
    key_weight,
    value_weight,
    forget_weight,
    forget_bias,
    query_gain,
    key_gain,
    output_weight,
    cache_keys,
    cache_values,
    cache_logcum,
    pending_keys,
    pending_values,
    pending_logcum,
    lengths,
    accepted,
    parents,
):
    seq_count, node_count, model_width = tokens.shape
    token_rows = seq_count * node_count
    head_size = query_gain.shape[0]
    query_cols = query_weight.shape[1]
    key_cols = key_weight.shape[1]
    local_heads = query_cols // head_size
    key_heads = key_cols // head_size
    sharing = local_heads // key_heads
    block_len = cache_keys.shape[1]
    most_taken = pending_keys.shape[1]
    scaling = head_size ** (-0.5)
    widened = tokens.reshape(token_rows, model_width).astype(jnp.float32)
    normed = (
        widened
        * lax.rsqrt(jnp.mean(widened * widened, axis=-1, keepdims=True) + EPSILON)
        * norm_gain
    ).astype(jnp.bfloat16)
    joined_weight = jnp.concatenate([query_weight, key_weight, value_weight], axis=1)
    summed = jnp.dot(normed, joined_weight, preferred_element_type=jnp.float32)
    query_part = head_norm(
        summed[:, :query_cols].reshape(token_rows, local_heads, head_size), query_gain
    )
    key_part = head_norm(
        summed[:, query_cols : query_cols + key_cols].reshape(token_rows, key_heads, head_size),
        key_gain,
    )
    queries = query_part.astype(jnp.bfloat16).reshape(
        seq_count, node_count, key_heads, sharing, head_size
    )
    keys_new = key_part.astype(jnp.bfloat16).reshape(seq_count, node_count, key_heads, head_size)
    values_new = (
        summed[:, query_cols + key_cols :]
        .astype(jnp.bfloat16)
        .reshape(seq_count, node_count, key_heads, head_size)
    )
    head_start = lax.axis_index("tp") * local_heads
    forget_cols = lax.dynamic_slice_in_dim(forget_weight, head_start, local_heads, 1)
    gate_bias = lax.dynamic_slice_in_dim(forget_bias, head_start, local_heads, 0)
    log_gates = jax.nn.log_sigmoid(
        jnp.dot(normed, forget_cols, preferred_element_type=jnp.float32) + gate_bias
    ).reshape(seq_count, node_count, local_heads)
    ancestry = ancestors(parents)
    choose = (jnp.arange(most_taken, dtype=jnp.int32)[None, :] == (accepted - 1)[:, None]).astype(
        jnp.float32
    )
    base_gate = jnp.einsum("sa,sah->sh", choose, pending_logcum, precision=HIGHEST)
    cumulative = base_gate[:, None, :] + jnp.einsum(
        "sij,sjh->sih", ancestry, log_gates, precision=HIGHEST
    )
    gate_rows = jnp.swapaxes(cumulative, 1, 2)
    token_place = lax.axis_index("kv") * block_len + jnp.arange(block_len, dtype=jnp.int32)
    offset = token_place[None, :] - lengths[:, None]
    inserted = (offset >= 0) & (offset < accepted[:, None])
    one_hot = (offset[..., None] == jnp.arange(most_taken, dtype=jnp.int32)) & inserted[..., None]
    hot_low = one_hot.astype(jnp.bfloat16)
    merged_keys = jnp.where(
        inserted[..., None, None],
        jnp.einsum(
            "sla,sakd->slkd", hot_low, pending_keys, preferred_element_type=jnp.float32
        ).astype(jnp.bfloat16),
        cache_keys,
    )
    merged_values = jnp.where(
        inserted[..., None, None],
        jnp.einsum(
            "sla,sakd->slkd", hot_low, pending_values, preferred_element_type=jnp.float32
        ).astype(jnp.bfloat16),
        cache_values,
    )
    log_cache = jnp.where(
        inserted[..., None],
        jnp.einsum("sla,sah->slh", one_hot.astype(jnp.float32), pending_logcum, precision=HIGHEST),
        cache_logcum,
    )
    usable = token_place[None, :] < (lengths + accepted)[:, None]
    raw_scores = jnp.einsum(
        "spkgd,slkd->skgpl", queries, merged_keys, preferred_element_type=jnp.float32
    )
    scores = (
        raw_scores.reshape(seq_count, local_heads, node_count, block_len) * scaling
        + gate_rows[..., None]
        - jnp.swapaxes(log_cache, 1, 2)[:, :, None, :]
    )
    visible = usable[:, None, None, :]
    block_max = jnp.max(jnp.where(visible, scores, NEG_LARGE), axis=-1)
    weights = jnp.where(visible, jnp.exp(scores - block_max[..., None]), 0.0)
    block_sum = jnp.sum(weights, axis=-1)
    block_acc = jnp.einsum(
        "skgpl,slkd->skgpd",
        weights.astype(jnp.bfloat16).reshape(seq_count, key_heads, sharing, node_count, block_len),
        merged_values,
        preferred_element_type=jnp.float32,
    )
    block_acc = block_acc.reshape(seq_count, local_heads, node_count, head_size)
    tree_raw = jnp.einsum(
        "spkgd,sjkd->skgpj", queries, keys_new, preferred_element_type=jnp.float32
    )
    tree_scores = (
        tree_raw.reshape(seq_count, local_heads, node_count, node_count) * scaling
        + gate_rows[..., :, None]
        - gate_rows[..., None, :]
    )
    tree_mask = ancestry[:, None] > 0.5
    tree_max = jnp.max(jnp.where(tree_mask, tree_scores, NEG_LARGE), axis=-1)
    tree_weights = jnp.where(tree_mask, jnp.exp(tree_scores - tree_max[..., None]), 0.0)
    tree_sum = jnp.sum(tree_weights, axis=-1)
    tree_acc = jnp.einsum(
        "skgpj,sjkd->skgpd",
        tree_weights.astype(jnp.bfloat16).reshape(
            seq_count, key_heads, sharing, node_count, node_count
        ),
        values_new,
        preferred_element_type=jnp.float32,
    )
    tree_acc = tree_acc.reshape(seq_count, local_heads, node_count, head_size)
    tree_max_rows = to_rows(tree_max)
    tree_sum_rows = to_rows(tree_sum)
    tree_acc_rows = to_rows(tree_acc)
    cache_max, cache_sum, cache_acc = joined((block_max, block_sum, block_acc), "kv", join_blocks)
    attended = finish_rows(
        to_rows(cache_max),
        to_rows(cache_sum),
        to_rows(cache_acc),
        tree_max_rows,
        tree_sum_rows,
        tree_acc_rows,
    )
    head_part = jnp.dot(attended, output_weight, preferred_element_type=jnp.float32)
    head_part = head_part.reshape(seq_count, node_count, output_weight.shape[1])
    return lax.psum_scatter(head_part.astype(jnp.bfloat16), "tp", scatter_dimension=2, tiled=True)


LOG2E = math.log2(math.e)
MASKED = 2.0**100
STAT_ROWS = 16
GRANT = 16 * 2**20
GO_ORDER = (2, 3, 1)
BACK_ORDER = (3, 2, 1)
NT = (((1,), (1,)), ((), ()))


def in_vmem(shape, dtype):
    return pltpu.VMEM(shape, dtype)


def held(array):
    return pltpu.with_memory_space_constraint(array, pltpu.VMEM)


def partner_of(place, step):
    return jnp.bitwise_xor(place, step)


def tile_rows(rows, nodes):
    return jnp.concatenate(
        [jnp.broadcast_to(rows[i : i + 1, :], (nodes, rows.shape[1])) for i in range(rows.shape[0])],
        axis=0,
    )


def stacked(columns, head_rows, lanes):
    lane = lax.broadcasted_iota(jnp.int32, (head_rows, lanes), 1)
    stats = jnp.zeros((head_rows, lanes), jnp.float32)
    for place, column in enumerate(columns):
        stats = jnp.where(lane == place, column, stats)
    return stats.T


def partials(queries, keys, values, decays, nodes, packed, extra=None):
    head_rows, head_size = queries[0].shape
    scale = head_size ** (-0.5) * LOG2E
    group = len(queries)
    raw = [
        lax.dot_general(q, k, NT, preferred_element_type=jnp.float32)
        for q, k in zip(queries, keys, strict=True)
    ]
    scores = [r * scale - tile_rows(d, nodes) for r, d in zip(raw, decays, strict=True)]
    tops = [jnp.max(s, axis=1, keepdims=True) for s in scores]
    if extra is not None:
        tree_scores, tree_values = extra
        tops = [
            jnp.maximum(t, jnp.max(s, axis=1, keepdims=True))
            for t, s in zip(tops, tree_scores, strict=True)
        ]
    tops = [t.astype(jnp.bfloat16).astype(jnp.float32) for t in tops]
    weights = [jnp.exp2(s - t) for s, t in zip(scores, tops, strict=True)]
    totals = [jnp.sum(w, axis=1, keepdims=True) for w in weights]
    sums = [
        jnp.dot(w.astype(jnp.bfloat16), v, preferred_element_type=jnp.float32)
        for w, v in zip(weights, values, strict=True)
    ]
    if extra is not None:
        weights = [jnp.exp2(s - t) for s, t in zip(tree_scores, tops, strict=True)]
        totals = [
            t + jnp.sum(w, axis=1, keepdims=True) for t, w in zip(totals, weights, strict=True)
        ]
        sums = [
            s + jnp.dot(w.astype(jnp.bfloat16), tree_values, preferred_element_type=jnp.float32)
            for s, w in zip(sums, weights, strict=True)
        ]
    for item in range(group):
        first = item * head_rows
        packed[first : first + head_rows, :] = sums[item].astype(jnp.bfloat16)
    high = [t.astype(jnp.bfloat16).astype(jnp.float32) for t in totals]
    low = [t - h for t, h in zip(totals, high, strict=True)]
    stats = stacked(tops + high + low, head_rows, head_size)
    packed[group * head_rows :, :head_rows] = stats[:STAT_ROWS, :].astype(jnp.bfloat16)
    packed[group * head_rows :, head_rows:] = jnp.zeros(
        (STAT_ROWS, head_size - head_rows), jnp.bfloat16
    )


def unit(vectors, gain_vec):
    mean = jnp.mean(vectors * vectors, axis=1, keepdims=True)
    return (vectors * lax.rsqrt(mean + EPSILON) * gain_vec).astype(jnp.bfloat16)


def normalized(tokens, first, count, nodes, gain, normed):
    for start in range(0, count, nodes):
        widened = tokens[pl.ds(first + start, nodes), :].astype(jnp.float32)
        mean = jnp.mean(widened * widened, axis=1, keepdims=True)
        normed[pl.ds(start, nodes), :] = (
            widened * lax.rsqrt(mean + EPSILON) * gain
        ).astype(jnp.bfloat16)


def queries_of(summed, gain, nodes):
    head_size = gain.shape[1]
    heads = summed.shape[1] // head_size
    normal = [
        unit(summed[:, head * head_size : (head + 1) * head_size], gain) for head in range(heads)
    ]
    return [
        jnp.concatenate([n[first : first + nodes, :] for n in normal], axis=0)
        for first in range(0, summed.shape[0], nodes)
    ]


def first_kernel(
    kv_size,
    lengths,
    tokens,
    norm_gain,
    query_weight,
    query_gain,
    cache_keys,
    cache_values,
    cache_logcum,
    packed,
    second_queries,
    weight_buf,
    decay_buf,
    length_buf,
    token_buf,
    gain_buf,
    query_gain_buf,
    key_buf,
    value_buf,
    logcum_buf,
    normed,
    small_sem,
    weight_sem,
):
    place = lax.axis_index("kv")
    rows, width = tokens.shape
    seq_count, block_len = cache_keys.shape[0], cache_keys.shape[1]
    heads = cache_logcum.shape[1]
    nodes = rows // seq_count
    group = seq_count // kv_size
    count = group * nodes
    depth_parts = weight_sem.shape[0]
    depth = width // depth_parts
    owner = partner_of(place, GO_ORDER[0])

    second = partner_of(place, GO_ORDER[1])
    cache_span = pl.ds(owner * group, group)
    small = [
        pltpu.make_async_copy(source, target, small_sem.at[i])
        for i, (source, target) in enumerate(
            (
                (norm_gain, gain_buf),
                (tokens.at[pl.ds(pl.multiple_of(owner * count, count), count)], token_buf.at[0]),
                (tokens.at[pl.ds(pl.multiple_of(second * count, count), count)], token_buf.at[1]),
                (cache_logcum, logcum_buf),
                (lengths, length_buf),
                (query_gain, query_gain_buf),
                (cache_keys.at[cache_span], key_buf),
                (cache_values.at[cache_span], value_buf),
            )
        )
    ]
    weight_copies = [
        pltpu.make_async_copy(
            query_weight.at[pl.ds(i * depth, depth)],
            weight_buf.at[pl.ds(i * depth, depth)],
            weight_sem.at[i],
        )
        for i in range(depth_parts)
    ]
    for copy in small[:3] + weight_copies + small[3:]:
        copy.start()

    small[0].wait()
    for item in range(2):
        small[1 + item].wait()
        normalized(token_buf.at[item], 0, count, nodes, gain_buf[...], normed.at[pl.ds(item * count, count)])
    summed = None
    for part in range(depth_parts):
        weight_copies[part].wait()
        span = pl.ds(part * depth, depth)
        product = jnp.dot(normed[:, span], weight_buf[span, :], preferred_element_type=jnp.float32)
        summed = product if part == 0 else summed + product
    for copy in small[3:]:
        copy.wait()
    column = lax.broadcasted_iota(jnp.int32, (heads, block_len), 1)
    for seq in range(seq_count):
        valid = length_buf[seq] - place * block_len
        decay_buf[seq] = jnp.where(column < valid, logcum_buf[seq] * LOG2E, MASKED)
    queries = queries_of(summed, query_gain_buf[...], nodes)
    for item in range(group):
        second_queries[item] = queries[group + item]
    partials(
        queries[:group],
        [key_buf[item] for item in range(group)],
        [value_buf[item] for item in range(group)],
        [decay_buf[owner * group + item] for item in range(group)],
        nodes,
        packed,
    )


def step_partials(step, nodes, tokens, norm_gain, query_weight, query_gain, keys, values, decays, normed, packed, extra_of=None):
    place = lax.axis_index("kv")
    count = normed.shape[0]
    group = count // nodes
    owner = partner_of(place, step)
    normalized(tokens, pl.multiple_of(owner * count, count), count, nodes, norm_gain[...], normed)
    summed = jnp.dot(normed[...], query_weight[...], preferred_element_type=jnp.float32)
    queries = queries_of(summed, query_gain[...], nodes)
    seqs = [owner * group + item for item in range(group)]
    partials(
        queries,
        [keys[seq] for seq in seqs],
        [values[seq] for seq in seqs],
        [decays[seq] for seq in seqs],
        nodes,
        packed,
        None if extra_of is None else extra_of(queries),
    )


def next_kernel(step, nodes, *refs):
    *operands, packed, normed = refs
    step_partials(step, nodes, *operands, normed, packed)


def second_kernel(step, nodes, queries, keys, values, decays, packed):
    group = queries.shape[0]
    seqs = [partner_of(lax.axis_index("kv"), step) * group + item for item in range(group)]
    partials(
        [queries[item] for item in range(group)],
        [keys[seq] for seq in seqs],
        [values[seq] for seq in seqs],
        [decays[seq] for seq in seqs],
        nodes,
        packed,
    )


def own_kernel(
    tp_size,
    nodes,
    accepted,
    forget_bias,
    parents,
    forget_rows,
    pending_keys,
    pending_values,
    pending_logcum,
    key_weight,
    value_weight,
    key_gain,
    tokens,
    norm_gain,
    query_weight,
    query_gain,
    keys,
    values,
    decays,
    packed,
    terms,
    key_buf,
    value_buf,
    normed,
):
    extra_of = functools.partial(
        tree_block,
        tp_size,
        nodes,
        accepted,
        forget_bias,
        parents,
        forget_rows,
        pending_keys,
        pending_values,
        pending_logcum,
        key_weight,
        value_weight,
        key_gain,
        terms,
        key_buf,
        value_buf,
        normed,
    )
    step_partials(
        0,
        nodes,
        tokens,
        norm_gain,
        query_weight,
        query_gain,
        keys,
        values,
        decays,
        normed,
        packed,
        extra_of,
    )


def tree_block(
    tp_size,
    nodes,
    accepted,
    forget_bias,
    parents,
    forget_rows,
    pending_keys,
    pending_values,
    pending_logcum,
    key_weight,
    value_weight,
    key_gain,
    terms,
    key_buf,
    value_buf,
    normed,
    queries,
):
    place = lax.axis_index("kv")
    side = lax.axis_index("tp")
    tree_rows = normed.shape[0]
    group = tree_rows // nodes
    most_taken, heads, seq_count = pending_logcum.shape
    head_rows, head_size = heads * nodes, key_gain.shape[1]
    size = 2 * tree_rows
    exact = dict(preferred_element_type=jnp.float32, precision=HIGHEST)

    key_buf[...] = jnp.zeros_like(key_buf)
    value_buf[...] = jnp.zeros_like(value_buf)
    summed = jnp.dot(
        normed[...],
        jnp.concatenate([key_weight[...], value_weight[...]], axis=1),
        preferred_element_type=jnp.float32,
    )
    key_buf[:tree_rows, :] = unit(summed[:, :head_size], key_gain[...]).astype(jnp.float32)
    value_buf[:tree_rows, :] = summed[:, head_size:]
    for item in range(group):
        rows = slice(tree_rows + item * most_taken, tree_rows + (item + 1) * most_taken)
        key_buf[rows, :] = pending_keys[place * group + item].astype(jnp.float32)
        value_buf[rows, :] = pending_values[place * group + item].astype(jnp.float32)
    gates = lax.dot_general(
        forget_rows[...], normed[...], NT, preferred_element_type=jnp.float32
    )

    lane = lax.broadcasted_iota(jnp.int32, (1, size), 1)
    in_tree = jnp.where(lane < tree_rows, 1, 0)
    tree_item, tree_node = lane // nodes, lane % nodes
    late = lane - tree_rows
    late_item, late_node = late // most_taken, late % most_taken
    in_late = jnp.where((late >= 0) & (late_item < group), 1, 0)
    item_of = jnp.where(late < 0, tree_item, late_item)
    taken = jnp.zeros((1, size), jnp.int32)
    for item in range(group):
        taken = jnp.where(item_of == item, accepted[place * group + item], taken)

    node_row = lax.broadcasted_iota(jnp.int32, (parents.shape[1], size), 0)
    spread = jnp.dot(
        parents[...].astype(jnp.float32),
        (node_row == tree_node).astype(jnp.float32),
        preferred_element_type=jnp.float32,
    )
    seq_row = lax.broadcasted_iota(jnp.int32, (seq_count, size), 0)
    own_seq = (seq_row == place * group + jnp.where(in_tree + in_late > 0, item_of, -seq_count)).astype(
        jnp.float32
    )
    parent = jnp.sum(own_seq * spread, axis=0, keepdims=True).astype(jnp.int32)
    square_row = lax.broadcasted_iota(jnp.int32, (size, size), 0)
    square_lane = lax.broadcasted_iota(jnp.int32, (size, size), 1)
    identity = (square_row == square_lane).astype(jnp.float32)
    linked = square_row == jnp.where((late < 0) & (parent >= 0), tree_item * nodes + parent, -1)
    reach = linked.astype(jnp.float32) + identity
    for _ in range((nodes - 1).bit_length()):
        low = reach.astype(jnp.bfloat16)
        reach = jnp.minimum(jnp.dot(low, low, preferred_element_type=jnp.float32), 1.0)
    low = reach.astype(jnp.bfloat16)
    ancestry = lax.dot_general(
        identity.astype(jnp.bfloat16), low, NT, preferred_element_type=jnp.float32
    )

    raw_gates = gates[:heads, :]
    for other in range(1, tp_size):
        raw_gates = jnp.where(side == other, gates[other * heads : (other + 1) * heads, :], raw_gates)
    bias = jnp.concatenate(
        [jnp.full((1, tree_rows), forget_bias[side * heads + head]) for head in range(heads)], axis=0
    )
    logits = raw_gates + bias
    log_gates = jnp.minimum(logits, 0.0) - jnp.log1p(jnp.exp(-jnp.abs(logits)))
    decay = jnp.dot(log_gates, reach[:tree_rows, :], **exact)
    decay = decay * in_tree.astype(jnp.float32)
    picked = jnp.where(late < 0, taken - 1, late_node)
    for node in range(most_taken):
        chosen = own_seq * (picked == node).astype(jnp.float32)
        decay = decay + jnp.dot(pending_logcum[node], chosen, **exact)
    decay = decay * LOG2E

    head_decay = tile_rows(decay, nodes)
    row = lax.broadcasted_iota(jnp.int32, (head_rows, size), 0)
    tree_keys = key_buf[...].astype(jnp.bfloat16)
    scale = head_size ** (-0.5) * LOG2E
    tree_scores, own_terms = [], []
    for item in range(group):
        raw = lax.dot_general(
            queries[item], tree_keys, NT, preferred_element_type=jnp.float32
        )
        own_terms.append(
            jnp.sum(
                jnp.where(lane == item * nodes + row % nodes, head_decay, 0.0),
                axis=1,
                keepdims=True,
            )
        )
        reached = jnp.concatenate([ancestry[item * nodes : (item + 1) * nodes, :]] * heads, axis=0)
        offered = jnp.where(late_item == item, jnp.where(late_node < taken, in_late, 0), 0)
        seen = reached * in_tree.astype(jnp.float32) + offered.astype(jnp.float32) > 0.5
        tree_scores.append(jnp.where(seen, raw * scale - head_decay, -MASKED))
    terms[...] = stacked(own_terms, head_rows, head_size)[: terms.shape[0], :]
    return tree_scores, value_buf[...].astype(jnp.bfloat16)


def merge_kernel(kv_size, terms, *refs):
    packed, chunk = refs[:kv_size], refs[kv_size]
    head_size = packed[0].shape[1]
    heads = chunk.shape[1] // head_size
    head_rows = terms.shape[1]
    nodes = head_rows // heads
    group = chunk.shape[0] // nodes
    base = group * head_rows
    term = terms[:group, :]
    stats = [p[base:, :head_rows].astype(jnp.float32) for p in packed]
    tops = [s[:group] + term for s in stats]
    top = functools.reduce(jnp.maximum, tops)
    factors = [jnp.exp2(t - top) for t in tops]
    bottom = sum(
        (s[group : 2 * group] + s[2 * group : 3 * group]) * f
        for s, f in zip(stats, factors, strict=True)
    )
    factors = [f / bottom for f in factors]
    row = lax.broadcasted_iota(jnp.int32, (head_rows, head_rows), 0)
    lane = lax.broadcasted_iota(jnp.int32, (head_rows, head_rows), 1)
    for item in range(group):
        rows = slice(item * head_rows, (item + 1) * head_rows)
        attended = jnp.zeros((head_rows, head_size), jnp.float32)
        for source in range(kv_size):
            spread = jnp.where(row == lane, factors[source][item : item + 1, :], 0.0)
            high = spread.astype(jnp.bfloat16)
            low = (spread - high.astype(jnp.float32)).astype(jnp.bfloat16)
            held_rows = packed[source][rows, :]
            attended += jnp.dot(high, held_rows, preferred_element_type=jnp.float32)
            attended += jnp.dot(low, held_rows, preferred_element_type=jnp.float32)
        attended = attended.astype(jnp.bfloat16)
        for head in range(heads):
            chunk[item * nodes : (item + 1) * nodes, head * head_size : (head + 1) * head_size] = (
                attended[head * nodes : (head + 1) * nodes, :]
            )


def project_kernel(kv_size, weight, *refs):
    chunks, (kept, sent) = refs[:kv_size], refs[kv_size:]
    place = lax.axis_index("kv")
    side = lax.axis_index("tp")
    rows = chunks[0].shape[0]
    cols = kept.shape[1]
    for out, half in ((sent, 1 - side), (kept, side)):
        part = weight[:, pl.ds(pl.multiple_of(half * cols, cols), cols)]
        for step in range(kv_size):
            first = pl.multiple_of(partner_of(place, step) * rows, rows)
            out[pl.ds(first, rows), :] = jnp.dot(
                chunks[step][...], part, preferred_element_type=jnp.float32
            ).astype(jnp.bfloat16)


def exchange(array, axis, size, step):
    return lax.ppermute(array, axis, [(i, i ^ step) for i in range(size)])


def fast_shards(
    tokens,
    norm_gain,
    query_weight,
    key_weight,
    value_weight,
    forget_weight,
    forget_bias,
    query_gain,
    key_gain,
    output_weight,
    cache_keys,
    cache_values,
    cache_logcum,
    pending_keys,
    pending_values,
    pending_logcum,
    lengths,
    accepted,
    parents,
):
    kv_size, tp_size = lax.axis_size("kv"), lax.axis_size("tp")
    seq_count, nodes, width = tokens.shape
    query_cols = query_weight.shape[1]
    head_size = query_gain.shape[0]
    heads = query_cols // head_size
    block_len = cache_keys.shape[1]
    most_taken = pending_keys.shape[1]
    rows = seq_count * nodes
    group = seq_count // kv_size
    head_rows = heads * nodes
    bf16, f32 = jnp.bfloat16, jnp.float32
    hbm = pl.BlockSpec(memory_space=pltpu.HBM)
    vmem = pl.BlockSpec(memory_space=pltpu.VMEM)
    smem = pl.BlockSpec(memory_space=pltpu.SMEM)
    depth_parts = 4
    count = group * nodes
    packed_shape = in_vmem((group * head_rows + STAT_ROWS, head_size), bf16)
    token_matrix = tokens.reshape(rows, width)
    norm_row = norm_gain.reshape(1, width)
    query_row = query_gain.reshape(1, head_size)
    key_array = cache_keys.reshape(seq_count, block_len, head_size)
    value_array = cache_values.reshape(seq_count, block_len, head_size)

    farthest, second_queries, query_matrix, decays = pl.pallas_call(
        functools.partial(first_kernel, kv_size),
        compiler_params=pltpu.CompilerParams(vmem_limit_bytes=GRANT),
        name="first",
        out_shape=[
            packed_shape,
            in_vmem((group, head_rows, head_size), bf16),
            in_vmem((width, query_cols), bf16),
            in_vmem((seq_count, heads, block_len), f32),
        ],
        in_specs=[hbm] * 8,
        out_specs=[vmem] * 4,
        scratch_shapes=[
            pltpu.SMEM((seq_count,), jnp.int32),
            pltpu.VMEM((2, count, width), bf16),
            pltpu.VMEM((1, width), f32),
            pltpu.VMEM((1, head_size), f32),
            pltpu.VMEM((group, block_len, head_size), bf16),
            pltpu.VMEM((group, block_len, head_size), bf16),
            pltpu.VMEM((seq_count, heads, block_len), f32),
            pltpu.VMEM((2 * count, width), bf16),
            pltpu.SemaphoreType.DMA((8,)),
            pltpu.SemaphoreType.DMA((depth_parts,)),
        ],
    )(
        *[
            pltpu.with_memory_space_constraint(a, pltpu.HBM)
            for a in (
                lengths,
                token_matrix,
                norm_row,
                query_weight,
                query_row,
                key_array,
                value_array,
                jnp.swapaxes(cache_logcum, 1, 2),
            )
        ]
    )
    shared = [
        held(a)
        for a in (token_matrix, norm_row, query_matrix, query_row, key_array, value_array, decays)
    ]
    packed = {GO_ORDER[0]: farthest}
    packed[GO_ORDER[1]] = pl.pallas_call(
        functools.partial(second_kernel, GO_ORDER[1], nodes),
        compiler_params=pltpu.CompilerParams(vmem_limit_bytes=GRANT),
        name="second",
        out_shape=packed_shape,
        in_specs=[vmem] * 4,
        out_specs=vmem,
    )(held(second_queries), *shared[4:])
    for step in GO_ORDER[2:]:
        packed[step] = pl.pallas_call(
            functools.partial(next_kernel, step, nodes),
            compiler_params=pltpu.CompilerParams(vmem_limit_bytes=GRANT),
            out_shape=packed_shape,
            in_specs=[vmem] * 7,
            out_specs=vmem,
            scratch_shapes=[pltpu.VMEM((count, width), bf16)],
        )(*shared)
    moved = {}
    for step in GO_ORDER:
        moved[step] = exchange(packed[step], "kv", kv_size, step)
    own, terms = pl.pallas_call(
        functools.partial(own_kernel, tp_size, nodes),
        compiler_params=pltpu.CompilerParams(vmem_limit_bytes=GRANT),
        name="own",
        out_shape=[packed_shape, in_vmem((8, head_rows), f32)],
        in_specs=[smem, smem] + [vmem] * 15,
        out_specs=[vmem, vmem],
        scratch_shapes=[pltpu.VMEM((2 * count, head_size), f32)] * 2
        + [pltpu.VMEM((count, width), bf16)],
        cost_estimate=pl.CostEstimate(flops=4_000_000_000, bytes_accessed=1_000_000, transcendentals=0),
    )(
        accepted,
        forget_bias,
        parents,
        forget_weight.T,
        pending_keys.reshape(seq_count, most_taken, head_size),
        pending_values.reshape(seq_count, most_taken, head_size),
        jnp.transpose(pending_logcum, (1, 2, 0)),
        held(key_weight),
        held(value_weight),
        key_gain.reshape(1, head_size),
        *shared,
    )
    chunk = pl.pallas_call(
        functools.partial(merge_kernel, kv_size),
        compiler_params=pltpu.CompilerParams(vmem_limit_bytes=GRANT),
        name="merge",
        out_shape=in_vmem((group * nodes, query_cols), bf16),
        in_specs=[vmem] * (kv_size + 1),
        out_specs=vmem,
    )(held(terms), held(own), *[held(moved[s]) for s in range(1, kv_size)])
    chunks = {0: chunk}
    for step in BACK_ORDER:
        chunks[step] = exchange(chunk, "kv", kv_size, step)
    cols = output_weight.shape[1] // tp_size
    kept, sent = pl.pallas_call(
        functools.partial(project_kernel, kv_size),
        compiler_params=pltpu.CompilerParams(vmem_limit_bytes=GRANT),
        name="project",
        out_shape=[in_vmem((rows, cols), bf16), in_vmem((rows, cols), bf16)],
        in_specs=[vmem] * (kv_size + 1),
        out_specs=[vmem, vmem],
    )(held(output_weight), *[held(chunks[c]) for c in range(kv_size)])
    received = exchange(sent, "tp", tp_size, 1)
    summed = (kept.astype(f32) + received.astype(f32)).astype(bf16)
    return summed.reshape(seq_count, nodes, cols)


def fits_fast(mesh, shapes):
    kv_size = mesh.shape["kv"]
    seq_count = shapes["tokens"][0] // mesh.shape["dp"]
    one_key_head = shapes["cache_keys"][2] == mesh.shape["tp"]
    small = kv_size == 4
    return small and one_key_head and mesh.shape["tp"] == 2 and seq_count % kv_size == 0


def chosen_shards(mesh):
    def run(*args):
        shapes = {"tokens": args[0].shape, "cache_keys": args[10].shape}
        shapes["tokens"] = (shapes["tokens"][0] * mesh.shape["dp"],)
        shapes["cache_keys"] = (0, 0, shapes["cache_keys"][2] * mesh.shape["tp"])
        if not fits_fast(mesh, shapes):
            return shards(*args)
        return fast_shards(*args)

    return run


def solution(mesh):
    placed = (
        P("dp", None, None),
        P(),
        P(None, "tp"),
        P(None, "tp"),
        P(None, "tp"),
        P(),
        P(),
        P(),
        P(),
        P("tp", "kv"),
        P("dp", "kv", "tp", None),
        P("dp", "kv", "tp", None),
        P("dp", "kv", "tp"),
        P("dp", None, "tp", None),
        P("dp", None, "tp", None),
        P("dp", None, "tp"),
        P("dp"),
        P("dp"),
        P("dp", None),
    )
    return jax.shard_map(
        chosen_shards(mesh), mesh=mesh, in_specs=placed, out_specs=P("dp", None, ("kv", "tp")), check_vma=False
    )
```

```python
import functools
import math

import jax
import jax.numpy as jnp
from jax import lax
from jax.experimental import pallas as pl
from jax.experimental.pallas import tpu as pltpu
from jax.sharding import PartitionSpec as P

EPSILON = 1e-06
NEG_LARGE = -1e30
HIGHEST = lax.Precision.HIGHEST


def joined(shard, axis, join):
    gathered = jax.tree.map(
        lambda a, kind: lax.all_gather(a.astype(kind), axis),
        shard,
        (jnp.bfloat16, jnp.bfloat16, jnp.bfloat16),
    )

    def take(source):
        return jax.tree.map(
            lambda a, own: lax.dynamic_index_in_dim(a, source, 0, False).astype(own.dtype),
            gathered,
            shard,
        )

    return lax.fori_loop(
        1, lax.axis_size(axis), lambda source, state: join(state, take(source)), take(0)
    )


def head_norm(vectors, gain_vec):
    return (
        vectors
        * lax.rsqrt(jnp.mean(vectors * vectors, axis=-1, keepdims=True) + EPSILON)
        * gain_vec
    )


def ancestors(parents):
    node_count = parents.shape[-1]
    indices = jnp.arange(node_count, dtype=jnp.int32)
    reachable = (parents[..., None] == indices).astype(jnp.float32) + jnp.eye(
        node_count, dtype=jnp.float32
    )
    for _ in range((node_count - 1).bit_length()):
        reachable = jnp.minimum(
            jnp.einsum("sij,sjk->sik", reachable, reachable, precision=HIGHEST), 1.0
        )
    return reachable


def join_blocks(earlier, later):
    larger = jnp.maximum(earlier[0], later[0])
    left_factor = jnp.exp(earlier[0] - larger)
    right_factor = jnp.exp(later[0] - larger)
    return (
        larger,
        earlier[1] * left_factor + later[1] * right_factor,
        earlier[2] * left_factor[..., None] + later[2] * right_factor[..., None],
    )


def to_rows(values):
    moved = jnp.swapaxes(values, 1, 2)
    return moved.reshape((moved.shape[0] * moved.shape[1],) + moved.shape[2:])


def finish_rows(cache_max, cache_sum, cache_acc, tree_max, tree_sum, tree_acc):
    overall = jnp.maximum(cache_max, tree_max)
    factor_cache = jnp.exp(cache_max - overall)
    factor_tree = jnp.exp(tree_max - overall)
    denominator = cache_sum * factor_cache + tree_sum * factor_tree
    numerator = cache_acc * factor_cache[..., None] + tree_acc * factor_tree[..., None]
    attended = (numerator / denominator[..., None]).astype(jnp.bfloat16)
    return attended.reshape(attended.shape[0], attended.shape[1] * attended.shape[2])


def shards(
    tokens,
    norm_gain,
    query_weight,
    key_weight,
    value_weight,
    forget_weight,
    forget_bias,
    query_gain,
    key_gain,
    output_weight,
    cache_keys,
    cache_values,
    cache_logcum,
    pending_keys,
    pending_values,
    pending_logcum,
    lengths,
    accepted,
    parents,
):
    seq_count, node_count, model_width = tokens.shape
    token_rows = seq_count * node_count
    head_size = query_gain.shape[0]
    query_cols = query_weight.shape[1]
    key_cols = key_weight.shape[1]
    local_heads = query_cols // head_size
    key_heads = key_cols // head_size
    sharing = local_heads // key_heads
    block_len = cache_keys.shape[1]
    most_taken = pending_keys.shape[1]
    scaling = head_size ** (-0.5)
    widened = tokens.reshape(token_rows, model_width).astype(jnp.float32)
    normed = (
        widened
        * lax.rsqrt(jnp.mean(widened * widened, axis=-1, keepdims=True) + EPSILON)
        * norm_gain
    ).astype(jnp.bfloat16)
    joined_weight = jnp.concatenate([query_weight, key_weight, value_weight], axis=1)
    summed = jnp.dot(normed, joined_weight, preferred_element_type=jnp.float32)
    query_part = head_norm(
        summed[:, :query_cols].reshape(token_rows, local_heads, head_size), query_gain
    )
    key_part = head_norm(
        summed[:, query_cols : query_cols + key_cols].reshape(token_rows, key_heads, head_size),
        key_gain,
    )
    queries = query_part.astype(jnp.bfloat16).reshape(
        seq_count, node_count, key_heads, sharing, head_size
    )
    keys_new = key_part.astype(jnp.bfloat16).reshape(seq_count, node_count, key_heads, head_size)
    values_new = (
        summed[:, query_cols + key_cols :]
        .astype(jnp.bfloat16)
        .reshape(seq_count, node_count, key_heads, head_size)
    )
    head_start = lax.axis_index("tp") * local_heads
    forget_cols = lax.dynamic_slice_in_dim(forget_weight, head_start, local_heads, 1)
    gate_bias = lax.dynamic_slice_in_dim(forget_bias, head_start, local_heads, 0)
    log_gates = jax.nn.log_sigmoid(
        jnp.dot(normed, forget_cols, preferred_element_type=jnp.float32) + gate_bias
    ).reshape(seq_count, node_count, local_heads)
    ancestry = ancestors(parents)
    choose = (jnp.arange(most_taken, dtype=jnp.int32)[None, :] == (accepted - 1)[:, None]).astype(
        jnp.float32
    )
    base_gate = jnp.einsum("sa,sah->sh", choose, pending_logcum, precision=HIGHEST)
    cumulative = base_gate[:, None, :] + jnp.einsum(
        "sij,sjh->sih", ancestry, log_gates, precision=HIGHEST
    )
    gate_rows = jnp.swapaxes(cumulative, 1, 2)
    token_place = lax.axis_index("kv") * block_len + jnp.arange(block_len, dtype=jnp.int32)
    offset = token_place[None, :] - lengths[:, None]
    inserted = (offset >= 0) & (offset < accepted[:, None])
    one_hot = (offset[..., None] == jnp.arange(most_taken, dtype=jnp.int32)) & inserted[..., None]
    hot_low = one_hot.astype(jnp.bfloat16)
    merged_keys = jnp.where(
        inserted[..., None, None],
        jnp.einsum(
            "sla,sakd->slkd", hot_low, pending_keys, preferred_element_type=jnp.float32
        ).astype(jnp.bfloat16),
        cache_keys,
    )
    merged_values = jnp.where(
        inserted[..., None, None],
        jnp.einsum(
            "sla,sakd->slkd", hot_low, pending_values, preferred_element_type=jnp.float32
        ).astype(jnp.bfloat16),
        cache_values,
    )
    log_cache = jnp.where(
        inserted[..., None],
        jnp.einsum("sla,sah->slh", one_hot.astype(jnp.float32), pending_logcum, precision=HIGHEST),
        cache_logcum,
    )
    usable = token_place[None, :] < (lengths + accepted)[:, None]
    raw_scores = jnp.einsum(
        "spkgd,slkd->skgpl", queries, merged_keys, preferred_element_type=jnp.float32
    )
    scores = (
        raw_scores.reshape(seq_count, local_heads, node_count, block_len) * scaling
        + gate_rows[..., None]
        - jnp.swapaxes(log_cache, 1, 2)[:, :, None, :]
    )
    visible = usable[:, None, None, :]
    block_max = jnp.max(jnp.where(visible, scores, NEG_LARGE), axis=-1)
    weights = jnp.where(visible, jnp.exp(scores - block_max[..., None]), 0.0)
    block_sum = jnp.sum(weights, axis=-1)
    block_acc = jnp.einsum(
        "skgpl,slkd->skgpd",
        weights.astype(jnp.bfloat16).reshape(seq_count, key_heads, sharing, node_count, block_len),
        merged_values,
        preferred_element_type=jnp.float32,
    )
    block_acc = block_acc.reshape(seq_count, local_heads, node_count, head_size)
    tree_raw = jnp.einsum(
        "spkgd,sjkd->skgpj", queries, keys_new, preferred_element_type=jnp.float32
    )
    tree_scores = (
        tree_raw.reshape(seq_count, local_heads, node_count, node_count) * scaling
        + gate_rows[..., :, None]
        - gate_rows[..., None, :]
    )
    tree_mask = ancestry[:, None] > 0.5
    tree_max = jnp.max(jnp.where(tree_mask, tree_scores, NEG_LARGE), axis=-1)
    tree_weights = jnp.where(tree_mask, jnp.exp(tree_scores - tree_max[..., None]), 0.0)
    tree_sum = jnp.sum(tree_weights, axis=-1)
    tree_acc = jnp.einsum(
        "skgpj,sjkd->skgpd",
        tree_weights.astype(jnp.bfloat16).reshape(
            seq_count, key_heads, sharing, node_count, node_count
        ),
        values_new,
        preferred_element_type=jnp.float32,
    )
    tree_acc = tree_acc.reshape(seq_count, local_heads, node_count, head_size)
    tree_max_rows = to_rows(tree_max)
    tree_sum_rows = to_rows(tree_sum)
    tree_acc_rows = to_rows(tree_acc)
    cache_max, cache_sum, cache_acc = joined((block_max, block_sum, block_acc), "kv", join_blocks)
    attended = finish_rows(
        to_rows(cache_max),
        to_rows(cache_sum),
        to_rows(cache_acc),
        tree_max_rows,
        tree_sum_rows,
        tree_acc_rows,
    )
    head_part = jnp.dot(attended, output_weight, preferred_element_type=jnp.float32)
    head_part = head_part.reshape(seq_count, node_count, output_weight.shape[1])
    return lax.psum_scatter(head_part.astype(jnp.bfloat16), "tp", scatter_dimension=2, tiled=True)


LOG2E = math.log2(math.e)
MASKED = 2.0**100
STAT_ROWS = 16
GRANT = 16 * 2**20
GO_ORDER = (2, 3, 1)
BACK_ORDER = (3, 2, 1)
EARLY, LATE = (0, 1, 3), (2,)
NT = (((1,), (1,)), ((), ()))


def in_vmem(shape, dtype):
    return pltpu.VMEM(shape, dtype)


def held(array):
    return pltpu.with_memory_space_constraint(array, pltpu.VMEM)


def partner_of(place, step):
    return jnp.bitwise_xor(place, step)


def tile_rows(rows, nodes):
    return jnp.concatenate(
        [jnp.broadcast_to(rows[i : i + 1, :], (nodes, rows.shape[1])) for i in range(rows.shape[0])],
        axis=0,
    )


def stacked(columns, head_rows, lanes):
    lane = lax.broadcasted_iota(jnp.int32, (head_rows, lanes), 1)
    stats = jnp.zeros((head_rows, lanes), jnp.float32)
    for place, column in enumerate(columns):
        stats = jnp.where(lane == place, column, stats)
    return stats.T


def partials(queries, keys, values, decays, nodes, packed, extra=None):
    head_rows, head_size = queries[0].shape
    scale = head_size ** (-0.5) * LOG2E
    group = len(queries)
    raw = [
        lax.dot_general(q, k, NT, preferred_element_type=jnp.float32)
        for q, k in zip(queries, keys, strict=True)
    ]
    scores = [r * scale - tile_rows(d, nodes) for r, d in zip(raw, decays, strict=True)]
    tops = [jnp.max(s, axis=1, keepdims=True) for s in scores]
    if extra is not None:
        tree_scores, tree_values = extra
        tops = [
            jnp.maximum(t, jnp.max(s, axis=1, keepdims=True))
            for t, s in zip(tops, tree_scores, strict=True)
        ]
    tops = [t.astype(jnp.bfloat16).astype(jnp.float32) for t in tops]
    weights = [jnp.exp2(s - t) for s, t in zip(scores, tops, strict=True)]
    totals = [jnp.sum(w, axis=1, keepdims=True) for w in weights]
    sums = [
        jnp.dot(w.astype(jnp.bfloat16), v, preferred_element_type=jnp.float32)
        for w, v in zip(weights, values, strict=True)
    ]
    if extra is not None:
        weights = [jnp.exp2(s - t) for s, t in zip(tree_scores, tops, strict=True)]
        totals = [
            t + jnp.sum(w, axis=1, keepdims=True) for t, w in zip(totals, weights, strict=True)
        ]
        sums = [
            s + jnp.dot(w.astype(jnp.bfloat16), tree_values, preferred_element_type=jnp.float32)
            for s, w in zip(sums, weights, strict=True)
        ]
    for item in range(group):
        first = item * head_rows
        packed[first : first + head_rows, :] = sums[item].astype(jnp.bfloat16)
    high = [t.astype(jnp.bfloat16).astype(jnp.float32) for t in totals]
    low = [t - h for t, h in zip(totals, high, strict=True)]
    stats = stacked(tops + high + low, head_rows, head_size)
    packed[group * head_rows :, :head_rows] = stats[:STAT_ROWS, :].astype(jnp.bfloat16)
    packed[group * head_rows :, head_rows:] = jnp.zeros(
        (STAT_ROWS, head_size - head_rows), jnp.bfloat16
    )


def unit(vectors, gain_vec):
    mean = jnp.mean(vectors * vectors, axis=1, keepdims=True)
    return (vectors * lax.rsqrt(mean + EPSILON) * gain_vec).astype(jnp.bfloat16)


def normalized(tokens, first, count, nodes, gain, normed):
    for start in range(0, count, nodes):
        widened = tokens[pl.ds(first + start, nodes), :].astype(jnp.float32)
        mean = jnp.mean(widened * widened, axis=1, keepdims=True)
        normed[pl.ds(start, nodes), :] = (
            widened * lax.rsqrt(mean + EPSILON) * gain
        ).astype(jnp.bfloat16)


def queries_of(summed, gain, nodes):
    head_size = gain.shape[1]
    heads = summed.shape[1] // head_size
    normal = [
        unit(summed[:, head * head_size : (head + 1) * head_size], gain) for head in range(heads)
    ]
    return [
        jnp.concatenate([n[first : first + nodes, :] for n in normal], axis=0)
        for first in range(0, summed.shape[0], nodes)
    ]


def first_kernel(
    kv_size,
    lengths,
    tokens,
    norm_gain,
    query_weight,
    query_gain,
    cache_keys,
    cache_values,
    cache_logcum,
    packed,
    second_queries,
    weight_buf,
    decay_buf,
    length_buf,
    token_buf,
    gain_buf,
    query_gain_buf,
    key_buf,
    value_buf,
    logcum_buf,
    normed,
    small_sem,
    weight_sem,
):
    place = lax.axis_index("kv")
    rows, width = tokens.shape
    seq_count, block_len = cache_keys.shape[0], cache_keys.shape[1]
    heads = cache_logcum.shape[1]
    nodes = rows // seq_count
    group = seq_count // kv_size
    count = group * nodes
    depth_parts = weight_sem.shape[0]
    depth = width // depth_parts
    owner = partner_of(place, GO_ORDER[0])

    second = partner_of(place, GO_ORDER[1])
    cache_span = pl.ds(owner * group, group)
    small = [
        pltpu.make_async_copy(source, target, small_sem.at[i])
        for i, (source, target) in enumerate(
            (
                (norm_gain, gain_buf),
                (tokens.at[pl.ds(pl.multiple_of(owner * count, count), count)], token_buf.at[0]),
                (tokens.at[pl.ds(pl.multiple_of(second * count, count), count)], token_buf.at[1]),
                (cache_logcum, logcum_buf),
                (lengths, length_buf),
                (query_gain, query_gain_buf),
                (cache_keys.at[cache_span], key_buf),
                (cache_values.at[cache_span], value_buf),
            )
        )
    ]
    weight_copies = [
        pltpu.make_async_copy(
            query_weight.at[pl.ds(i * depth, depth)],
            weight_buf.at[pl.ds(i * depth, depth)],
            weight_sem.at[i],
        )
        for i in range(depth_parts)
    ]
    for copy in small[:3] + weight_copies + small[3:]:
        copy.start()

    small[0].wait()
    for item in range(2):
        small[1 + item].wait()
        normalized(token_buf.at[item], 0, count, nodes, gain_buf[...], normed.at[pl.ds(item * count, count)])
    summed = None
    for part in range(depth_parts):
        weight_copies[part].wait()
        span = pl.ds(part * depth, depth)
        product = jnp.dot(normed[:, span], weight_buf[span, :], preferred_element_type=jnp.float32)
        summed = product if part == 0 else summed + product
    for copy in small[3:]:
        copy.wait()
    column = lax.broadcasted_iota(jnp.int32, (heads, block_len), 1)
    for seq in range(seq_count):
        valid = length_buf[seq] - place * block_len
        decay_buf[seq] = jnp.where(column < valid, logcum_buf[seq] * LOG2E, MASKED)
    queries = queries_of(summed, query_gain_buf[...], nodes)
    for item in range(group):
        second_queries[item] = queries[group + item]
    partials(
        queries[:group],
        [key_buf[item] for item in range(group)],
        [value_buf[item] for item in range(group)],
        [decay_buf[owner * group + item] for item in range(group)],
        nodes,
        packed,
    )


def step_partials(step, nodes, tokens, norm_gain, query_weight, query_gain, keys, values, decays, normed, packed, extra_of=None):
    place = lax.axis_index("kv")
    count = normed.shape[0]
    group = count // nodes
    owner = partner_of(place, step)
    normalized(tokens, pl.multiple_of(owner * count, count), count, nodes, norm_gain[...], normed)
    summed = jnp.dot(normed[...], query_weight[...], preferred_element_type=jnp.float32)
    queries = queries_of(summed, query_gain[...], nodes)
    seqs = [owner * group + item for item in range(group)]
    partials(
        queries,
        [keys[seq] for seq in seqs],
        [values[seq] for seq in seqs],
        [decays[seq] for seq in seqs],
        nodes,
        packed,
        None if extra_of is None else extra_of(queries),
    )


def next_kernel(step, nodes, *refs):
    *operands, packed, normed = refs
    step_partials(step, nodes, *operands, normed, packed)


def second_kernel(step, nodes, queries, keys, values, decays, packed):
    group = queries.shape[0]
    seqs = [partner_of(lax.axis_index("kv"), step) * group + item for item in range(group)]
    partials(
        [queries[item] for item in range(group)],
        [keys[seq] for seq in seqs],
        [values[seq] for seq in seqs],
        [decays[seq] for seq in seqs],
        nodes,
        packed,
    )


def own_kernel(
    tp_size,
    nodes,
    accepted,
    forget_bias,
    parents,
    forget_rows,
    pending_keys,
    pending_values,
    pending_logcum,
    key_weight,
    value_weight,
    key_gain,
    tokens,
    norm_gain,
    query_weight,
    query_gain,
    keys,
    values,
    decays,
    packed,
    terms,
    key_buf,
    value_buf,
    normed,
):
    extra_of = functools.partial(
        tree_block,
        tp_size,
        nodes,
        accepted,
        forget_bias,
        parents,
        forget_rows,
        pending_keys,
        pending_values,
        pending_logcum,
        key_weight,
        value_weight,
        key_gain,
        terms,
        key_buf,
        value_buf,
        normed,
    )
    step_partials(
        0,
        nodes,
        tokens,
        norm_gain,
        query_weight,
        query_gain,
        keys,
        values,
        decays,
        normed,
        packed,
        extra_of,
    )


def tree_block(
    tp_size,
    nodes,
    accepted,
    forget_bias,
    parents,
    forget_rows,
    pending_keys,
    pending_values,
    pending_logcum,
    key_weight,
    value_weight,
    key_gain,
    terms,
    key_buf,
    value_buf,
    normed,
    queries,
):
    place = lax.axis_index("kv")
    side = lax.axis_index("tp")
    tree_rows = normed.shape[0]
    group = tree_rows // nodes
    most_taken, heads, seq_count = pending_logcum.shape
    head_rows, head_size = heads * nodes, key_gain.shape[1]
    size = 2 * tree_rows
    exact = dict(preferred_element_type=jnp.float32, precision=HIGHEST)

    key_buf[...] = jnp.zeros_like(key_buf)
    value_buf[...] = jnp.zeros_like(value_buf)
    summed = jnp.dot(
        normed[...],
        jnp.concatenate([key_weight[...], value_weight[...]], axis=1),
        preferred_element_type=jnp.float32,
    )
    key_buf[:tree_rows, :] = unit(summed[:, :head_size], key_gain[...]).astype(jnp.float32)
    value_buf[:tree_rows, :] = summed[:, head_size:]
    for item in range(group):
        rows = slice(tree_rows + item * most_taken, tree_rows + (item + 1) * most_taken)
        key_buf[rows, :] = pending_keys[place * group + item].astype(jnp.float32)
        value_buf[rows, :] = pending_values[place * group + item].astype(jnp.float32)
    gates = lax.dot_general(
        forget_rows[...], normed[...], NT, preferred_element_type=jnp.float32
    )

    lane = lax.broadcasted_iota(jnp.int32, (1, size), 1)
    in_tree = jnp.where(lane < tree_rows, 1, 0)
    tree_item, tree_node = lane // nodes, lane % nodes
    late = lane - tree_rows
    late_item, late_node = late // most_taken, late % most_taken
    in_late = jnp.where((late >= 0) & (late_item < group), 1, 0)
    item_of = jnp.where(late < 0, tree_item, late_item)
    taken = jnp.zeros((1, size), jnp.int32)
    for item in range(group):
        taken = jnp.where(item_of == item, accepted[place * group + item], taken)

    node_row = lax.broadcasted_iota(jnp.int32, (parents.shape[1], size), 0)
    spread = jnp.dot(
        parents[...].astype(jnp.float32),
        (node_row == tree_node).astype(jnp.float32),
        preferred_element_type=jnp.float32,
    )
    seq_row = lax.broadcasted_iota(jnp.int32, (seq_count, size), 0)
    own_seq = (seq_row == place * group + jnp.where(in_tree + in_late > 0, item_of, -seq_count)).astype(
        jnp.float32
    )
    parent = jnp.sum(own_seq * spread, axis=0, keepdims=True).astype(jnp.int32)
    square_row = lax.broadcasted_iota(jnp.int32, (size, size), 0)
    square_lane = lax.broadcasted_iota(jnp.int32, (size, size), 1)
    identity = (square_row == square_lane).astype(jnp.float32)
    linked = square_row == jnp.where((late < 0) & (parent >= 0), tree_item * nodes + parent, -1)
    reach = linked.astype(jnp.float32) + identity
    for _ in range((nodes - 1).bit_length()):
        low = reach.astype(jnp.bfloat16)
        reach = jnp.minimum(jnp.dot(low, low, preferred_element_type=jnp.float32), 1.0)
    low = reach.astype(jnp.bfloat16)
    ancestry = lax.dot_general(
        identity.astype(jnp.bfloat16), low, NT, preferred_element_type=jnp.float32
    )

    raw_gates = gates[:heads, :]
    for other in range(1, tp_size):
        raw_gates = jnp.where(side == other, gates[other * heads : (other + 1) * heads, :], raw_gates)
    bias = jnp.concatenate(
        [jnp.full((1, tree_rows), forget_bias[side * heads + head]) for head in range(heads)], axis=0
    )
    logits = raw_gates + bias
    log_gates = jnp.minimum(logits, 0.0) - jnp.log1p(jnp.exp(-jnp.abs(logits)))
    decay = jnp.dot(log_gates, reach[:tree_rows, :], **exact)
    decay = decay * in_tree.astype(jnp.float32)
    picked = jnp.where(late < 0, taken - 1, late_node)
    for node in range(most_taken):
        chosen = own_seq * (picked == node).astype(jnp.float32)
        decay = decay + jnp.dot(pending_logcum[node], chosen, **exact)
    decay = decay * LOG2E

    head_decay = tile_rows(decay, nodes)
    row = lax.broadcasted_iota(jnp.int32, (head_rows, size), 0)
    tree_keys = key_buf[...].astype(jnp.bfloat16)
    scale = head_size ** (-0.5) * LOG2E
    tree_scores, own_terms = [], []
    for item in range(group):
        raw = lax.dot_general(
            queries[item], tree_keys, NT, preferred_element_type=jnp.float32
        )
        own_terms.append(
            jnp.sum(
                jnp.where(lane == item * nodes + row % nodes, head_decay, 0.0),
                axis=1,
                keepdims=True,
            )
        )
        reached = jnp.concatenate([ancestry[item * nodes : (item + 1) * nodes, :]] * heads, axis=0)
        offered = jnp.where(late_item == item, jnp.where(late_node < taken, in_late, 0), 0)
        seen = reached * in_tree.astype(jnp.float32) + offered.astype(jnp.float32) > 0.5
        tree_scores.append(jnp.where(seen, raw * scale - head_decay, -MASKED))
    terms[...] = stacked(own_terms, head_rows, head_size)[: terms.shape[0], :]
    return tree_scores, value_buf[...].astype(jnp.bfloat16)


def merge_kernel(kv_size, terms, *refs):
    packed, chunk = refs[:kv_size], refs[kv_size]
    head_size = packed[0].shape[1]
    heads = chunk.shape[1] // head_size
    head_rows = terms.shape[1]
    nodes = head_rows // heads
    group = chunk.shape[0] // nodes
    base = group * head_rows
    term = terms[:group, :]
    stats = [p[base:, :head_rows].astype(jnp.float32) for p in packed]
    tops = [s[:group] + term for s in stats]
    top = functools.reduce(jnp.maximum, tops)
    factors = [jnp.exp2(t - top) for t in tops]
    bottom = sum(
        (s[group : 2 * group] + s[2 * group : 3 * group]) * f
        for s, f in zip(stats, factors, strict=True)
    )
    factors = [f / bottom for f in factors]
    row = lax.broadcasted_iota(jnp.int32, (head_rows, head_rows), 0)
    lane = lax.broadcasted_iota(jnp.int32, (head_rows, head_rows), 1)
    for item in range(group):
        rows = slice(item * head_rows, (item + 1) * head_rows)
        attended = jnp.zeros((head_rows, head_size), jnp.float32)
        for source in range(kv_size):
            spread = jnp.where(row == lane, factors[source][item : item + 1, :], 0.0)
            high = spread.astype(jnp.bfloat16)
            low = (spread - high.astype(jnp.float32)).astype(jnp.bfloat16)
            held_rows = packed[source][rows, :]
            attended += jnp.dot(high, held_rows, preferred_element_type=jnp.float32)
            attended += jnp.dot(low, held_rows, preferred_element_type=jnp.float32)
        attended = attended.astype(jnp.bfloat16)
        for head in range(heads):
            chunk[item * nodes : (item + 1) * nodes, head * head_size : (head + 1) * head_size] = (
                attended[head * nodes : (head + 1) * nodes, :]
            )


def project_kernel(other, weight, *refs):
    *chunks, out = refs
    side = lax.axis_index("tp")
    half = 1 - side if other else side
    rows, cols = chunks[0].shape[0], out.shape[1]
    part = weight[:, pl.ds(pl.multiple_of(half * cols, cols), cols)]
    for i, chunk in enumerate(chunks):
        out[i * rows : (i + 1) * rows, :] = jnp.dot(
            chunk[...], part, preferred_element_type=jnp.float32
        ).astype(jnp.bfloat16)


def add_kernel(kept, early, late, out, buf, sem):
    place = lax.axis_index("kv")
    rows = late.shape[0] // len(LATE)
    copies = []
    for i, step in enumerate(EARLY + LATE):
        span = slice(i * rows, (i + 1) * rows)
        first = (i - len(EARLY)) * rows
        received = late[first : first + rows, :] if i >= len(EARLY) else early[span, :]
        buf[span, :] = (kept[span, :].astype(jnp.float32) + received.astype(jnp.float32)).astype(
            jnp.bfloat16
        )
        target = pl.ds(pl.multiple_of(partner_of(place, step) * rows, rows), rows)
        copies.append(pltpu.make_async_copy(buf.at[pl.ds(i * rows, rows)], out.at[target], sem.at[i]))
        copies[-1].start()
    for copy in copies:
        copy.wait()


def exchange(array, axis, size, step):
    return lax.ppermute(array, axis, [(i, i ^ step) for i in range(size)])


def fast_shards(
    tokens,
    norm_gain,
    query_weight,
    key_weight,
    value_weight,
    forget_weight,
    forget_bias,
    query_gain,
    key_gain,
    output_weight,
    cache_keys,
    cache_values,
    cache_logcum,
    pending_keys,
    pending_values,
    pending_logcum,
    lengths,
    accepted,
    parents,
):
    kv_size, tp_size = lax.axis_size("kv"), lax.axis_size("tp")
    seq_count, nodes, width = tokens.shape
    query_cols = query_weight.shape[1]
    head_size = query_gain.shape[0]
    heads = query_cols // head_size
    block_len = cache_keys.shape[1]
    most_taken = pending_keys.shape[1]
    rows = seq_count * nodes
    group = seq_count // kv_size
    head_rows = heads * nodes
    bf16, f32 = jnp.bfloat16, jnp.float32
    hbm = pl.BlockSpec(memory_space=pltpu.HBM)
    vmem = pl.BlockSpec(memory_space=pltpu.VMEM)
    smem = pl.BlockSpec(memory_space=pltpu.SMEM)
    depth_parts = 4
    count = group * nodes
    packed_shape = in_vmem((group * head_rows + STAT_ROWS, head_size), bf16)
    token_matrix = tokens.reshape(rows, width)
    norm_row = norm_gain.reshape(1, width)
    query_row = query_gain.reshape(1, head_size)
    key_array = cache_keys.reshape(seq_count, block_len, head_size)
    value_array = cache_values.reshape(seq_count, block_len, head_size)

    farthest, second_queries, query_matrix, decays = pl.pallas_call(
        functools.partial(first_kernel, kv_size),
        compiler_params=pltpu.CompilerParams(vmem_limit_bytes=GRANT),
        name="first",
        out_shape=[
            packed_shape,
            in_vmem((group, head_rows, head_size), bf16),
            in_vmem((width, query_cols), bf16),
            in_vmem((seq_count, heads, block_len), f32),
        ],
        in_specs=[hbm] * 8,
        out_specs=[vmem] * 4,
        scratch_shapes=[
            pltpu.SMEM((seq_count,), jnp.int32),
            pltpu.VMEM((2, count, width), bf16),
            pltpu.VMEM((1, width), f32),
            pltpu.VMEM((1, head_size), f32),
            pltpu.VMEM((group, block_len, head_size), bf16),
            pltpu.VMEM((group, block_len, head_size), bf16),
            pltpu.VMEM((seq_count, heads, block_len), f32),
            pltpu.VMEM((2 * count, width), bf16),
            pltpu.SemaphoreType.DMA((8,)),
            pltpu.SemaphoreType.DMA((depth_parts,)),
        ],
    )(
        *[
            pltpu.with_memory_space_constraint(a, pltpu.HBM)
            for a in (
                lengths,
                token_matrix,
                norm_row,
                query_weight,
                query_row,
                key_array,
                value_array,
                jnp.swapaxes(cache_logcum, 1, 2),
            )
        ]
    )
    shared = [
        held(a)
        for a in (token_matrix, norm_row, query_matrix, query_row, key_array, value_array, decays)
    ]
    packed = {GO_ORDER[0]: farthest}
    packed[GO_ORDER[1]] = pl.pallas_call(
        functools.partial(second_kernel, GO_ORDER[1], nodes),
        compiler_params=pltpu.CompilerParams(vmem_limit_bytes=GRANT),
        name="second",
        out_shape=packed_shape,
        in_specs=[vmem] * 4,
        out_specs=vmem,
    )(held(second_queries), *shared[4:])
    for step in GO_ORDER[2:]:
        packed[step] = pl.pallas_call(
            functools.partial(next_kernel, step, nodes),
            compiler_params=pltpu.CompilerParams(vmem_limit_bytes=GRANT),
            out_shape=packed_shape,
            in_specs=[vmem] * 7,
            out_specs=vmem,
            scratch_shapes=[pltpu.VMEM((count, width), bf16)],
        )(*shared)
    moved = {}
    for step in GO_ORDER:
        moved[step] = exchange(packed[step], "kv", kv_size, step)
    own, terms = pl.pallas_call(
        functools.partial(own_kernel, tp_size, nodes),
        compiler_params=pltpu.CompilerParams(vmem_limit_bytes=GRANT),
        name="own",
        out_shape=[packed_shape, in_vmem((8, head_rows), f32)],
        in_specs=[smem, smem] + [vmem] * 15,
        out_specs=[vmem, vmem],
        scratch_shapes=[pltpu.VMEM((2 * count, head_size), f32)] * 2
        + [pltpu.VMEM((count, width), bf16)],
        cost_estimate=pl.CostEstimate(flops=4_000_000_000, bytes_accessed=1_000_000, transcendentals=0),
    )(
        accepted,
        forget_bias,
        parents,
        forget_weight.T,
        pending_keys.reshape(seq_count, most_taken, head_size),
        pending_values.reshape(seq_count, most_taken, head_size),
        jnp.transpose(pending_logcum, (1, 2, 0)),
        held(key_weight),
        held(value_weight),
        key_gain.reshape(1, head_size),
        *shared,
    )
    chunk = pl.pallas_call(
        functools.partial(merge_kernel, kv_size),
        compiler_params=pltpu.CompilerParams(vmem_limit_bytes=GRANT),
        name="merge",
        out_shape=in_vmem((group * nodes, query_cols), bf16),
        in_specs=[vmem] * (kv_size + 1),
        out_specs=vmem,
    )(held(terms), held(own), *[held(moved[s]) for s in range(1, kv_size)])
    chunks = {0: chunk}
    for step in BACK_ORDER:
        chunks[step] = exchange(chunk, "kv", kv_size, step)
    cols = output_weight.shape[1] // tp_size
    weight = held(output_weight)

    def project(steps, other):
        return pl.pallas_call(
            functools.partial(project_kernel, other),
            compiler_params=pltpu.CompilerParams(vmem_limit_bytes=GRANT),
            name="project",
            out_shape=in_vmem((len(steps) * count, cols), bf16),
            in_specs=[vmem] * (len(steps) + 1),
            out_specs=vmem,
            cost_estimate=pl.CostEstimate(flops=1_000_000_000, bytes_accessed=0, transcendentals=0),
        )(weight, *[held(chunks[step]) for step in steps])

    received = []
    for steps in (EARLY, LATE):
        sent = project(steps, True)
        received.append(held(exchange(sent, "tp", tp_size, 1)))
    kept = project(EARLY + LATE, False)
    summed = pl.pallas_call(
        add_kernel,
        compiler_params=pltpu.CompilerParams(vmem_limit_bytes=GRANT),
        name="add",
        out_shape=jax.ShapeDtypeStruct((rows, cols), bf16),
        in_specs=[vmem] * 3,
        out_specs=hbm,
        scratch_shapes=[pltpu.VMEM((rows, cols), bf16), pltpu.SemaphoreType.DMA((kv_size,))],
    )(held(kept), *received)
    return summed.reshape(seq_count, nodes, cols)


def fits_fast(mesh, shapes):
    kv_size = mesh.shape["kv"]
    seq_count = shapes["tokens"][0] // mesh.shape["dp"]
    one_key_head = shapes["cache_keys"][2] == mesh.shape["tp"]
    small = kv_size == 4
    return small and one_key_head and mesh.shape["tp"] == 2 and seq_count % kv_size == 0


def chosen_shards(mesh):
    def run(*args):
        shapes = {"tokens": args[0].shape, "cache_keys": args[10].shape}
        shapes["tokens"] = (shapes["tokens"][0] * mesh.shape["dp"],)
        shapes["cache_keys"] = (0, 0, shapes["cache_keys"][2] * mesh.shape["tp"])
        if not fits_fast(mesh, shapes):
            return shards(*args)
        return fast_shards(*args)

    return run


def solution(mesh):
    placed = (
        P("dp", None, None),
        P(),
        P(None, "tp"),
        P(None, "tp"),
        P(None, "tp"),
        P(),
        P(),
        P(),
        P(),
        P("tp", "kv"),
        P("dp", "kv", "tp", None),
        P("dp", "kv", "tp", None),
        P("dp", "kv", "tp"),
        P("dp", None, "tp", None),
        P("dp", None, "tp", None),
        P("dp", None, "tp"),
        P("dp"),
        P("dp"),
        P("dp", None),
    )
    return jax.shard_map(
        chosen_shards(mesh), mesh=mesh, in_specs=placed, out_specs=P("dp", None, ("kv", "tp")), check_vma=False
    )
```

```python
import functools
import math

import jax
import jax.numpy as jnp
from jax import lax
from jax.experimental import pallas as pl
from jax.experimental.pallas import tpu as pltpu
from jax.sharding import PartitionSpec as P

EPSILON = 1e-06
NEG_LARGE = -1e30
HIGHEST = lax.Precision.HIGHEST


def joined(shard, axis, join):
    gathered = jax.tree.map(
        lambda a, kind: lax.all_gather(a.astype(kind), axis),
        shard,
        (jnp.bfloat16, jnp.bfloat16, jnp.bfloat16),
    )

    def take(source):
        return jax.tree.map(
            lambda a, own: lax.dynamic_index_in_dim(a, source, 0, False).astype(own.dtype),
            gathered,
            shard,
        )

    return lax.fori_loop(
        1, lax.axis_size(axis), lambda source, state: join(state, take(source)), take(0)
    )


def head_norm(vectors, gain_vec):
    return (
        vectors
        * lax.rsqrt(jnp.mean(vectors * vectors, axis=-1, keepdims=True) + EPSILON)
        * gain_vec
    )


def ancestors(parents):
    node_count = parents.shape[-1]
    indices = jnp.arange(node_count, dtype=jnp.int32)
    reachable = (parents[..., None] == indices).astype(jnp.float32) + jnp.eye(
        node_count, dtype=jnp.float32
    )
    for _ in range((node_count - 1).bit_length()):
        reachable = jnp.minimum(
            jnp.einsum("sij,sjk->sik", reachable, reachable, precision=HIGHEST), 1.0
        )
    return reachable


def join_blocks(earlier, later):
    larger = jnp.maximum(earlier[0], later[0])
    left_factor = jnp.exp(earlier[0] - larger)
    right_factor = jnp.exp(later[0] - larger)
    return (
        larger,
        earlier[1] * left_factor + later[1] * right_factor,
        earlier[2] * left_factor[..., None] + later[2] * right_factor[..., None],
    )


def to_rows(values):
    moved = jnp.swapaxes(values, 1, 2)
    return moved.reshape((moved.shape[0] * moved.shape[1],) + moved.shape[2:])


def finish_rows(cache_max, cache_sum, cache_acc, tree_max, tree_sum, tree_acc):
    overall = jnp.maximum(cache_max, tree_max)
    factor_cache = jnp.exp(cache_max - overall)
    factor_tree = jnp.exp(tree_max - overall)
    denominator = cache_sum * factor_cache + tree_sum * factor_tree
    numerator = cache_acc * factor_cache[..., None] + tree_acc * factor_tree[..., None]
    attended = (numerator / denominator[..., None]).astype(jnp.bfloat16)
    return attended.reshape(attended.shape[0], attended.shape[1] * attended.shape[2])


def shards(
    tokens,
    norm_gain,
    query_weight,
    key_weight,
    value_weight,
    forget_weight,
    forget_bias,
    query_gain,
    key_gain,
    output_weight,
    cache_keys,
    cache_values,
    cache_logcum,
    pending_keys,
    pending_values,
    pending_logcum,
    lengths,
    accepted,
    parents,
):
    seq_count, node_count, model_width = tokens.shape
    token_rows = seq_count * node_count
    head_size = query_gain.shape[0]
    query_cols = query_weight.shape[1]
    key_cols = key_weight.shape[1]
    local_heads = query_cols // head_size
    key_heads = key_cols // head_size
    sharing = local_heads // key_heads
    block_len = cache_keys.shape[1]
    most_taken = pending_keys.shape[1]
    scaling = head_size ** (-0.5)
    widened = tokens.reshape(token_rows, model_width).astype(jnp.float32)
    normed = (
        widened
        * lax.rsqrt(jnp.mean(widened * widened, axis=-1, keepdims=True) + EPSILON)
        * norm_gain
    ).astype(jnp.bfloat16)
    joined_weight = jnp.concatenate([query_weight, key_weight, value_weight], axis=1)
    summed = jnp.dot(normed, joined_weight, preferred_element_type=jnp.float32)
    query_part = head_norm(
        summed[:, :query_cols].reshape(token_rows, local_heads, head_size), query_gain
    )
    key_part = head_norm(
        summed[:, query_cols : query_cols + key_cols].reshape(token_rows, key_heads, head_size),
        key_gain,
    )
    queries = query_part.astype(jnp.bfloat16).reshape(
        seq_count, node_count, key_heads, sharing, head_size
    )
    keys_new = key_part.astype(jnp.bfloat16).reshape(seq_count, node_count, key_heads, head_size)
    values_new = (
        summed[:, query_cols + key_cols :]
        .astype(jnp.bfloat16)
        .reshape(seq_count, node_count, key_heads, head_size)
    )
    head_start = lax.axis_index("tp") * local_heads
    forget_cols = lax.dynamic_slice_in_dim(forget_weight, head_start, local_heads, 1)
    gate_bias = lax.dynamic_slice_in_dim(forget_bias, head_start, local_heads, 0)
    log_gates = jax.nn.log_sigmoid(
        jnp.dot(normed, forget_cols, preferred_element_type=jnp.float32) + gate_bias
    ).reshape(seq_count, node_count, local_heads)
    ancestry = ancestors(parents)
    choose = (jnp.arange(most_taken, dtype=jnp.int32)[None, :] == (accepted - 1)[:, None]).astype(
        jnp.float32
    )
    base_gate = jnp.einsum("sa,sah->sh", choose, pending_logcum, precision=HIGHEST)
    cumulative = base_gate[:, None, :] + jnp.einsum(
        "sij,sjh->sih", ancestry, log_gates, precision=HIGHEST
    )
    gate_rows = jnp.swapaxes(cumulative, 1, 2)
    token_place = lax.axis_index("kv") * block_len + jnp.arange(block_len, dtype=jnp.int32)
    offset = token_place[None, :] - lengths[:, None]
    inserted = (offset >= 0) & (offset < accepted[:, None])
    one_hot = (offset[..., None] == jnp.arange(most_taken, dtype=jnp.int32)) & inserted[..., None]
    hot_low = one_hot.astype(jnp.bfloat16)
    merged_keys = jnp.where(
        inserted[..., None, None],
        jnp.einsum(
            "sla,sakd->slkd", hot_low, pending_keys, preferred_element_type=jnp.float32
        ).astype(jnp.bfloat16),
        cache_keys,
    )
    merged_values = jnp.where(
        inserted[..., None, None],
        jnp.einsum(
            "sla,sakd->slkd", hot_low, pending_values, preferred_element_type=jnp.float32
        ).astype(jnp.bfloat16),
        cache_values,
    )
    log_cache = jnp.where(
        inserted[..., None],
        jnp.einsum("sla,sah->slh", one_hot.astype(jnp.float32), pending_logcum, precision=HIGHEST),
        cache_logcum,
    )
    usable = token_place[None, :] < (lengths + accepted)[:, None]
    raw_scores = jnp.einsum(
        "spkgd,slkd->skgpl", queries, merged_keys, preferred_element_type=jnp.float32
    )
    scores = (
        raw_scores.reshape(seq_count, local_heads, node_count, block_len) * scaling
        + gate_rows[..., None]
        - jnp.swapaxes(log_cache, 1, 2)[:, :, None, :]
    )
    visible = usable[:, None, None, :]
    block_max = jnp.max(jnp.where(visible, scores, NEG_LARGE), axis=-1)
    weights = jnp.where(visible, jnp.exp(scores - block_max[..., None]), 0.0)
    block_sum = jnp.sum(weights, axis=-1)
    block_acc = jnp.einsum(
        "skgpl,slkd->skgpd",
        weights.astype(jnp.bfloat16).reshape(seq_count, key_heads, sharing, node_count, block_len),
        merged_values,
        preferred_element_type=jnp.float32,
    )
    block_acc = block_acc.reshape(seq_count, local_heads, node_count, head_size)
    tree_raw = jnp.einsum(
        "spkgd,sjkd->skgpj", queries, keys_new, preferred_element_type=jnp.float32
    )
    tree_scores = (
        tree_raw.reshape(seq_count, local_heads, node_count, node_count) * scaling
        + gate_rows[..., :, None]
        - gate_rows[..., None, :]
    )
    tree_mask = ancestry[:, None] > 0.5
    tree_max = jnp.max(jnp.where(tree_mask, tree_scores, NEG_LARGE), axis=-1)
    tree_weights = jnp.where(tree_mask, jnp.exp(tree_scores - tree_max[..., None]), 0.0)
    tree_sum = jnp.sum(tree_weights, axis=-1)
    tree_acc = jnp.einsum(
        "skgpj,sjkd->skgpd",
        tree_weights.astype(jnp.bfloat16).reshape(
            seq_count, key_heads, sharing, node_count, node_count
        ),
        values_new,
        preferred_element_type=jnp.float32,
    )
    tree_acc = tree_acc.reshape(seq_count, local_heads, node_count, head_size)
    tree_max_rows = to_rows(tree_max)
    tree_sum_rows = to_rows(tree_sum)
    tree_acc_rows = to_rows(tree_acc)
    cache_max, cache_sum, cache_acc = joined((block_max, block_sum, block_acc), "kv", join_blocks)
    attended = finish_rows(
        to_rows(cache_max),
        to_rows(cache_sum),
        to_rows(cache_acc),
        tree_max_rows,
        tree_sum_rows,
        tree_acc_rows,
    )
    head_part = jnp.dot(attended, output_weight, preferred_element_type=jnp.float32)
    head_part = head_part.reshape(seq_count, node_count, output_weight.shape[1])
    return lax.psum_scatter(head_part.astype(jnp.bfloat16), "tp", scatter_dimension=2, tiled=True)


LOG2E = math.log2(math.e)
MASKED = 2.0**100
STAT_ROWS = 16
GRANT = 16 * 2**20
GO_ORDER = (2, 3, 1)
BACK_ORDER = (3, 2, 1)
EARLY, LATE = (0, 1, 3), (2,)
NT = (((1,), (1,)), ((), ()))


def in_vmem(shape, dtype):
    return pltpu.VMEM(shape, dtype)


def held(array):
    return pltpu.with_memory_space_constraint(array, pltpu.VMEM)


def partner_of(place, step):
    return jnp.bitwise_xor(place, step)


def tile_rows(rows, nodes):
    return jnp.concatenate(
        [jnp.broadcast_to(rows[i : i + 1, :], (nodes, rows.shape[1])) for i in range(rows.shape[0])],
        axis=0,
    )


def stacked(columns, head_rows, lanes):
    lane = lax.broadcasted_iota(jnp.int32, (head_rows, lanes), 1)
    stats = jnp.zeros((head_rows, lanes), jnp.float32)
    for place, column in enumerate(columns):
        stats = jnp.where(lane == place, column, stats)
    return stats.T


def partials(queries, keys, values, decays, nodes, packed, extra=None):
    head_rows, head_size = queries[0].shape
    scale = head_size ** (-0.5) * LOG2E
    group = len(queries)
    raw = [
        lax.dot_general(q, k, NT, preferred_element_type=jnp.float32)
        for q, k in zip(queries, keys, strict=True)
    ]
    scores = [r * scale - tile_rows(d, nodes) for r, d in zip(raw, decays, strict=True)]
    tops = [jnp.max(s, axis=1, keepdims=True) for s in scores]
    if extra is not None:
        tree_scores, tree_values = extra
        tops = [
            jnp.maximum(t, jnp.max(s, axis=1, keepdims=True))
            for t, s in zip(tops, tree_scores, strict=True)
        ]
    tops = [t.astype(jnp.bfloat16).astype(jnp.float32) for t in tops]
    weights = [jnp.exp2(s - t) for s, t in zip(scores, tops, strict=True)]
    totals = [jnp.sum(w, axis=1, keepdims=True) for w in weights]
    sums = [
        jnp.dot(w.astype(jnp.bfloat16), v, preferred_element_type=jnp.float32)
        for w, v in zip(weights, values, strict=True)
    ]
    if extra is not None:
        weights = [jnp.exp2(s - t) for s, t in zip(tree_scores, tops, strict=True)]
        totals = [
            t + jnp.sum(w, axis=1, keepdims=True) for t, w in zip(totals, weights, strict=True)
        ]
        sums = [
            s + jnp.dot(w.astype(jnp.bfloat16), tree_values, preferred_element_type=jnp.float32)
            for s, w in zip(sums, weights, strict=True)
        ]
    for item in range(group):
        first = item * head_rows
        packed[first : first + head_rows, :] = sums[item].astype(jnp.bfloat16)
    high = [t.astype(jnp.bfloat16).astype(jnp.float32) for t in totals]
    low = [t - h for t, h in zip(totals, high, strict=True)]
    stats = stacked(tops + high + low, head_rows, head_size)
    packed[group * head_rows :, :head_rows] = stats[:STAT_ROWS, :].astype(jnp.bfloat16)
    packed[group * head_rows :, head_rows:] = jnp.zeros(
        (STAT_ROWS, head_size - head_rows), jnp.bfloat16
    )


def unit(vectors, gain_vec):
    mean = jnp.mean(vectors * vectors, axis=1, keepdims=True)
    return (vectors * lax.rsqrt(mean + EPSILON) * gain_vec).astype(jnp.bfloat16)


def normalized(tokens, first, count, nodes, gain, normed):
    for start in range(0, count, nodes):
        widened = tokens[pl.ds(first + start, nodes), :].astype(jnp.float32)
        mean = jnp.mean(widened * widened, axis=1, keepdims=True)
        normed[pl.ds(start, nodes), :] = (
            widened * lax.rsqrt(mean + EPSILON) * gain
        ).astype(jnp.bfloat16)


def queries_of(summed, gain, nodes):
    head_size = gain.shape[1]
    heads = summed.shape[1] // head_size
    normal = [
        unit(summed[:, head * head_size : (head + 1) * head_size], gain) for head in range(heads)
    ]
    return [
        jnp.concatenate([n[first : first + nodes, :] for n in normal], axis=0)
        for first in range(0, summed.shape[0], nodes)
    ]


def first_kernel(
    kv_size,
    lengths,
    tokens,
    norm_gain,
    query_weight,
    query_gain,
    cache_keys,
    cache_values,
    cache_logcum,
    packed,
    second_queries,
    weight_buf,
    decay_buf,
    length_buf,
    token_buf,
    gain_buf,
    query_gain_buf,
    key_buf,
    value_buf,
    logcum_buf,
    normed,
    small_sem,
    weight_sem,
):
    place = lax.axis_index("kv")
    rows, width = tokens.shape
    seq_count, block_len = cache_keys.shape[0], cache_keys.shape[1]
    heads = cache_logcum.shape[1]
    nodes = rows // seq_count
    group = seq_count // kv_size
    count = group * nodes
    depth_parts = weight_sem.shape[0]
    depth = width // depth_parts
    owner = partner_of(place, GO_ORDER[0])

    second = partner_of(place, GO_ORDER[1])
    cache_span = pl.ds(owner * group, group)
    small = [
        pltpu.make_async_copy(source, target, small_sem.at[i])
        for i, (source, target) in enumerate(
            (
                (norm_gain, gain_buf),
                (tokens.at[pl.ds(pl.multiple_of(owner * count, count), count)], token_buf.at[0]),
                (tokens.at[pl.ds(pl.multiple_of(second * count, count), count)], token_buf.at[1]),
                (cache_logcum, logcum_buf),
                (lengths, length_buf),
                (query_gain, query_gain_buf),
                (cache_keys.at[cache_span], key_buf),
                (cache_values.at[cache_span], value_buf),
            )
        )
    ]
    weight_copies = [
        pltpu.make_async_copy(
            query_weight.at[pl.ds(i * depth, depth)],
            weight_buf.at[pl.ds(i * depth, depth)],
            weight_sem.at[i],
        )
        for i in range(depth_parts)
    ]
    for copy in small[:6] + weight_copies + small[6:]:
        copy.start()

    small[0].wait()
    for item in range(2):
        small[1 + item].wait()
        normalized(token_buf.at[item], 0, count, nodes, gain_buf[...], normed.at[pl.ds(item * count, count)])
    for copy in small[3:6]:
        copy.wait()
    column = lax.broadcasted_iota(jnp.int32, (heads, block_len), 1)
    for seq in range(seq_count):
        valid = length_buf[seq] - place * block_len
        decay_buf[seq] = jnp.where(column < valid, logcum_buf[seq] * LOG2E, MASKED)
    summed = None
    for part in range(depth_parts):
        weight_copies[part].wait()
        span = pl.ds(part * depth, depth)
        product = jnp.dot(normed[:, span], weight_buf[span, :], preferred_element_type=jnp.float32)
        summed = product if part == 0 else summed + product
    for copy in small[6:]:
        copy.wait()
    queries = queries_of(summed, query_gain_buf[...], nodes)
    for item in range(group):
        second_queries[item] = queries[group + item]
    partials(
        queries[:group],
        [key_buf[item] for item in range(group)],
        [value_buf[item] for item in range(group)],
        [decay_buf[owner * group + item] for item in range(group)],
        nodes,
        packed,
    )


def step_partials(step, nodes, tokens, norm_gain, query_weight, query_gain, keys, values, decays, normed, packed, extra_of=None):
    place = lax.axis_index("kv")
    count = normed.shape[0]
    group = count // nodes
    owner = partner_of(place, step)
    normalized(tokens, pl.multiple_of(owner * count, count), count, nodes, norm_gain[...], normed)
    summed = jnp.dot(normed[...], query_weight[...], preferred_element_type=jnp.float32)
    queries = queries_of(summed, query_gain[...], nodes)
    seqs = [owner * group + item for item in range(group)]
    partials(
        queries,
        [keys[seq] for seq in seqs],
        [values[seq] for seq in seqs],
        [decays[seq] for seq in seqs],
        nodes,
        packed,
        None if extra_of is None else extra_of(queries),
    )


def next_kernel(step, nodes, *refs):
    *operands, packed, normed = refs
    step_partials(step, nodes, *operands, normed, packed)


def second_kernel(step, nodes, queries, keys, values, decays, packed):
    group = queries.shape[0]
    seqs = [partner_of(lax.axis_index("kv"), step) * group + item for item in range(group)]
    partials(
        [queries[item] for item in range(group)],
        [keys[seq] for seq in seqs],
        [values[seq] for seq in seqs],
        [decays[seq] for seq in seqs],
        nodes,
        packed,
    )


def own_kernel(
    tp_size,
    nodes,
    accepted,
    forget_bias,
    parents,
    forget_rows,
    pending_keys,
    pending_values,
    pending_logcum,
    key_weight,
    value_weight,
    key_gain,
    tokens,
    norm_gain,
    query_weight,
    query_gain,
    keys,
    values,
    decays,
    packed,
    terms,
    key_buf,
    value_buf,
    normed,
):
    extra_of = functools.partial(
        tree_block,
        tp_size,
        nodes,
        accepted,
        forget_bias,
        parents,
        forget_rows,
        pending_keys,
        pending_values,
        pending_logcum,
        key_weight,
        value_weight,
        key_gain,
        terms,
        key_buf,
        value_buf,
        normed,
    )
    step_partials(
        0,
        nodes,
        tokens,
        norm_gain,
        query_weight,
        query_gain,
        keys,
        values,
        decays,
        normed,
        packed,
        extra_of,
    )


def tree_block(
    tp_size,
    nodes,
    accepted,
    forget_bias,
    parents,
    forget_rows,
    pending_keys,
    pending_values,
    pending_logcum,
    key_weight,
    value_weight,
    key_gain,
    terms,
    key_buf,
    value_buf,
    normed,
    queries,
):
    place = lax.axis_index("kv")
    side = lax.axis_index("tp")
    tree_rows = normed.shape[0]
    group = tree_rows // nodes
    most_taken, heads, seq_count = pending_logcum.shape
    head_rows, head_size = heads * nodes, key_gain.shape[1]
    size = 2 * tree_rows
    exact = dict(preferred_element_type=jnp.float32, precision=HIGHEST)

    key_buf[...] = jnp.zeros_like(key_buf)
    value_buf[...] = jnp.zeros_like(value_buf)
    summed = jnp.dot(
        normed[...],
        jnp.concatenate([key_weight[...], value_weight[...]], axis=1),
        preferred_element_type=jnp.float32,
    )
    key_buf[:tree_rows, :] = unit(summed[:, :head_size], key_gain[...]).astype(jnp.float32)
    value_buf[:tree_rows, :] = summed[:, head_size:]
    for item in range(group):
        rows = slice(tree_rows + item * most_taken, tree_rows + (item + 1) * most_taken)
        key_buf[rows, :] = pending_keys[place * group + item].astype(jnp.float32)
        value_buf[rows, :] = pending_values[place * group + item].astype(jnp.float32)
    gates = lax.dot_general(
        forget_rows[...], normed[...], NT, preferred_element_type=jnp.float32
    )

    lane = lax.broadcasted_iota(jnp.int32, (1, size), 1)
    in_tree = jnp.where(lane < tree_rows, 1, 0)
    tree_item, tree_node = lane // nodes, lane % nodes
    late = lane - tree_rows
    late_item, late_node = late // most_taken, late % most_taken
    in_late = jnp.where((late >= 0) & (late_item < group), 1, 0)
    item_of = jnp.where(late < 0, tree_item, late_item)
    taken = jnp.zeros((1, size), jnp.int32)
    for item in range(group):
        taken = jnp.where(item_of == item, accepted[place * group + item], taken)

    node_row = lax.broadcasted_iota(jnp.int32, (parents.shape[1], size), 0)
    spread = jnp.dot(
        parents[...].astype(jnp.float32),
        (node_row == tree_node).astype(jnp.float32),
        preferred_element_type=jnp.float32,
    )
    seq_row = lax.broadcasted_iota(jnp.int32, (seq_count, size), 0)
    own_seq = (seq_row == place * group + jnp.where(in_tree + in_late > 0, item_of, -seq_count)).astype(
        jnp.float32
    )
    parent = jnp.sum(own_seq * spread, axis=0, keepdims=True).astype(jnp.int32)
    square_row = lax.broadcasted_iota(jnp.int32, (size, size), 0)
    square_lane = lax.broadcasted_iota(jnp.int32, (size, size), 1)
    identity = (square_row == square_lane).astype(jnp.float32)
    linked = square_row == jnp.where((late < 0) & (parent >= 0), tree_item * nodes + parent, -1)
    reach = linked.astype(jnp.float32) + identity
    for _ in range((nodes - 1).bit_length()):
        low = reach.astype(jnp.bfloat16)
        reach = jnp.minimum(jnp.dot(low, low, preferred_element_type=jnp.float32), 1.0)
    low = reach.astype(jnp.bfloat16)
    ancestry = lax.dot_general(
        identity.astype(jnp.bfloat16), low, NT, preferred_element_type=jnp.float32
    )

    raw_gates = gates[:heads, :]
    for other in range(1, tp_size):
        raw_gates = jnp.where(side == other, gates[other * heads : (other + 1) * heads, :], raw_gates)
    bias = jnp.concatenate(
        [jnp.full((1, tree_rows), forget_bias[side * heads + head]) for head in range(heads)], axis=0
    )
    logits = raw_gates + bias
    log_gates = jnp.minimum(logits, 0.0) - jnp.log1p(jnp.exp(-jnp.abs(logits)))
    decay = jnp.dot(log_gates, reach[:tree_rows, :], **exact)
    decay = decay * in_tree.astype(jnp.float32)
    picked = jnp.where(late < 0, taken - 1, late_node)
    for node in range(most_taken):
        chosen = own_seq * (picked == node).astype(jnp.float32)
        decay = decay + jnp.dot(pending_logcum[node], chosen, **exact)
    decay = decay * LOG2E

    head_decay = tile_rows(decay, nodes)
    row = lax.broadcasted_iota(jnp.int32, (head_rows, size), 0)
    tree_keys = key_buf[...].astype(jnp.bfloat16)
    scale = head_size ** (-0.5) * LOG2E
    tree_scores, own_terms = [], []
    for item in range(group):
        raw = lax.dot_general(
            queries[item], tree_keys, NT, preferred_element_type=jnp.float32
        )
        own_terms.append(
            jnp.sum(
                jnp.where(lane == item * nodes + row % nodes, head_decay, 0.0),
                axis=1,
                keepdims=True,
            )
        )
        reached = jnp.concatenate([ancestry[item * nodes : (item + 1) * nodes, :]] * heads, axis=0)
        offered = jnp.where(late_item == item, jnp.where(late_node < taken, in_late, 0), 0)
        seen = reached * in_tree.astype(jnp.float32) + offered.astype(jnp.float32) > 0.5
        tree_scores.append(jnp.where(seen, raw * scale - head_decay, -MASKED))
    terms[...] = stacked(own_terms, head_rows, head_size)[: terms.shape[0], :]
    return tree_scores, value_buf[...].astype(jnp.bfloat16)


def merge_kernel(kv_size, terms, *refs):
    packed, chunk = refs[:kv_size], refs[kv_size]
    head_size = packed[0].shape[1]
    heads = chunk.shape[1] // head_size
    head_rows = terms.shape[1]
    nodes = head_rows // heads
    group = chunk.shape[0] // nodes
    base = group * head_rows
    term = terms[:group, :]
    stats = [p[base:, :head_rows].astype(jnp.float32) for p in packed]
    tops = [s[:group] + term for s in stats]
    top = functools.reduce(jnp.maximum, tops)
    factors = [jnp.exp2(t - top) for t in tops]
    bottom = sum(
        (s[group : 2 * group] + s[2 * group : 3 * group]) * f
        for s, f in zip(stats, factors, strict=True)
    )
    factors = [f / bottom for f in factors]
    row = lax.broadcasted_iota(jnp.int32, (head_rows, head_rows), 0)
    lane = lax.broadcasted_iota(jnp.int32, (head_rows, head_rows), 1)
    for item in range(group):
        rows = slice(item * head_rows, (item + 1) * head_rows)
        attended = jnp.zeros((head_rows, head_size), jnp.float32)
        for source in range(kv_size):
            spread = jnp.where(row == lane, factors[source][item : item + 1, :], 0.0)
            high = spread.astype(jnp.bfloat16)
            low = (spread - high.astype(jnp.float32)).astype(jnp.bfloat16)
            held_rows = packed[source][rows, :]
            attended += jnp.dot(high, held_rows, preferred_element_type=jnp.float32)
            attended += jnp.dot(low, held_rows, preferred_element_type=jnp.float32)
        attended = attended.astype(jnp.bfloat16)
        for head in range(heads):
            chunk[item * nodes : (item + 1) * nodes, head * head_size : (head + 1) * head_size] = (
                attended[head * nodes : (head + 1) * nodes, :]
            )


def project_kernel(other, weight, *refs):
    *chunks, out = refs
    side = lax.axis_index("tp")
    half = 1 - side if other else side
    rows, cols = chunks[0].shape[0], out.shape[1]
    part = weight[:, pl.ds(pl.multiple_of(half * cols, cols), cols)]
    for i, chunk in enumerate(chunks):
        out[i * rows : (i + 1) * rows, :] = jnp.dot(
            chunk[...], part, preferred_element_type=jnp.float32
        ).astype(jnp.bfloat16)


def add_kernel(kept, early, late, out, buf, sem):
    place = lax.axis_index("kv")
    rows = late.shape[0] // len(LATE)
    copies = []
    for i, step in enumerate(EARLY + LATE):
        span = slice(i * rows, (i + 1) * rows)
        first = (i - len(EARLY)) * rows
        received = late[first : first + rows, :] if i >= len(EARLY) else early[span, :]
        buf[span, :] = (kept[span, :].astype(jnp.float32) + received.astype(jnp.float32)).astype(
            jnp.bfloat16
        )
        target = pl.ds(pl.multiple_of(partner_of(place, step) * rows, rows), rows)
        copies.append(pltpu.make_async_copy(buf.at[pl.ds(i * rows, rows)], out.at[target], sem.at[i]))
        copies[-1].start()
    for copy in copies:
        copy.wait()


def exchange(array, axis, size, step):
    return lax.ppermute(array, axis, [(i, i ^ step) for i in range(size)])


def fast_shards(
    tokens,
    norm_gain,
    query_weight,
    key_weight,
    value_weight,
    forget_weight,
    forget_bias,
    query_gain,
    key_gain,
    output_weight,
    cache_keys,
    cache_values,
    cache_logcum,
    pending_keys,
    pending_values,
    pending_logcum,
    lengths,
    accepted,
    parents,
):
    kv_size, tp_size = lax.axis_size("kv"), lax.axis_size("tp")
    seq_count, nodes, width = tokens.shape
    query_cols = query_weight.shape[1]
    head_size = query_gain.shape[0]
    heads = query_cols // head_size
    block_len = cache_keys.shape[1]
    most_taken = pending_keys.shape[1]
    rows = seq_count * nodes
    group = seq_count // kv_size
    head_rows = heads * nodes
    bf16, f32 = jnp.bfloat16, jnp.float32
    hbm = pl.BlockSpec(memory_space=pltpu.HBM)
    vmem = pl.BlockSpec(memory_space=pltpu.VMEM)
    smem = pl.BlockSpec(memory_space=pltpu.SMEM)
    depth_parts = 4
    count = group * nodes
    packed_shape = in_vmem((group * head_rows + STAT_ROWS, head_size), bf16)
    token_matrix = tokens.reshape(rows, width)
    norm_row = norm_gain.reshape(1, width)
    query_row = query_gain.reshape(1, head_size)
    key_array = cache_keys.reshape(seq_count, block_len, head_size)
    value_array = cache_values.reshape(seq_count, block_len, head_size)

    farthest, second_queries, query_matrix, decays = pl.pallas_call(
        functools.partial(first_kernel, kv_size),
        compiler_params=pltpu.CompilerParams(vmem_limit_bytes=GRANT),
        name="first",
        out_shape=[
            packed_shape,
            in_vmem((group, head_rows, head_size), bf16),
            in_vmem((width, query_cols), bf16),
            in_vmem((seq_count, heads, block_len), f32),
        ],
        in_specs=[hbm] * 8,
        out_specs=[vmem] * 4,
        scratch_shapes=[
            pltpu.SMEM((seq_count,), jnp.int32),
            pltpu.VMEM((2, count, width), bf16),
            pltpu.VMEM((1, width), f32),
            pltpu.VMEM((1, head_size), f32),
            pltpu.VMEM((group, block_len, head_size), bf16),
            pltpu.VMEM((group, block_len, head_size), bf16),
            pltpu.VMEM((seq_count, heads, block_len), f32),
            pltpu.VMEM((2 * count, width), bf16),
            pltpu.SemaphoreType.DMA((8,)),
            pltpu.SemaphoreType.DMA((depth_parts,)),
        ],
    )(
        *[
            pltpu.with_memory_space_constraint(a, pltpu.HBM)
            for a in (
                lengths,
                token_matrix,
                norm_row,
                query_weight,
                query_row,
                key_array,
                value_array,
                jnp.swapaxes(cache_logcum, 1, 2),
            )
        ]
    )
    shared = [
        held(a)
        for a in (token_matrix, norm_row, query_matrix, query_row, key_array, value_array, decays)
    ]
    packed = {GO_ORDER[0]: farthest}
    packed[GO_ORDER[1]] = pl.pallas_call(
        functools.partial(second_kernel, GO_ORDER[1], nodes),
        compiler_params=pltpu.CompilerParams(vmem_limit_bytes=GRANT),
        name="second",
        out_shape=packed_shape,
        in_specs=[vmem] * 4,
        out_specs=vmem,
    )(held(second_queries), *shared[4:])
    for step in GO_ORDER[2:]:
        packed[step] = pl.pallas_call(
            functools.partial(next_kernel, step, nodes),
            compiler_params=pltpu.CompilerParams(vmem_limit_bytes=GRANT),
            out_shape=packed_shape,
            in_specs=[vmem] * 7,
            out_specs=vmem,
            scratch_shapes=[pltpu.VMEM((count, width), bf16)],
        )(*shared)
    moved = {}
    for step in GO_ORDER:
        moved[step] = exchange(packed[step], "kv", kv_size, step)
    own, terms = pl.pallas_call(
        functools.partial(own_kernel, tp_size, nodes),
        compiler_params=pltpu.CompilerParams(vmem_limit_bytes=GRANT),
        name="own",
        out_shape=[packed_shape, in_vmem((8, head_rows), f32)],
        in_specs=[smem, smem] + [vmem] * 15,
        out_specs=[vmem, vmem],
        scratch_shapes=[pltpu.VMEM((2 * count, head_size), f32)] * 2
        + [pltpu.VMEM((count, width), bf16)],
        cost_estimate=pl.CostEstimate(flops=4_000_000_000, bytes_accessed=1_000_000, transcendentals=0),
    )(
        accepted,
        forget_bias,
        parents,
        forget_weight.T,
        pending_keys.reshape(seq_count, most_taken, head_size),
        pending_values.reshape(seq_count, most_taken, head_size),
        jnp.transpose(pending_logcum, (1, 2, 0)),
        held(key_weight),
        held(value_weight),
        key_gain.reshape(1, head_size),
        *shared,
    )
    chunk = pl.pallas_call(
        functools.partial(merge_kernel, kv_size),
        compiler_params=pltpu.CompilerParams(vmem_limit_bytes=GRANT),
        name="merge",
        out_shape=in_vmem((group * nodes, query_cols), bf16),
        in_specs=[vmem] * (kv_size + 1),
        out_specs=vmem,
    )(held(terms), held(own), *[held(moved[s]) for s in range(1, kv_size)])
    chunks = {0: chunk}
    for step in BACK_ORDER:
        chunks[step] = exchange(chunk, "kv", kv_size, step)
    cols = output_weight.shape[1] // tp_size
    weight = held(output_weight)

    def project(steps, other):
        return pl.pallas_call(
            functools.partial(project_kernel, other),
            compiler_params=pltpu.CompilerParams(vmem_limit_bytes=GRANT),
            name="project",
            out_shape=in_vmem((len(steps) * count, cols), bf16),
            in_specs=[vmem] * (len(steps) + 1),
            out_specs=vmem,
            cost_estimate=pl.CostEstimate(flops=1_000_000_000, bytes_accessed=0, transcendentals=0),
        )(weight, *[held(chunks[step]) for step in steps])

    received = []
    for steps in (EARLY, LATE):
        sent = project(steps, True)
        received.append(held(exchange(sent, "tp", tp_size, 1)))
    kept = project(EARLY + LATE, False)
    summed = pl.pallas_call(
        add_kernel,
        compiler_params=pltpu.CompilerParams(vmem_limit_bytes=GRANT),
        name="add",
        out_shape=jax.ShapeDtypeStruct((rows, cols), bf16),
        in_specs=[vmem] * 3,
        out_specs=hbm,
        scratch_shapes=[pltpu.VMEM((rows, cols), bf16), pltpu.SemaphoreType.DMA((kv_size,))],
    )(held(kept), *received)
    return summed.reshape(seq_count, nodes, cols)


def fits_fast(mesh, shapes):
    kv_size = mesh.shape["kv"]
    seq_count = shapes["tokens"][0] // mesh.shape["dp"]
    one_key_head = shapes["cache_keys"][2] == mesh.shape["tp"]
    small = kv_size == 4
    return small and one_key_head and mesh.shape["tp"] == 2 and seq_count % kv_size == 0


def chosen_shards(mesh):
    def run(*args):
        shapes = {"tokens": args[0].shape, "cache_keys": args[10].shape}
        shapes["tokens"] = (shapes["tokens"][0] * mesh.shape["dp"],)
        shapes["cache_keys"] = (0, 0, shapes["cache_keys"][2] * mesh.shape["tp"])
        if not fits_fast(mesh, shapes):
            return shards(*args)
        return fast_shards(*args)

    return run


def solution(mesh):
    placed = (
        P("dp", None, None),
        P(),
        P(None, "tp"),
        P(None, "tp"),
        P(None, "tp"),
        P(),
        P(),
        P(),
        P(),
        P("tp", "kv"),
        P("dp", "kv", "tp", None),
        P("dp", "kv", "tp", None),
        P("dp", "kv", "tp"),
        P("dp", None, "tp", None),
        P("dp", None, "tp", None),
        P("dp", None, "tp"),
        P("dp"),
        P("dp"),
        P("dp", None),
    )
    return jax.shard_map(
        chosen_shards(mesh), mesh=mesh, in_specs=placed, out_specs=P("dp", None, ("kv", "tp")), check_vma=False
    )
```
